32 devices in a mesh: fs: 4 (over z), rep: 4 (over y, x), tp: 2 (over core).
Axes of the slice: x: 2, y: 2, z: 4, core: 2. Of those that a mesh axis runs over, the one named last changes fastest.
Arguments:
- inputs: bfloat16 [4096, 2048], P(('fs', 'rep')), may hold values from -6 to 6
- cot_query: bfloat16 [4096, 2048], P(('fs', 'rep'), 'tp'), may hold values from -0.09375 to 0.09375
- cot_key: bfloat16 [4096, 512], P(('fs', 'rep'), 'tp'), may hold values from -0.09375 to 0.09375
- basis_query: bfloat16 [2048, 512], P('fs'), may hold values from -0.125 to 0.125
- basis_key: bfloat16 [2048, 512], P('fs'), may hold values from -0.125 to 0.125
- weight_query: float32 [2048, 2048], P('fs', 'tp'), may hold values from -0.125 to 0.125
- weight_key: float32 [2048, 512], P('fs', 'tp'), may hold values from -0.125 to 0.125
- moments_query: float32 [2, 512, 2048], P(None, 'fs', 'tp'), may hold values from -8 to 8, as said below
- moments_key: float32 [2, 512, 512], P(None, 'fs', 'tp'), may hold values from -8 to 8, as said below
Outputs:
- step_query: float32 [2048, 2048], P('fs', 'tp')
- step_key: float32 [2048, 512], P('fs', 'tp')
- new_weight_query: float32 [2048, 2048], P('fs', 'tp')
- new_weight_key: float32 [2048, 512], P('fs', 'tp')
- copy_query: bfloat16 [2048, 2048], P(None, 'tp')
- copy_key: bfloat16 [2048, 512], P(None, 'tp')
- new_moments_query: float32 [2, 512, 2048], P(None, 'fs', 'tp')
- new_moments_key: float32 [2, 512, 512], P(None, 'fs', 'tp')
The draws below stay inside these ranges and needn't reach their ends.
Inputs may be any that keep to these rules, and one draw needn't show every extreme that they name: `moments_query`: entry 1 along the first dimension is positive. `moments_key`: entry 1 along the first dimension is positive.
All inputs are finite; a program needn't handle non-finite values.
Results may differ from the reference program's by a relative error of at most 0.009.
Values may be sent and summed in bfloat16 or wider, within the bound.
A program may use at most 64 MiB of HBM per device.

```python
import math
import jax
import jax.numpy as jnp
from jax import lax

D = 2048
DQ = 2048
DKV = 512
RANK = 512
TOKENS = 4096


def moment_draw(key, columns):
    first_key, second_key = jax.random.split(jax.random.fold_in(key, 7))
    position = jnp.arange(RANK, dtype=jnp.float32) / max(RANK - 1, 1)
    level = 0.1 * 10.0 ** position[:, None]
    first = jnp.clip(jax.random.normal(first_key, (RANK, columns), jnp.float32), -4.0, 4.0)
    spread = jnp.exp(jax.random.uniform(second_key, (RANK, columns), jnp.float32, math.log(0.05), math.log(0.5)))
    return jnp.stack([first * level, spread * level * level]).astype(jnp.float32)


def draw_moments_query(key, part):
    return moment_draw(key, DQ)


def draw_moments_key(key, part):
    return moment_draw(key, DKV)


def shard_levels(stream_key, shape, shards, smallest, largest):
    gain, own = 1.0, jax.random.fold_in(stream_key, 6)
    for dim, shards_of in shards:
        heights = jnp.exp(jax.random.uniform(jax.random.fold_in(own, dim), (shards_of,), jnp.float32, smallest / len(shards), largest / len(shards)))
        gain = gain * jnp.repeat(heights, shape[dim] // shards_of).reshape([-1 if axis == dim else 1 for axis in range(len(shape))])
    return gain


def scatter_about(own_key, shape, width, limit, cuts=(), kind=jnp.bfloat16):
    gain = shard_levels(own_key, shape, cuts, -0.22, 0.18) if cuts else 1.0
    drawn = jax.random.normal(own_key, shape, jnp.float32) * width * gain
    return jnp.minimum(jnp.maximum(drawn, -limit), limit).astype(kind)


def setup_inputs(seed: int = 0) -> dict:
    streams_of = jax.random.split(jax.random.key(seed), 10)
    inputs = scatter_about(streams_of[0], (TOKENS, D), 1.0, 6.0, ((0, 16),))
    cot_query = scatter_about(streams_of[1], (TOKENS, DQ), (1.0 / (TOKENS ** 0.5)), 0.09375, ((0, 16), (1, 2)))
    cot_key = scatter_about(streams_of[2], (TOKENS, DKV), (1.0 / (TOKENS ** 0.5)), 0.09375, ((0, 16), (1, 2)))
    basis_query = scatter_about(streams_of[3], (D, RANK), D ** -0.5, 0.125, ((0, 4),))
    basis_key = scatter_about(streams_of[4], (D, RANK), D ** -0.5, 0.125, ((0, 4),))
    weight_query = scatter_about(streams_of[5], (D, DQ), D ** -0.5, 0.125, ((0, 4), (1, 2)), jnp.float32)
    weight_key = scatter_about(streams_of[6], (D, DKV), D ** -0.5, 0.125, ((0, 4), (1, 2)), jnp.float32)
    moments_query = draw_moments_query(jax.random.fold_in(streams_of[9], 71), 0)
    moments_key = draw_moments_key(jax.random.fold_in(streams_of[9], 71), 0)
    return dict(inputs=inputs, cot_query=cot_query, cot_key=cot_key, basis_query=basis_query, basis_key=basis_key, weight_query=weight_query, weight_key=weight_key, moments_query=moments_query, moments_key=moments_key)


def reference(inputs, cot_query, cot_key, basis_query, basis_key, weight_query, weight_key, moments_query, moments_key):
    span = math.gcd(TOKENS, 8192)
    blocks = TOKENS // span
    in_blocks = inputs.reshape(blocks, span, D)
    query_blocks = cot_query.reshape(blocks, span, DQ)
    key_blocks = cot_key.reshape(blocks, span, DKV)

    def add_block(totals, pieces):
        rows, c_query, c_key = pieces
        rows = rows.astype(jnp.float32)
        grad_q = jnp.dot(rows.T, c_query.astype(jnp.float32), precision=lax.Precision.HIGHEST, preferred_element_type=jnp.float32)
        grad_k = jnp.dot(rows.T, c_key.astype(jnp.float32), precision=lax.Precision.HIGHEST, preferred_element_type=jnp.float32)
        return ((totals[0] + grad_q, totals[1] + grad_k), None)
    start = (jnp.zeros((D, DQ), jnp.float32), jnp.zeros((D, DKV), jnp.float32))
    (grad_query, grad_key), unused = lax.scan(add_block, start, (in_blocks, query_blocks, key_blocks))

    def update(grad, basis, weight, moments):
        low = jnp.dot(basis.astype(jnp.float32).T, grad, precision=lax.Precision.HIGHEST, preferred_element_type=jnp.float32)
        first = 0.9 * moments[0] + 0.1 * low
        second = 0.95 * moments[1] + 0.05 * low * low
        normed = first / (jnp.sqrt(second) + 1e-08)
        scale = lax.rsqrt(jnp.mean(normed * normed) + 1e-06)
        direction = normed.astype(jnp.bfloat16)
        step = scale * jnp.dot(basis, direction, preferred_element_type=jnp.float32)
        new_weight = weight - 0.02 * step
        return (step, new_weight, new_weight.astype(jnp.bfloat16), jnp.stack([first, second]))
    step_q, weight_q, copy_q, moments_q = update(grad_query, basis_query, weight_query, moments_query)
    step_k, weight_k, copy_k, moments_k = update(grad_key, basis_key, weight_key, moments_key)
    return (step_q, step_k, weight_q, weight_k, copy_q, copy_k, moments_q, moments_k)
```

```python
import functools
import jax
import jax.numpy as jnp
from jax import lax
from jax.experimental import pallas as pl
from jax.experimental.pallas import tpu as pltpu
from jax.sharding import PartitionSpec as P

MESH = pl.DeviceIdType.MESH
LANES = 128


def each(start, stop, body):
    if stop - start <= 4:
        for i in range(start, stop):
            body(i)
    else:
        lax.fori_loop(start, stop, lambda i, carry: (body(i), carry)[1], 0)


def remote(src, dst, send_sem, recv_sem, **device):
    return pltpu.make_async_remote_copy(
        src_ref=src,
        dst_ref=dst,
        send_sem=send_sem,
        recv_sem=recv_sem,
        device_id=device,
        device_id_type=MESH,
    )


def exchange(
    fs,
    rep,
    inputs_far,
    cot_query_far,
    cot_key_far,
    basis_query,
    basis_key,
    full_query,
    full_key,
    moments_query_far,
    moments_key_far,
    basis_all,
    weight_query_all,
    weight_key_all,
    dir_query,
    dir_key,
    low_query,
    low_key,
    totals,
    inputs,
    cot_query,
    cot_key,
    moments_query,
    moments_key,
    loaded_query,
    loaded_key,
    wide_query,
    wide_key,
    factor,
    part_send,
    part_recv,
    slab,
    slab_recv,
    low_all,
    squares,
    pair,
    az_s,
    az_r,
    ap_s,
    ap_r,
    ez_s,
    ez_r,
    ep_s,
    ep_r,
    bp_s,
    bp_r,
    bz_s,
    bz_r,
    lp_s,
    lp_r,
    dr_s,
    dl_s,
    dz_r,
    qz_s,
    qz_r,
    pair_s,
    pair_r,
    local,
):
    f, r, c = lax.axis_index("fs"), lax.axis_index("rep"), lax.axis_index("tp")
    height = basis_query.shape[0]
    part = height // rep
    rank = basis_query.shape[1]
    rows = rank // fs
    tokens = inputs.shape[0]
    per = part_send.shape[0] // rep
    query_units = cot_query.shape[1] // LANES
    units = query_units + cot_key.shape[1] // LANES

    def ahead(i):
        return lax.rem(f + i, fs)

    def behind(i):
        return lax.rem(f + fs - i, fs)

    def beside(j):
        return lax.rem(r + j, rep)

    near = r + 1 - 2 * lax.rem(r, 2)
    far = r + 2 - 4 * (r // 2)
    across = 3 - r
    owners = (r, r, near, far)
    targets = (near, far, far, near)
    senders = (near, far, across, across)

    def span_of(slot, width):
        return (pl.ds(0, width), pl.ds(0, width), pl.ds(0, width // 2), pl.ds(width // 2, width // 2))[slot]

    def piece(source, owner):
        return pl.ds(pl.multiple_of(source * height + owner * part, part), part)

    own_part = pl.ds(pl.multiple_of(r * part, part), part)
    own_block = pl.ds(pl.multiple_of(f * height, height), height)

    def low_rows(source):
        return pl.ds(pl.multiple_of(source * rows, rows), rows)

    loads = [
        pltpu.make_async_copy(source, target, local.at[3 + n])
        for n, (source, target) in enumerate(
            (
                (full_query, loaded_query),
                (full_key, loaded_key),
                (inputs_far, inputs),
                (cot_query_far, cot_query),
                (cot_key_far, cot_key),
                (moments_query_far, moments_query),
                (moments_key_far, moments_key),
            )
        )
    ]
    barrier = pltpu.get_barrier_semaphore()

    def greet_fs(i):
        pl.semaphore_signal(barrier, inc=1, device_id={"fs": ahead(i)}, device_id_type=MESH)

    def greet_rep(j):
        pl.semaphore_signal(barrier, inc=1, device_id={"rep": beside(j)}, device_id_type=MESH)

    each(1, fs, greet_fs)
    each(1, rep, greet_rep)
    pl.semaphore_signal(barrier, inc=1, device_id={"tp": 1 - c}, device_id_type=MESH)
    pl.semaphore_wait(barrier, fs + rep - 1)

    bases = (basis_query, basis_key)
    weights = ((wide_query, weight_query_all), (wide_key, weight_key_all))

    def basis_fs(x, source, target):
        return remote(
            bases[x].at[own_part],
            basis_all.at[c, piece(source, r)],
            az_s.at[target],
            az_r.at[source],
            fs=target,
        )

    for x in range(2):

        @pl.when(c == x)
        def start_basis():
            each(1, fs, lambda i: basis_fs(x, f, ahead(i)).start())
            pltpu.make_async_copy(bases[x], basis_all.at[c, own_block], local.at[0]).start()

    for load in loads:
        load.start()
    own_basis = pltpu.make_async_copy(basis_query, basis_all.at[c, own_block], local.at[0])

    def basis_hop(source, slot, owner):
        block = basis_all.at[c, piece(source, owner), span_of(slot, rank)]
        return remote(
            block, block, ap_s.at[source, slot], ap_r.at[source, slot], rep=targets[slot]
        )

    def weight_fs(x, source, target):
        return remote(
            weights[x][0].at[own_part],
            weights[x][1].at[piece(source, r)],
            ez_s.at[x, target],
            ez_r.at[x, source],
            fs=target,
        )

    def weight_hop(x, source, slot, owner):
        block = weights[x][1].at[piece(source, owner), span_of(slot, weights[x][1].shape[1])]
        return remote(
            block, block, ep_s.at[x, source, slot], ep_r.at[x, source, slot], rep=targets[slot]
        )

    for load in loads[:2]:
        load.wait()
    wide_query[...] = loaded_query[...].astype(jnp.bfloat16)
    wide_key[...] = loaded_key[...].astype(jnp.bfloat16)

    def spread_basis(i):
        source = behind(i)
        basis_fs(0, source, source).wait_recv()
        for slot in (0, 1):
            basis_hop(source, slot, owners[slot]).start()

    each(1, fs, spread_basis)

    own_copies = [
        pltpu.make_async_copy(wide_query, weight_query_all.at[own_block], local.at[1]),
        pltpu.make_async_copy(wide_key, weight_key_all.at[own_block], local.at[2]),
    ]
    for copy in own_copies:
        copy.start()

    def start_weight(i):
        weight_fs(0, f, ahead(i)).start()
        weight_fs(1, f, ahead(i)).start()

    each(1, fs, start_weight)

    def relay_basis(i):
        source = behind(i)
        for slot in (0, 1):
            basis_hop(source, slot, senders[slot]).wait_recv()
            basis_hop(source, slot + 2, owners[slot + 2]).start()

    def all_basis(i):
        for slot in (2, 3):
            basis_hop(behind(i), slot, senders[slot]).wait_recv()

    each(1, fs, relay_basis)
    each(1, fs, all_basis)
    own_basis.wait()
    for load in loads[2:]:
        load.wait()

    for t in range(0, tokens, LANES):
        value = jnp.dot(
            inputs[t : t + LANES, :], basis_all[c], preferred_element_type=jnp.float32
        )
        factor[c, :, t : t + LANES] = value.T.astype(jnp.bfloat16)
    for u in range(units, per * rep):
        part_send[u] = jnp.zeros(part_send.shape[1:], jnp.bfloat16)
    factor_copy = remote(
        factor.at[c], factor.at[c], pair_s.at[0], pair_r.at[0], tp=1 - c
    )
    factor_back = remote(
        factor.at[1 - c], factor.at[1 - c], pair_s.at[0], pair_r.at[0], tp=1 - c
    )
    factor_copy.start()
    swap = remote(basis_all.at[c], basis_all.at[c], pair_s.at[1], pair_r.at[1], tp=1 - c)
    swap_back = remote(
        basis_all.at[1 - c], basis_all.at[1 - c], pair_s.at[1], pair_r.at[1], tp=1 - c
    )
    factor_back.wait_recv()
    swap.start()

    for x, cot in ((0, cot_query), (1, cot_key)):
        columns = cot.shape[1]
        width = 2 * LANES if columns % (2 * LANES) == 0 else LANES
        for n in range(0, columns, width):
            value = jnp.dot(
                factor[x], cot[:, n : n + width], preferred_element_type=jnp.float32
            ).astype(jnp.bfloat16)
            for k in range(0, width, LANES):
                part_send[x * query_units + (n + k) // LANES] = value[:, k : k + LANES]

    def group(owner):
        return pl.ds(owner * per, per)

    def part_rep(source, target):
        return remote(
            part_send.at[group(target)],
            part_recv.at[source],
            bp_s.at[target],
            bp_r.at[source],
            rep=target,
        )

    each(1, rep, lambda j: part_rep(r, beside(j)).start())
    part_recv[r] = part_send[group(r)]
    each(1, rep, lambda j: part_rep(beside(j), beside(j)).wait_recv())
    for p in range(per):
        value = part_recv[0, p].astype(jnp.float32)
        for q in range(1, rep):
            value = value + part_recv[q, p].astype(jnp.float32)
        slab[p] = value.astype(jnp.bfloat16)

    def slab_fs(source, target):
        return remote(
            slab.at[:, low_rows(target)],
            slab_recv.at[source],
            bz_s.at[target],
            bz_r.at[source],
            fs=target,
        )

    each(1, fs, lambda i: slab_fs(f, ahead(i)).start())

    def spread_weight(i):
        source = behind(i)
        for x in range(2):
            weight_fs(x, source, source).wait_recv()
            for slot in (0, 1):
                weight_hop(x, source, slot, owners[slot]).start()

    def relay_weight(i):
        source = behind(i)
        for slot in (0, 1):
            for x in range(2):
                weight_hop(x, source, slot, senders[slot]).wait_recv()
                weight_hop(x, source, slot + 2, owners[slot + 2]).start()

    spread_weight(1)
    slab_recv[f] = slab[:, low_rows(f), :]
    each(1, fs, lambda i: slab_fs(behind(i), behind(i)).wait_recv())
    for p in range(per):
        value = slab_recv[0, p].astype(jnp.float32)
        for q in range(1, fs):
            value = value + slab_recv[q, p].astype(jnp.float32)
        low_all[r * per + p] = value.astype(jnp.bfloat16)

    def low_rep(owner, target):
        block = low_all.at[group(owner)]
        return remote(block, block, lp_s.at[target], lp_r.at[owner], rep=target)

    each(1, rep, lambda j: low_rep(r, beside(j)).start())
    each(1, rep, lambda j: low_rep(beside(j), beside(j)).wait_recv())

    for x, moments, direction, low_out in (
        (0, moments_query, dir_query, low_query),
        (1, moments_key, dir_key, low_key),
    ):
        total = jnp.zeros((8, LANES), jnp.float32)
        for n in range(0, moments.shape[2], LANES):
            span = slice(n, n + LANES)
            low = low_all[x * query_units + n // LANES].astype(jnp.float32)
            low_out[:, span] = low
            first = 0.9 * moments[0, :, span] + 0.1 * low
            second = 0.95 * moments[1, :, span] + 0.05 * low * low
            normed = first / (jnp.sqrt(second) + 1e-08)
            direction[low_rows(f), span] = normed.astype(jnp.bfloat16)
            total = total + jnp.sum((normed * normed).reshape(rows // 8, 8, LANES), axis=0)
        squares[f, x] = total

    directions = (dir_query, dir_key)

    right, left = ahead(1), behind(1)

    def move_right(x, source):
        block = directions[x].at[low_rows(source)]
        return remote(block, block, dr_s.at[x, source], dz_r.at[x, source], fs=right)

    def move_left(x, source):
        block = directions[x].at[low_rows(source)]
        return remote(block, block, dl_s.at[x, source], dz_r.at[x, source], fs=left)

    def squares_fs(source, target):
        block = squares.at[source]
        return remote(block, block, qz_s.at[target], qz_r.at[source], fs=target)

    each(1, fs, lambda i: squares_fs(f, ahead(i)).start())

    @pl.when(f + 1 < fs)
    def start_right():
        for x in range(2):
            move_right(x, f).start()

    @pl.when(f > 0)
    def start_left():
        for x in range(2):
            move_left(x, f).start()

    each(2, fs, spread_weight)

    def relay_direction(k):
        @pl.when(f - k >= 0)
        def from_left():
            for x in range(2):
                move_right(x, f - k).wait_recv()

                @pl.when(f + 1 < fs)
                def onward():
                    move_right(x, f - k).start()

        @pl.when(f + k < fs)
        def from_right():
            for x in range(2):
                move_left(x, f + k).wait_recv()

                @pl.when(f > 0)
                def onward():
                    move_left(x, f + k).start()

    def relay_both(k):
        relay_weight(k)
        relay_direction(k)

    each(1, fs, relay_both)

    each(1, fs, lambda i: squares_fs(behind(i), behind(i)).wait_recv())
    total = squares[0]
    for q in range(1, fs):
        total = total + squares[q]
    pair[c] = total
    total_copy = remote(pair.at[c], pair.at[c], pair_s.at[2], pair_r.at[2], tp=1 - c)
    total_back = remote(pair.at[1 - c], pair.at[1 - c], pair_s.at[2], pair_r.at[2], tp=1 - c)
    total_copy.start()
    total_back.wait_recv()
    totals[...] = pair[0] + pair[1]

    def end_fs(i):
        source, target = behind(i), ahead(i)
        for x in range(2):
            for slot in (2, 3):
                weight_hop(x, source, slot, senders[slot]).wait_recv()
            for slot in range(4):
                weight_hop(x, source, slot, owners[slot]).wait_send()
            weight_fs(x, f, target).wait_send()
        for slot in range(4):
            basis_hop(source, slot, owners[slot]).wait_send()
        basis_fs(0, f, target).wait_send()
        slab_fs(f, target).wait_send()
        squares_fs(f, target).wait_send()

    def end_direction(k):
        @pl.when((f - k >= 0) & (f + 1 < fs))
        def end_right():
            for x in range(2):
                move_right(x, f - k).wait_send()

        @pl.when((f + k < fs) & (f > 0))
        def end_left():
            for x in range(2):
                move_left(x, f + k).wait_send()

    def end_rep(j):
        part_rep(r, beside(j)).wait_send()
        low_rep(r, beside(j)).wait_send()

    each(1, fs, end_fs)
    each(0, fs, end_direction)
    each(1, rep, end_rep)
    swap_back.wait_recv()
    factor_copy.wait_send()
    swap.wait_send()
    total_copy.wait_send()
    for copy in own_copies:
        copy.wait()


def exchange_grid(
    fs,
    rep,
    inputs_far,
    cot_query_far,
    cot_key_far,
    basis_query,
    basis_key,
    full_query,
    full_key,
    moments_query_far,
    moments_key_far,
    basis_all,
    weight_query_all,
    weight_key_all,
    dir_query,
    dir_key,
    low_query,
    low_key,
    totals,
    inputs,
    cot_query,
    cot_key,
    moments_query,
    moments_key,
    loaded_query,
    loaded_key,
    factor,
    part,
    got_first,
    pair_sum,
    got_second,
    slab,
    slab_recv,
    low_all,
    part_squares,
    squares,
    pair,
    az_s,
    az_r,
    ap_s,
    ap_r,
    wz_s,
    wz_r,
    wp_s,
    wp_r,
    kz_s,
    kz_r,
    h1_s,
    h1_r,
    h2_s,
    h2_r,
    bz_s,
    bz_r,
    lp_s,
    lp_r,
    dz_s,
    dz_r,
    dp_s,
    dp_r,
    qz_s,
    qz_r,
    pair_s,
    pair_r,
    local,
):
    f, r, c = lax.axis_index("fs"), lax.axis_index("rep"), lax.axis_index("tp")
    height, rank = basis_query.shape
    quarter = height // rep
    rows = rank // fs
    own = rows // rep
    tokens = inputs.shape[0]
    query_units = cot_query.shape[1] // LANES
    units = query_units + cot_key.shape[1] // LANES
    streams = ((0, units // 2), (units // 2, units // 2))
    f32, bf16 = jnp.float32, jnp.bfloat16

    near = r + 1 - 2 * lax.rem(r, 2)
    far = r + 2 - 4 * (r // 2)
    across = 3 - r
    pending = []

    def when(conds, body):
        if not conds:
            body()
            return
        test = conds[0]
        for cond in conds[1:]:
            test = test & cond
        pl.when(test)(body)

    def send(make, *conds):
        when(conds, lambda: make().start())
        pending.append((make, conds))

    def receive(make, *conds):
        when(conds, lambda: make().wait_recv())

    def sources(d):
        return ((f - d, f >= d), (f + d, f + d < fs))

    def beside(j):
        return lax.rem(r + j, rep)

    def rows_of(start, size):
        return pl.ds(pl.multiple_of(start, size), size)

    chunks = 2
    chunk = quarter // chunks

    def piece(source, owner, k):
        return rows_of(source * height + owner * quarter + k * chunk, chunk)

    mirror = f // (fs // 2)
    place_in_half = f + mirror * (fs - 1 - 2 * f)

    def other(n):
        low_side = n - 1 + (n + fs - 1 - place_in_half) // fs
        return low_side + mirror * (fs - 1 - 2 * low_side)

    own_block = rows_of(f * height, height)

    loads = [
        pltpu.make_async_copy(source, target, local.at[1 + n])
        for n, (source, target) in enumerate(
            (
                (full_query, loaded_query),
                (full_key, loaded_key),
                (inputs_far, inputs),
                (cot_query_far, cot_query),
                (cot_key_far, cot_key),
                (moments_query_far, moments_query),
                (moments_key_far, moments_key),
            )
        )
    ]
    barrier = pltpu.get_barrier_semaphore()
    for i in range(1, fs):
        pl.semaphore_signal(
            barrier, inc=1, device_id={"fs": lax.rem(f + i, fs)}, device_id_type=MESH
        )
    for mate in (near, far):
        pl.semaphore_signal(barrier, inc=1, device_id={"rep": mate}, device_id_type=MESH)
    pl.semaphore_signal(barrier, inc=1, device_id={"tp": 1 - c}, device_id_type=MESH)
    pl.semaphore_wait(barrier, fs + 2)

    bases = (basis_query, basis_key)

    def basis_z(source, up, k):
        block = basis_all.at[c, piece(source, r, k)]
        return remote(
            block, block, az_s.at[1 - up, source, k], az_r.at[source, k], fs=f + 2 * up - 1
        )

    def basis_start(x, up, k):
        return remote(
            bases[x].at[rows_of(r * quarter + k * chunk, chunk)],
            basis_all.at[c, piece(f, r, k)],
            az_s.at[1 - up, f, k],
            az_r.at[f, k],
            fs=f + 2 * up - 1,
        )

    ways = ((1, f + 1 < fs), (0, f > 0))
    for x in range(2):

        @pl.when(c == x)
        def start_basis():
            for k in range(chunks):
                for up, there in ways:
                    pl.when(there)(lambda: basis_start(x, up, k).start())
            pltpu.make_async_copy(bases[x], basis_all.at[c, own_block], local.at[0]).start()

    for k in range(chunks):
        for up, there in ways:
            pending.append((functools.partial(basis_z, f, up, k), (there,)))
    for load in loads:
        load.start()
    own_basis = pltpu.make_async_copy(basis_query, basis_all.at[c, own_block], local.at[0])

    def hop_span(slot, width):
        return (pl.ds(0, width), pl.ds(0, width), pl.ds(0, width // 2), pl.ds(width // 2, width // 2))[slot]

    targets = (near, far, far, near)
    sent = (r, r, near, far)
    arriving = (near, far, across, across)

    def basis_hop(k, source, slot, owner):
        block = basis_all.at[c, piece(source, owner, k), hop_span(slot, rank)]
        return remote(
            block, block, ap_s.at[source, slot, k], ap_r.at[source, slot, k], rep=targets[slot]
        )

    def weight_hop(k, source, slot, owner):
        width = weight_query_all.shape[1]
        block = weight_query_all.at[piece(source, owner, k), hop_span(slot, width)]
        return remote(
            block, block, wp_s.at[source, slot, k], wp_r.at[source, slot, k], rep=targets[slot]
        )

    def spread(hop, source, *there):
        for slot in (0, 1):
            send(functools.partial(hop, source, slot, sent[slot]), *there)

    def relay(hop, source, *there):
        for slot in (0, 1):
            receive(functools.partial(hop, source, slot, arriving[slot]), *there)
            send(functools.partial(hop, source, slot + 2, sent[slot + 2]), *there)

    def finish(hop, source, *there):
        for slot in (2, 3):
            receive(functools.partial(hop, source, slot, arriving[slot]), *there)

    def query_z(source, up, k):
        block = weight_query_all.at[piece(source, r, k)]
        return remote(
            block, block, wz_s.at[1 - up, source, k], wz_r.at[source, k], fs=f + 2 * up - 1
        )

    def key_z(source, up, k):
        block = weight_key_all.at[rows_of(source * height + k * (height // chunks), height // chunks)]
        return remote(
            block, block, kz_s.at[1 - up, source, k], kz_r.at[source, k], fs=f + 2 * up - 1
        )

    def launch(line):
        for k in range(chunks):
            for up, there in ways:
                send(functools.partial(line, f, up, k), there)

    def onward(line, d, k):
        below, above = f - d, f + d
        receive(functools.partial(line, below, 1, k), f >= d)
        if d + 1 < fs:
            send(functools.partial(line, below, 1, k), f >= d, f + 1 < fs)
        receive(functools.partial(line, above, 0, k), f + d < fs)
        if d + 1 < fs:
            send(functools.partial(line, above, 0, k), f + d < fs, f > 0)

    def onward_all(line, d):
        for k in range(chunks):
            onward(line, d, k)

    for load in loads[:2]:
        load.wait()
    weight_query_all[own_block, :] = loaded_query[...].astype(bf16)
    weight_key_all[own_block, :] = loaded_key[...].astype(bf16)

    steps = [(d, k) for d in range(1, fs) for k in range(chunks)]
    for n, (d, k) in enumerate(steps):
        onward(basis_z, d, k)
        for source, there in sources(d):
            spread(functools.partial(basis_hop, k), source, there)
        if (d, k) == (max(fs - 2, 1), chunks - 1):
            launch(query_z)
            launch(key_z)
        if n >= chunks:
            before, j = steps[n - chunks]
            for source, there in sources(before):
                relay(functools.partial(basis_hop, j), source, there)
    for d, k in steps[-chunks:]:
        for source, there in sources(d):
            relay(functools.partial(basis_hop, k), source, there)
    onward_all(query_z, 1)
    spread(functools.partial(weight_hop, 0), other(1))
    for d, k in steps:
        for source, there in sources(d):
            finish(functools.partial(basis_hop, k), source, there)
    own_basis.wait()
    for load in loads[2:]:
        load.wait()

    for t in range(0, tokens, LANES):
        value = jnp.dot(inputs[t : t + LANES, :], basis_all[c], preferred_element_type=f32)
        factor[c, :, t : t + LANES] = value.T.astype(bf16)

    def partner(block, back, n):
        return (
            remote(block, block, pair_s.at[n], pair_r.at[n], tp=1 - c),
            remote(back, back, pair_s.at[n], pair_r.at[n], tp=1 - c),
        )

    factor_copy, factor_back = partner(factor.at[c], factor.at[1 - c], 0)
    swap, swap_back = partner(basis_all.at[c], basis_all.at[1 - c], 1)
    factor_copy.start()
    factor_back.wait_recv()
    swap.start()

    for x, cot in ((0, cot_query), (1, cot_key)):
        columns = cot.shape[1]
        width = 2 * LANES if columns % (2 * LANES) == 0 else LANES
        for n in range(0, columns, width):
            value = jnp.dot(
                factor[x], cot[:, n : n + width], preferred_element_type=f32
            ).astype(bf16)
            for k in range(0, width, LANES):
                for q in range(rep):
                    for s in range(fs):
                        part[x * query_units + (n + k) // LANES, q, s * own : (s + 1) * own] = value[
                            s * rows + q * own : s * rows + (q + 1) * own, k : k + LANES
                        ]

    half = rows // 2
    spans = (slice(0, half), slice(half, rows))
    mates = ((near, far), (far, near))

    def columns_of(g):
        return pl.ds(streams[g][0], streams[g][1])

    def first_hop(h, g, w):
        owner = (across, mates[h][0])[w]
        return remote(
            part.at[columns_of(g), owner, pl.ds(h * half, half)],
            got_first.at[h, w, columns_of(g)],
            h1_s.at[h, w, g],
            h1_r.at[h, w, g],
            rep=mates[h][0],
        )

    def second_hop(h, g):
        return remote(
            pair_sum.at[h, columns_of(g)],
            got_second.at[h, columns_of(g)],
            h2_s.at[h, g],
            h2_r.at[h, g],
            rep=mates[h][1],
        )

    def start_first(g, w):
        for h in range(2):
            send(functools.partial(first_hop, h, g, w))

    def start_second(g):
        for h in range(2):
            receive(functools.partial(first_hop, h, g, 0))
            for u in range(streams[g][0], sum(streams[g])):
                pair_sum[h, u] = (
                    part[u, mates[h][1], spans[h]].astype(f32) + got_first[h, 0, u].astype(f32)
                ).astype(bf16)
            send(functools.partial(second_hop, h, g))

    def slab_z(g, source, target):
        return remote(
            slab.at[columns_of(g), rows_of(target * own, own)],
            slab_recv.at[source, columns_of(g)],
            bz_s.at[g, target],
            bz_r.at[g, source],
            fs=target,
        )

    def end_rep(g):
        for h in range(2):
            receive(functools.partial(first_hop, h, g, 1))
            receive(functools.partial(second_hop, h, g))
            for u in range(streams[g][0], sum(streams[g])):
                slab[u, spans[h]] = (
                    part[u, r, spans[h]].astype(f32)
                    + got_first[h, 1, u].astype(f32)
                    + got_second[h, u].astype(f32)
                ).astype(bf16)
        for d in range(fs - 1, 0, -1):
            for target, there in sources(d):
                send(functools.partial(slab_z, g, f, target), there)
        for u in range(streams[g][0], sum(streams[g])):
            slab_recv[f, u] = slab[u, rows_of(f * own, own)]

    start_first(0, 0)
    start_first(0, 1)
    start_first(1, 0)
    start_second(0)
    start_first(1, 1)
    start_second(1)
    for k in range(1, chunks):
        spread(functools.partial(weight_hop, k), other(1))
    end_rep(0)
    end_rep(1)
    onward_all(query_z, 2)
    for k in range(chunks):
        spread(functools.partial(weight_hop, k), other(2))

    directions, lows = (dir_query, dir_key), (low_query, low_key)
    moments = (moments_query, moments_key)

    def place(u):
        x = 0 if u < query_units else 1
        n = (u - x * query_units) * LANES
        return x, slice(n, n + LANES)

    def pieces(g):
        first, last = streams[g][0], sum(streams[g])
        found = []
        if first < query_units:
            found.append((0, first * LANES, (min(last, query_units) - first) * LANES))
        if last > query_units:
            start = max(first, query_units)
            found.append((1, (start - query_units) * LANES, (last - start) * LANES))
        return found

    def dir_rows(source, owner):
        return rows_of(source * rows + owner * own, own)

    def update(g, owner):
        sums = [jnp.zeros((8, LANES), f32), jnp.zeros((8, LANES), f32)]
        mine = rows_of(owner * own, own)
        for u in range(streams[g][0], sum(streams[g])):
            x, span = place(u)
            low = low_all[owner, u].astype(f32)
            lows[x][mine, span] = low
            first = 0.9 * moments[x][0, mine, span] + 0.1 * low
            second = 0.95 * moments[x][1, mine, span] + 0.05 * low * low
            normed = first / (jnp.sqrt(second) + 1e-08)
            directions[x][dir_rows(f, owner), span] = normed.astype(bf16)
            sums[x] = sums[x] + jnp.sum((normed * normed).reshape(own // 8, 8, LANES), axis=0)
        for x in range(2):
            part_squares[owner, g, x] = sums[x]

    def low_hop(g, slot, owner):
        block = low_all.at[owner, columns_of(g)]
        return remote(block, block, lp_s.at[slot, g], lp_r.at[slot, g], rep=targets[slot])

    def dir_z(g, n, source, target):
        x, start, size = pieces(g)[n]
        block = directions[x].at[dir_rows(source, r), pl.ds(start, size)]
        return remote(block, block, dz_s.at[g, n, target], dz_r.at[g, n, source], fs=target)

    def dir_hop(g, n, slot, source, owner):
        x, start, size = pieces(g)[n]
        block = directions[x].at[dir_rows(source, owner), pl.ds(start, size)]
        return remote(
            block,
            block,
            dp_s.at[g, n, slot, source],
            dp_r.at[g, n, slot, source],
            rep=targets[slot],
        )

    def end_fs(g):
        for d in range(1, fs):
            for source, there in sources(d):
                receive(functools.partial(slab_z, g, source, source), there)
        for u in range(streams[g][0], sum(streams[g])):
            value = slab_recv[0, u].astype(f32)
            for q in range(1, fs):
                value = value + slab_recv[q, u].astype(f32)
            low_all[r, u] = value.astype(bf16)
        for slot in (0, 1):
            send(functools.partial(low_hop, g, slot, r))
        update(g, r)
        for d in range(fs - 1, 0, -1):
            for target, there in sources(d):
                for n in range(len(pieces(g))):
                    send(functools.partial(dir_z, g, n, f, target), there)

    end_fs(0)
    end_fs(1)

    def spread_dir(g, d):
        for source, there in sources(d):
            for n in range(len(pieces(g))):
                receive(functools.partial(dir_z, g, n, source, source), there)
                for slot in (0, 1):
                    send(functools.partial(dir_hop, g, n, slot, source, r), there)

    def relay_dir(d):
        for source, there in sources(d):
            for g in range(2):
                for n in range(len(pieces(g))):
                    receive(functools.partial(dir_hop, g, n, g, source, arriving[g]), there)
                    send(functools.partial(dir_hop, g, n, g + 2, source, sent[g + 2]), there)

    def finish_dir(d):
        for source, there in sources(d):
            for g in range(2):
                for n in range(len(pieces(g))):
                    receive(functools.partial(dir_hop, g, n, 1 - g, source, arriving[1 - g]), there)
                    receive(functools.partial(dir_hop, g, n, g + 2, source, across), there)

    onward_all(key_z, 1)
    for k in range(chunks):
        relay(functools.partial(weight_hop, k), other(1))
    for g in range(2):
        receive(functools.partial(low_hop, g, g, arriving[g]))
        send(functools.partial(low_hop, g, g + 2, sent[g + 2]))
    spread_dir(0, 1)
    spread_dir(1, 1)
    for d in range(2, fs):
        spread_dir(0, d)
        spread_dir(1, d)
        relay_dir(d - 1)
    relay_dir(fs - 1)
    for k in range(chunks):
        relay(functools.partial(weight_hop, k), other(2))
    for n in range(3, fs):
        for k in range(chunks):
            onward(query_z, n, k)
            spread(functools.partial(weight_hop, k), other(n))
    for d in range(2, fs - 1):
        onward_all(key_z, d)
    for g in range(2):
        receive(functools.partial(low_hop, g, 1 - g, arriving[1 - g]))
        receive(functools.partial(low_hop, g, g + 2, across))
        for j in range(1, rep):
            update(g, beside(j))
    for x in range(2):
        total = part_squares[0, 0, x] + part_squares[0, 1, x]
        for q in range(1, rep):
            total = total + (part_squares[q, 0, x] + part_squares[q, 1, x])
        squares[f, x] = total

    def squares_z(source, target):
        block = squares.at[source]
        return remote(block, block, qz_s.at[target], qz_r.at[source], fs=target)

    for d in range(1, fs):
        for target, there in sources(d):
            send(functools.partial(squares_z, f, target), there)
    for d in range(1, fs):
        for source, there in sources(d):
            receive(functools.partial(squares_z, source, source), there)
    total = squares[0]
    for q in range(1, fs):
        total = total + squares[q]
    pair[c] = total
    total_copy, total_back = partner(pair.at[c], pair.at[1 - c], 2)
    total_copy.start()

    for d in range(1, fs):
        finish_dir(d)
    for n in range(3, fs):
        for k in range(chunks):
            relay(functools.partial(weight_hop, k), other(n))
    onward_all(key_z, fs - 1)
    for n in range(1, fs):
        for k in range(chunks):
            finish(functools.partial(weight_hop, k), other(n))
    total_back.wait_recv()
    totals[...] = pair[0] + pair[1]
    for make, conds in pending:
        when(conds, lambda: make().wait_send())
    swap_back.wait_recv()
    for copy in (factor_copy, swap, total_copy):
        copy.wait_send()


def apply(
    count_query,
    count_key,
    totals,
    dir_query,
    dir_key,
    low_query,
    low_key,
    moments_query,
    moments_key,
    basis_all,
    weight_query_all,
    weight_key_all,
    basis_query,
    basis_key,
    weight_query,
    weight_key,
    step_query,
    step_key,
    new_weight_query,
    new_weight_key,
    copy_query,
    copy_key,
    new_moments_query,
    new_moments_key,
):
    parts = (
        (count_query, dir_query, weight_query_all, basis_query, weight_query),
        (count_key, dir_key, weight_key_all, basis_key, weight_key),
    )
    outs = (
        (step_query, new_weight_query, copy_query),
        (step_key, new_weight_key, copy_key),
    )
    for x in range(2):
        count, direction, weight_all, basis, weight = parts[x]
        step_out, new_weight_out, copy_out = outs[x]
        scale = lax.rsqrt(jnp.sum(totals[x], keepdims=True) / count + 1e-06)
        step = scale * jnp.dot(basis[...], direction[...], preferred_element_type=jnp.float32)
        step_out[...] = step
        new_weight_out[...] = weight[...] - 0.02 * step
        whole = scale * jnp.dot(
            basis_all[x], direction[...], preferred_element_type=jnp.float32
        )
        copy_out[...] = (weight_all[...].astype(jnp.float32) - 0.02 * whole).astype(jnp.bfloat16)

    @pl.when(pl.program_id(0) == 0)
    def moments_once():
        for moments, low_ref, out in (
            (moments_query, low_query, new_moments_query),
            (moments_key, low_key, new_moments_key),
        ):
            low = low_ref[...]
            out[0] = 0.9 * moments[0] + 0.1 * low
            out[1] = 0.95 * moments[1] + 0.05 * low * low


def on_device(
    inputs,
    cot_query,
    cot_key,
    basis_query,
    basis_key,
    weight_query,
    weight_key,
    moments_query,
    moments_key,
):
    fs, rep, tp = lax.axis_size("fs"), lax.axis_size("rep"), lax.axis_size("tp")
    assert tp == 2 and rep == 4
    height, rank = basis_query.shape
    rows = rank // fs
    tokens = inputs.shape[0]
    query_cols, key_cols = cot_query.shape[1], cot_key.shape[1]
    per = -(-((query_cols + key_cols) // LANES) // rep)
    vmem = pl.BlockSpec(memory_space=pltpu.VMEM)
    hbm = pl.BlockSpec(memory_space=pl.ANY)
    bf16, f32 = jnp.bfloat16, jnp.float32
    dma = pltpu.SemaphoreType.DMA
    shape = jax.ShapeDtypeStruct
    out_shape = (
        shape((2, height * fs, rank), bf16),
        shape((height * fs, query_cols), bf16),
        shape((height * fs, key_cols), bf16),
        shape((rank, query_cols), bf16),
        shape((rank, key_cols), bf16),
        shape((rows, query_cols), f32),
        shape((rows, key_cols), f32),
        shape((2, 8, LANES), f32),
    )
    own, units = rows // rep, (query_cols + key_cols) // LANES
    if own % 16 == 0 and fs % 2 == 0 and units % 2 == 0 and rows % rep == 0:
        kernel, out_specs = exchange_grid, (vmem,) * 8
        scratch = [
            pltpu.VMEM((tokens, inputs.shape[1]), bf16),
            pltpu.VMEM((tokens, query_cols), bf16),
            pltpu.VMEM((tokens, key_cols), bf16),
            pltpu.VMEM((2, rows, query_cols), f32),
            pltpu.VMEM((2, rows, key_cols), f32),
            pltpu.VMEM((height, query_cols), f32),
            pltpu.VMEM((height, key_cols), f32),
            pltpu.VMEM((2, rank, tokens), bf16),
            pltpu.VMEM((units, rep, rows, LANES), bf16),
            pltpu.VMEM((2, 2, units, rows // 2, LANES), bf16),
            pltpu.VMEM((2, units, rows // 2, LANES), bf16),
            pltpu.VMEM((2, units, rows // 2, LANES), bf16),
            pltpu.VMEM((units, rows, LANES), bf16),
            pltpu.VMEM((fs, units, own, LANES), bf16),
            pltpu.VMEM((rep, units, own, LANES), bf16),
            pltpu.VMEM((rep, 2, 2, 8, LANES), f32),
            pltpu.VMEM((fs, 2, 8, LANES), f32),
            pltpu.VMEM((2, 2, 8, LANES), f32),
            dma((2, fs, 2)),
            dma((fs, 2)),
            dma((fs, rep, 2)),
            dma((fs, rep, 2)),
            dma((2, fs, 2)),
            dma((fs, 2)),
            dma((fs, rep, 2)),
            dma((fs, rep, 2)),
            dma((2, fs, 2)),
            dma((fs, 2)),
            dma((2, 2, 2)),
            dma((2, 2, 2)),
            dma((2, 2)),
            dma((2, 2)),
            dma((2, fs)),
            dma((2, fs)),
            dma((4, 2)),
            dma((4, 2)),
            dma((2, 2, fs)),
            dma((2, 2, fs)),
            dma((2, 2, 4, fs)),
            dma((2, 2, 4, fs)),
            dma((fs,)),
            dma((fs,)),
            dma((3,)),
            dma((3,)),
            dma((8,)),
        ]
    else:
        kernel, out_specs = exchange, (vmem, hbm, hbm, vmem, vmem, vmem, vmem, vmem)
        scratch = [
            pltpu.VMEM((tokens, inputs.shape[1]), bf16),
            pltpu.VMEM((tokens, query_cols), bf16),
            pltpu.VMEM((tokens, key_cols), bf16),
            pltpu.VMEM((2, rows, query_cols), f32),
            pltpu.VMEM((2, rows, key_cols), f32),
            pltpu.VMEM((height, query_cols), f32),
            pltpu.VMEM((height, key_cols), f32),
            pltpu.VMEM((height, query_cols), bf16),
            pltpu.VMEM((height, key_cols), bf16),
            pltpu.VMEM((2, rank, tokens), bf16),
            pltpu.VMEM((per * rep, rank, LANES), bf16),
            pltpu.VMEM((rep, per, rank, LANES), bf16),
            pltpu.VMEM((per, rank, LANES), bf16),
            pltpu.VMEM((fs, per, rows, LANES), bf16),
            pltpu.VMEM((per * rep, rows, LANES), bf16),
            pltpu.VMEM((fs, 2, 8, LANES), f32),
            pltpu.VMEM((2, 2, 8, LANES), f32),
            dma((fs,)),
            dma((fs,)),
            dma((fs, rep)),
            dma((fs, rep)),
            dma((2, fs)),
            dma((2, fs)),
            dma((2, fs, rep)),
            dma((2, fs, rep)),
            dma((rep,)),
            dma((rep,)),
            dma((fs,)),
            dma((fs,)),
            dma((rep,)),
            dma((rep,)),
            dma((2, fs)),
            dma((2, fs)),
            dma((2, fs)),
            dma((fs,)),
            dma((fs,)),
            dma((3,)),
            dma((3,)),
            dma((10,)),
        ]
    (
        basis_all,
        weight_query_all,
        weight_key_all,
        dir_query,
        dir_key,
        low_query,
        low_key,
        totals,
    ) = pl.pallas_call(
        functools.partial(kernel, fs, rep),
        out_shape=out_shape,
        in_specs=[pl.BlockSpec(memory_space=pltpu.HBM)] * 9,
        out_specs=out_specs,
        scratch_shapes=scratch,
        compiler_params=pltpu.CompilerParams(
            collective_id=0, has_side_effects=True, vmem_limit_bytes=32 * 1024 * 1024
        ),
    )(
        *(
            pltpu.with_memory_space_constraint(operand, pltpu.HBM)
            for operand in (
                inputs,
                cot_query,
                cot_key,
                basis_query,
                basis_key,
                weight_query,
                weight_key,
                moments_query,
                moments_key,
            )
        )
    )

    steps = min(8, height // 16)
    tall, short = height * fs // steps, height // steps

    def fixed(*dims):
        return pl.BlockSpec(dims, lambda i: (0,) * len(dims))

    def banded(*dims):
        return pl.BlockSpec(dims, lambda i: (i, 0))

    owned = tuple(
        shape((height, columns), f32) for columns in (query_cols, key_cols, query_cols, key_cols)
    )
    owned_specs = tuple(
        banded(short, columns) for columns in (query_cols, key_cols, query_cols, key_cols)
    )
    return pl.pallas_call(
        functools.partial(
            apply, float(rank * query_cols * tp), float(rank * key_cols * tp)
        ),
        grid=(steps,),
        out_shape=owned
        + (
            shape((height * fs, query_cols), bf16),
            shape((height * fs, key_cols), bf16),
            shape((2, rows, query_cols), f32),
            shape((2, rows, key_cols), f32),
        ),
        in_specs=[
            fixed(2, 8, LANES),
            fixed(rank, query_cols),
            fixed(rank, key_cols),
            fixed(rows, query_cols),
            fixed(rows, key_cols),
            fixed(2, rows, query_cols),
            fixed(2, rows, key_cols),
            pl.BlockSpec((2, tall, rank), lambda i: (0, i, 0)),
            banded(tall, query_cols),
            banded(tall, key_cols),
            banded(short, rank),
            banded(short, rank),
            banded(short, query_cols),
            banded(short, key_cols),
        ],
        out_specs=owned_specs
        + (
            banded(tall, query_cols),
            banded(tall, key_cols),
            fixed(2, rows, query_cols),
            fixed(2, rows, key_cols),
        ),
        compiler_params=pltpu.CompilerParams(
            dimension_semantics=("arbitrary",), vmem_limit_bytes=32 * 1024 * 1024
        ),
    )(
        totals,
        dir_query,
        dir_key,
        low_query,
        low_key,
        moments_query,
        moments_key,
        basis_all,
        weight_query_all,
        weight_key_all,
        basis_query,
        basis_key,
        weight_query,
        weight_key,
    )


def solution(mesh):
    in_specs = (
        P(("fs", "rep"), None),
        P(("fs", "rep"), "tp"),
        P(("fs", "rep"), "tp"),
        P("fs", None),
        P("fs", None),
        P("fs", "tp"),
        P("fs", "tp"),
        P(None, "fs", "tp"),
        P(None, "fs", "tp"),
    )
    out_specs = (
        P("fs", "tp"),
        P("fs", "tp"),
        P("fs", "tp"),
        P("fs", "tp"),
        P(None, "tp"),
        P(None, "tp"),
        P(None, "fs", "tp"),
        P(None, "fs", "tp"),
    )
    return jax.shard_map(
        on_device, mesh=mesh, in_specs=in_specs, out_specs=out_specs, check_vma=False
    )
```

```python
import functools
import jax
import jax.numpy as jnp
from jax import lax
from jax.experimental import pallas as pl
from jax.experimental.pallas import tpu as pltpu
from jax.sharding import PartitionSpec as P

MESH = pl.DeviceIdType.MESH
LANES = 128


def each(start, stop, body):
    if stop - start <= 4:
        for i in range(start, stop):
            body(i)
    else:
        lax.fori_loop(start, stop, lambda i, carry: (body(i), carry)[1], 0)


def remote(src, dst, send_sem, recv_sem, **device):
    return pltpu.make_async_remote_copy(
        src_ref=src,
        dst_ref=dst,
        send_sem=send_sem,
        recv_sem=recv_sem,
        device_id=device,
        device_id_type=MESH,
    )


def exchange(
    fs,
    rep,
    inputs_far,
    cot_query_far,
    cot_key_far,
    basis_query,
    basis_key,
    full_query,
    full_key,
    moments_query_far,
    moments_key_far,
    basis_all,
    weight_query_all,
    weight_key_all,
    dir_query,
    dir_key,
    low_query,
    low_key,
    totals,
    inputs,
    cot_query,
    cot_key,
    moments_query,
    moments_key,
    loaded_query,
    loaded_key,
    wide_query,
    wide_key,
    factor,
    part_send,
    part_recv,
    slab,
    slab_recv,
    low_all,
    squares,
    pair,
    az_s,
    az_r,
    ap_s,
    ap_r,
    ez_s,
    ez_r,
    ep_s,
    ep_r,
    bp_s,
    bp_r,
    bz_s,
    bz_r,
    lp_s,
    lp_r,
    dr_s,
    dl_s,
    dz_r,
    qz_s,
    qz_r,
    pair_s,
    pair_r,
    local,
):
    f, r, c = lax.axis_index("fs"), lax.axis_index("rep"), lax.axis_index("tp")
    height = basis_query.shape[0]
    part = height // rep
    rank = basis_query.shape[1]
    rows = rank // fs
    tokens = inputs.shape[0]
    per = part_send.shape[0] // rep
    query_units = cot_query.shape[1] // LANES
    units = query_units + cot_key.shape[1] // LANES

    def ahead(i):
        return lax.rem(f + i, fs)

    def behind(i):
        return lax.rem(f + fs - i, fs)

    def beside(j):
        return lax.rem(r + j, rep)

    near = r + 1 - 2 * lax.rem(r, 2)
    far = r + 2 - 4 * (r // 2)
    across = 3 - r
    owners = (r, r, near, far)
    targets = (near, far, far, near)
    senders = (near, far, across, across)

    def span_of(slot, width):
        return (pl.ds(0, width), pl.ds(0, width), pl.ds(0, width // 2), pl.ds(width // 2, width // 2))[slot]

    def piece(source, owner):
        return pl.ds(pl.multiple_of(source * height + owner * part, part), part)

    own_part = pl.ds(pl.multiple_of(r * part, part), part)
    own_block = pl.ds(pl.multiple_of(f * height, height), height)

    def low_rows(source):
        return pl.ds(pl.multiple_of(source * rows, rows), rows)

    loads = [
        pltpu.make_async_copy(source, target, local.at[3 + n])
        for n, (source, target) in enumerate(
            (
                (full_query, loaded_query),
                (full_key, loaded_key),
                (inputs_far, inputs),
                (cot_query_far, cot_query),
                (cot_key_far, cot_key),
                (moments_query_far, moments_query),
                (moments_key_far, moments_key),
            )
        )
    ]
    barrier = pltpu.get_barrier_semaphore()

    def greet_fs(i):
        pl.semaphore_signal(barrier, inc=1, device_id={"fs": ahead(i)}, device_id_type=MESH)

    def greet_rep(j):
        pl.semaphore_signal(barrier, inc=1, device_id={"rep": beside(j)}, device_id_type=MESH)

    each(1, fs, greet_fs)
    each(1, rep, greet_rep)
    pl.semaphore_signal(barrier, inc=1, device_id={"tp": 1 - c}, device_id_type=MESH)
    pl.semaphore_wait(barrier, fs + rep - 1)

    bases = (basis_query, basis_key)
    weights = ((wide_query, weight_query_all), (wide_key, weight_key_all))

    def basis_fs(x, source, target):
        return remote(
            bases[x].at[own_part],
            basis_all.at[c, piece(source, r)],
            az_s.at[target],
            az_r.at[source],
            fs=target,
        )

    for x in range(2):

        @pl.when(c == x)
        def start_basis():
            each(1, fs, lambda i: basis_fs(x, f, ahead(i)).start())
            pltpu.make_async_copy(bases[x], basis_all.at[c, own_block], local.at[0]).start()

    for load in loads:
        load.start()
    own_basis = pltpu.make_async_copy(basis_query, basis_all.at[c, own_block], local.at[0])

    def basis_hop(source, slot, owner):
        block = basis_all.at[c, piece(source, owner), span_of(slot, rank)]
        return remote(
            block, block, ap_s.at[source, slot], ap_r.at[source, slot], rep=targets[slot]
        )

    def weight_fs(x, source, target):
        return remote(
            weights[x][0].at[own_part],
            weights[x][1].at[piece(source, r)],
            ez_s.at[x, target],
            ez_r.at[x, source],
            fs=target,
        )

    def weight_hop(x, source, slot, owner):
        block = weights[x][1].at[piece(source, owner), span_of(slot, weights[x][1].shape[1])]
        return remote(
            block, block, ep_s.at[x, source, slot], ep_r.at[x, source, slot], rep=targets[slot]
        )

    for load in loads[:2]:
        load.wait()
    wide_query[...] = loaded_query[...].astype(jnp.bfloat16)
    wide_key[...] = loaded_key[...].astype(jnp.bfloat16)

    def spread_basis(i):
        source = behind(i)
        basis_fs(0, source, source).wait_recv()
        for slot in (0, 1):
            basis_hop(source, slot, owners[slot]).start()

    each(1, fs, spread_basis)

    own_copies = [
        pltpu.make_async_copy(wide_query, weight_query_all.at[own_block], local.at[1]),
        pltpu.make_async_copy(wide_key, weight_key_all.at[own_block], local.at[2]),
    ]
    for copy in own_copies:
        copy.start()

    def start_weight(i):
        weight_fs(0, f, ahead(i)).start()
        weight_fs(1, f, ahead(i)).start()

    each(1, fs, start_weight)

    def relay_basis(i):
        source = behind(i)
        for slot in (0, 1):
            basis_hop(source, slot, senders[slot]).wait_recv()
            basis_hop(source, slot + 2, owners[slot + 2]).start()

    def all_basis(i):
        for slot in (2, 3):
            basis_hop(behind(i), slot, senders[slot]).wait_recv()

    each(1, fs, relay_basis)
    each(1, fs, all_basis)
    own_basis.wait()
    for load in loads[2:]:
        load.wait()

    for t in range(0, tokens, LANES):
        value = jnp.dot(
            inputs[t : t + LANES, :], basis_all[c], preferred_element_type=jnp.float32
        )
        factor[c, :, t : t + LANES] = value.T.astype(jnp.bfloat16)
    for u in range(units, per * rep):
        part_send[u] = jnp.zeros(part_send.shape[1:], jnp.bfloat16)
    factor_copy = remote(
        factor.at[c], factor.at[c], pair_s.at[0], pair_r.at[0], tp=1 - c
    )
    factor_back = remote(
        factor.at[1 - c], factor.at[1 - c], pair_s.at[0], pair_r.at[0], tp=1 - c
    )
    factor_copy.start()
    swap = remote(basis_all.at[c], basis_all.at[c], pair_s.at[1], pair_r.at[1], tp=1 - c)
    swap_back = remote(
        basis_all.at[1 - c], basis_all.at[1 - c], pair_s.at[1], pair_r.at[1], tp=1 - c
    )
    factor_back.wait_recv()
    swap.start()

    for x, cot in ((0, cot_query), (1, cot_key)):
        columns = cot.shape[1]
        width = 2 * LANES if columns % (2 * LANES) == 0 else LANES
        for n in range(0, columns, width):
            value = jnp.dot(
                factor[x], cot[:, n : n + width], preferred_element_type=jnp.float32
            ).astype(jnp.bfloat16)
            for k in range(0, width, LANES):
                part_send[x * query_units + (n + k) // LANES] = value[:, k : k + LANES]

    def group(owner):
        return pl.ds(owner * per, per)

    def part_rep(source, target):
        return remote(
            part_send.at[group(target)],
            part_recv.at[source],
            bp_s.at[target],
            bp_r.at[source],
            rep=target,
        )

    each(1, rep, lambda j: part_rep(r, beside(j)).start())
    part_recv[r] = part_send[group(r)]
    each(1, rep, lambda j: part_rep(beside(j), beside(j)).wait_recv())
    for p in range(per):
        value = part_recv[0, p].astype(jnp.float32)
        for q in range(1, rep):
            value = value + part_recv[q, p].astype(jnp.float32)
        slab[p] = value.astype(jnp.bfloat16)

    def slab_fs(source, target):
        return remote(
            slab.at[:, low_rows(target)],
            slab_recv.at[source],
            bz_s.at[target],
            bz_r.at[source],
            fs=target,
        )

    each(1, fs, lambda i: slab_fs(f, ahead(i)).start())

    def spread_weight(i):
        source = behind(i)
        for x in range(2):
            weight_fs(x, source, source).wait_recv()
            for slot in (0, 1):
                weight_hop(x, source, slot, owners[slot]).start()

    def relay_weight(i):
        source = behind(i)
        for slot in (0, 1):
            for x in range(2):
                weight_hop(x, source, slot, senders[slot]).wait_recv()
                weight_hop(x, source, slot + 2, owners[slot + 2]).start()

    spread_weight(1)
    slab_recv[f] = slab[:, low_rows(f), :]
    each(1, fs, lambda i: slab_fs(behind(i), behind(i)).wait_recv())
    for p in range(per):
        value = slab_recv[0, p].astype(jnp.float32)
        for q in range(1, fs):
            value = value + slab_recv[q, p].astype(jnp.float32)
        low_all[r * per + p] = value.astype(jnp.bfloat16)

    def low_rep(owner, target):
        block = low_all.at[group(owner)]
        return remote(block, block, lp_s.at[target], lp_r.at[owner], rep=target)

    each(1, rep, lambda j: low_rep(r, beside(j)).start())
    each(1, rep, lambda j: low_rep(beside(j), beside(j)).wait_recv())

    for x, moments, direction, low_out in (
        (0, moments_query, dir_query, low_query),
        (1, moments_key, dir_key, low_key),
    ):
        total = jnp.zeros((8, LANES), jnp.float32)
        for n in range(0, moments.shape[2], LANES):
            span = slice(n, n + LANES)
            low = low_all[x * query_units + n // LANES].astype(jnp.float32)
            low_out[:, span] = low
            first = 0.9 * moments[0, :, span] + 0.1 * low
            second = 0.95 * moments[1, :, span] + 0.05 * low * low
            normed = first / (jnp.sqrt(second) + 1e-08)
            direction[low_rows(f), span] = normed.astype(jnp.bfloat16)
            total = total + jnp.sum((normed * normed).reshape(rows // 8, 8, LANES), axis=0)
        squares[f, x] = total

    directions = (dir_query, dir_key)

    right, left = ahead(1), behind(1)

    def move_right(x, source):
        block = directions[x].at[low_rows(source)]
        return remote(block, block, dr_s.at[x, source], dz_r.at[x, source], fs=right)

    def move_left(x, source):
        block = directions[x].at[low_rows(source)]
        return remote(block, block, dl_s.at[x, source], dz_r.at[x, source], fs=left)

    def squares_fs(source, target):
        block = squares.at[source]
        return remote(block, block, qz_s.at[target], qz_r.at[source], fs=target)

    each(1, fs, lambda i: squares_fs(f, ahead(i)).start())

    @pl.when(f + 1 < fs)
    def start_right():
        for x in range(2):
            move_right(x, f).start()

    @pl.when(f > 0)
    def start_left():
        for x in range(2):
            move_left(x, f).start()

    each(2, fs, spread_weight)

    def relay_direction(k):
        @pl.when(f - k >= 0)
        def from_left():
            for x in range(2):
                move_right(x, f - k).wait_recv()

                @pl.when(f + 1 < fs)
                def onward():
                    move_right(x, f - k).start()

        @pl.when(f + k < fs)
        def from_right():
            for x in range(2):
                move_left(x, f + k).wait_recv()

                @pl.when(f > 0)
                def onward():
                    move_left(x, f + k).start()

    def relay_both(k):
        relay_weight(k)
        relay_direction(k)

    each(1, fs, relay_both)

    each(1, fs, lambda i: squares_fs(behind(i), behind(i)).wait_recv())
    total = squares[0]
    for q in range(1, fs):
        total = total + squares[q]
    pair[c] = total
    total_copy = remote(pair.at[c], pair.at[c], pair_s.at[2], pair_r.at[2], tp=1 - c)
    total_back = remote(pair.at[1 - c], pair.at[1 - c], pair_s.at[2], pair_r.at[2], tp=1 - c)
    total_copy.start()
    total_back.wait_recv()
    totals[...] = pair[0] + pair[1]

    def end_fs(i):
        source, target = behind(i), ahead(i)
        for x in range(2):
            for slot in (2, 3):
                weight_hop(x, source, slot, senders[slot]).wait_recv()
            for slot in range(4):
                weight_hop(x, source, slot, owners[slot]).wait_send()
            weight_fs(x, f, target).wait_send()
        for slot in range(4):
            basis_hop(source, slot, owners[slot]).wait_send()
        basis_fs(0, f, target).wait_send()
        slab_fs(f, target).wait_send()
        squares_fs(f, target).wait_send()

    def end_direction(k):
        @pl.when((f - k >= 0) & (f + 1 < fs))
        def end_right():
            for x in range(2):
                move_right(x, f - k).wait_send()

        @pl.when((f + k < fs) & (f > 0))
        def end_left():
            for x in range(2):
                move_left(x, f + k).wait_send()

    def end_rep(j):
        part_rep(r, beside(j)).wait_send()
        low_rep(r, beside(j)).wait_send()

    each(1, fs, end_fs)
    each(0, fs, end_direction)
    each(1, rep, end_rep)
    swap_back.wait_recv()
    factor_copy.wait_send()
    swap.wait_send()
    total_copy.wait_send()
    for copy in own_copies:
        copy.wait()


def exchange_grid(
    fs,
    rep,
    inputs_far,
    cot_query_far,
    cot_key_far,
    basis_query,
    basis_key,
    full_query,
    full_key,
    moments_query_far,
    moments_key_far,
    step_query,
    step_key,
    new_weight_query,
    new_weight_key,
    copy_query,
    copy_key,
    new_moments_query,
    new_moments_key,
    basis_all,
    weight_query_all,
    weight_key_all,
    dir_query,
    dir_key,
    inputs,
    cot_query,
    cot_key,
    moments_query,
    moments_key,
    loaded_query,
    loaded_key,
    factor,
    part,
    got_first,
    pair_sum,
    got_second,
    slab,
    slab_recv,
    low_all,
    part_squares,
    squares,
    pair,
    line_s,
    key_s,
    basis_line_r,
    query_line_r,
    key_line_r,
    hop_s,
    basis_hop_r,
    query_hop_r,
    basis_end_r,
    query_end_r,
    halve_s,
    first_r,
    second_r,
    slab_s,
    slab_r,
    low_s,
    low_r,
    low_end_r,
    dir_s,
    dir_r,
    dir_hop_s,
    dir_hop_r,
    dir_end_r,
    squares_s,
    squares_r,
    pair_s,
    pair_r,
    local,
):
    f, r, c = lax.axis_index("fs"), lax.axis_index("rep"), lax.axis_index("tp")
    height, rank = basis_query.shape
    quarter = height // rep
    rows = rank // fs
    own = rows // rep
    tokens = inputs.shape[0]
    query_units = cot_query.shape[1] // LANES
    units = query_units + cot_key.shape[1] // LANES
    streams = ((0, units // 2), (units // 2, units // 2))
    f32, bf16 = jnp.float32, jnp.bfloat16

    near = r + 1 - 2 * lax.rem(r, 2)
    far = r + 2 - 4 * (r // 2)
    across = 3 - r

    def when(conds, body):
        if not conds:
            body()
            return
        test = conds[0]
        for cond in conds[1:]:
            test = test & cond
        pl.when(test)(body)

    def send(make, *conds):
        when(conds, lambda: make().start())

    def arrived(block, sem, *conds):
        when(conds, lambda: remote(block, block, sem, sem, tp=1 - c).wait_recv())

    def departed(block, sem, *conds):
        when(conds, lambda: remote(block, block, sem, sem, tp=1 - c).wait_send())

    def sources(d):
        return ((f - d, f >= d), (f + d, f + d < fs))

    def beside(j):
        return lax.rem(r + j, rep)

    def rows_of(start, size):
        return pl.ds(pl.multiple_of(start, size), size)

    chunks = 2
    chunk = quarter // chunks

    def piece(source, owner, k):
        return rows_of(source * height + owner * quarter + k * chunk, chunk)

    mirror = f // (fs // 2)
    place_in_half = f + mirror * (fs - 1 - 2 * f)

    def other(n):
        low_side = n - 1 + (n + fs - 1 - place_in_half) // fs
        return low_side + mirror * (fs - 1 - 2 * low_side)

    own_block = rows_of(f * height, height)

    loads = [
        pltpu.make_async_copy(source, target, local.at[1 + n])
        for n, (source, target) in enumerate(
            (
                (full_query, loaded_query),
                (full_key, loaded_key),
                (inputs_far, inputs),
                (cot_query_far, cot_query),
                (cot_key_far, cot_key),
                (moments_query_far, moments_query),
                (moments_key_far, moments_key),
            )
        )
    ]
    barrier = pltpu.get_barrier_semaphore()
    for i in range(1, fs):
        pl.semaphore_signal(
            barrier, inc=1, device_id={"fs": lax.rem(f + i, fs)}, device_id_type=MESH
        )
    for mate in (near, far):
        pl.semaphore_signal(barrier, inc=1, device_id={"rep": mate}, device_id_type=MESH)
    pl.semaphore_signal(barrier, inc=1, device_id={"tp": 1 - c}, device_id_type=MESH)
    pl.semaphore_wait(barrier, fs + 2)

    bases = (basis_query, basis_key)

    def basis_z(source, up, k):
        block = basis_all.at[c, piece(source, r, k)]
        return remote(block, block, line_s.at[0], basis_line_r.at[source, k], fs=f + 2 * up - 1)

    def basis_start(x, up, k):
        return remote(
            bases[x].at[rows_of(r * quarter + k * chunk, chunk)],
            basis_all.at[c, piece(f, r, k)],
            line_s.at[0],
            basis_line_r.at[f, k],
            fs=f + 2 * up - 1,
        )

    ways = ((1, f + 1 < fs), (0, f > 0))
    for x in range(2):

        @pl.when(c == x)
        def start_basis():
            for k in range(chunks):
                for up, there in ways:
                    pl.when(there)(lambda: basis_start(x, up, k).start())
            pltpu.make_async_copy(bases[x], basis_all.at[c, own_block], local.at[0]).start()

    for load in loads:
        load.start()
    own_basis = pltpu.make_async_copy(basis_query, basis_all.at[c, own_block], local.at[0])

    def hop_span(slot, width):
        return (pl.ds(0, width), pl.ds(0, width), pl.ds(0, width // 2), pl.ds(width // 2, width // 2))[slot]

    targets = (near, far, far, near)
    sent = (r, r, near, far)

    def basis_hop(k, source, slot):
        block = basis_all.at[c, piece(source, sent[slot], k), hop_span(slot, rank)]
        landed = basis_hop_r.at[source, k] if slot < 2 else basis_end_r.at[0]
        return remote(block, block, hop_s.at[0], landed, rep=targets[slot])

    def weight_hop(k, source, slot):
        width = weight_query_all.shape[1]
        block = weight_query_all.at[piece(source, sent[slot], k), hop_span(slot, width)]
        landed = query_hop_r.at[source, k] if slot < 2 else query_end_r.at[source]
        return remote(block, block, hop_s.at[1], landed, rep=targets[slot])

    def spread(hop, source, *there):
        for slot in (0, 1):
            send(functools.partial(hop, source, slot), *there)

    def relay(hop, both, sem, source, *there):
        arrived(both, sem, *there)
        for slot in (2, 3):
            send(functools.partial(hop, source, slot), *there)

    def relay_basis(k, source, *there):
        both = basis_all.at[c, pl.ds(0, 2 * chunk)]
        relay(functools.partial(basis_hop, k), both, basis_hop_r.at[source, k], source, *there)

    def relay_weight(k, source):
        both = weight_query_all.at[pl.ds(0, 2 * chunk)]
        relay(functools.partial(weight_hop, k), both, query_hop_r.at[source, k], source)

    def query_z(source, up, k):
        block = weight_query_all.at[piece(source, r, k)]
        return remote(block, block, line_s.at[1], query_line_r.at[source, k], fs=f + 2 * up - 1)

    def key_z(source, up, k):
        block = weight_key_all.at[rows_of(source * height, height)]
        return remote(block, block, key_s.at[up], key_line_r.at[source], fs=f + 2 * up - 1)

    def launch(line, parts=chunks):
        for k in range(parts):
            for up, there in ways:
                send(functools.partial(line, f, up, k), there)

    def onward(line, d, k):
        below, above = f - d, f + d
        when((f >= d,), lambda: line(below, 1, k).wait_recv())
        if d + 1 < fs:
            send(functools.partial(line, below, 1, k), f >= d, f + 1 < fs)
        when((f + d < fs,), lambda: line(above, 0, k).wait_recv())
        if d + 1 < fs:
            send(functools.partial(line, above, 0, k), f + d < fs, f > 0)

    def onward_all(line, d, parts=chunks):
        for k in range(parts):
            onward(line, d, k)

    for load in loads[:2]:
        load.wait()
    weight_query_all[own_block, :] = loaded_query[...].astype(bf16)
    weight_key_all[own_block, :] = loaded_key[...].astype(bf16)

    steps = [(d, k) for d in range(1, fs) for k in range(chunks)]
    for n, (d, k) in enumerate(steps):
        onward(basis_z, d, k)
        for source, there in sources(d):
            spread(functools.partial(basis_hop, k), source, there)
        if (d, k) == (max(fs - 2, 1), chunks - 1):
            launch(query_z)
            launch(key_z, 1)
        if n >= chunks:
            before, j = steps[n - chunks]
            for source, there in sources(before):
                relay_basis(j, source, there)
    for d, k in steps[-chunks:]:
        for source, there in sources(d):
            relay_basis(k, source, there)
    onward_all(query_z, 1)
    spread(functools.partial(weight_hop, 0), other(1))
    arrived(basis_all.at[c, pl.ds(0, (fs - 1) * quarter)], basis_end_r.at[0])
    own_basis.wait()
    for load in loads[2:]:
        load.wait()

    for t in range(0, tokens, LANES):
        value = jnp.dot(inputs[t : t + LANES, :], basis_all[c], preferred_element_type=f32)
        factor[c, :, t : t + LANES] = value.T.astype(bf16)

    def partner(block, back, n):
        return (
            remote(block, block, pair_s.at[n], pair_r.at[n], tp=1 - c),
            remote(back, back, pair_s.at[n], pair_r.at[n], tp=1 - c),
        )

    factor_copy, factor_back = partner(factor.at[c], factor.at[1 - c], 0)
    swap, swap_back = partner(basis_all.at[c], basis_all.at[1 - c], 1)
    factor_copy.start()
    factor_back.wait_recv()
    swap.start()

    for x, cot in ((0, cot_query), (1, cot_key)):
        columns = cot.shape[1]
        width = 2 * LANES if columns % (2 * LANES) == 0 else LANES
        for n in range(0, columns, width):
            value = jnp.dot(
                factor[x], cot[:, n : n + width], preferred_element_type=f32
            ).astype(bf16)
            for k in range(0, width, LANES):
                for q in range(rep):
                    for s in range(fs):
                        part[x * query_units + (n + k) // LANES, q, s * own : (s + 1) * own] = value[
                            s * rows + q * own : s * rows + (q + 1) * own, k : k + LANES
                        ]

    half = rows // 2
    spans = (slice(0, half), slice(half, rows))
    mates = ((near, far), (far, near))

    def columns_of(g):
        return pl.ds(streams[g][0], streams[g][1])

    def first_hop(h, g, w):
        owner = (across, mates[h][0])[w]
        return remote(
            part.at[columns_of(g), owner, pl.ds(h * half, half)],
            got_first.at[h, w, columns_of(g)],
            halve_s.at[0],
            (first_r, second_r)[w].at[g],
            rep=mates[h][0],
        )

    def second_hop(h, g):
        return remote(
            pair_sum.at[h, columns_of(g)],
            got_second.at[h, columns_of(g)],
            halve_s.at[1],
            second_r.at[g],
            rep=mates[h][1],
        )

    def start_first(g, w):
        for h in range(2):
            first_hop(h, g, w).start()

    def start_second(g):
        arrived(got_first.at[:, 0, columns_of(g)], first_r.at[g])
        for h in range(2):
            for u in range(streams[g][0], sum(streams[g])):
                pair_sum[h, u] = (
                    part[u, mates[h][1], spans[h]].astype(f32) + got_first[h, 0, u].astype(f32)
                ).astype(bf16)
            second_hop(h, g).start()

    def slab_z(g, source, target):
        return remote(
            slab.at[columns_of(g), rows_of(target * own, own)],
            slab_recv.at[source, columns_of(g)],
            slab_s.at[0],
            slab_r.at[g],
            fs=target,
        )

    def end_rep(g):
        arrived(got_first.at[:, :, columns_of(g)], second_r.at[g])
        for h in range(2):
            for u in range(streams[g][0], sum(streams[g])):
                slab[u, spans[h]] = (
                    part[u, r, spans[h]].astype(f32)
                    + got_first[h, 1, u].astype(f32)
                    + got_second[h, u].astype(f32)
                ).astype(bf16)
        for n in range(fs - 1, 0, -1):
            slab_z(g, f, other(n)).start()
        for u in range(streams[g][0], sum(streams[g])):
            slab_recv[f, u] = slab[u, rows_of(f * own, own)]

    start_first(0, 0)
    start_first(0, 1)
    start_first(1, 0)
    start_second(0)
    start_first(1, 1)
    start_second(1)
    for k in range(1, chunks):
        spread(functools.partial(weight_hop, k), other(1))
    end_rep(0)
    end_rep(1)
    onward_all(query_z, 2)
    for k in range(chunks):
        spread(functools.partial(weight_hop, k), other(2))

    directions, new_moments = (dir_query, dir_key), (new_moments_query, new_moments_key)
    moments = (moments_query, moments_key)

    def place(u):
        x = 0 if u < query_units else 1
        n = (u - x * query_units) * LANES
        return x, slice(n, n + LANES)

    def pieces(g):
        first, last = streams[g][0], sum(streams[g])
        found = []
        if first < query_units:
            found.append((0, first * LANES, (min(last, query_units) - first) * LANES))
        if last > query_units:
            start = max(first, query_units)
            found.append((1, (start - query_units) * LANES, (last - start) * LANES))
        return found

    def dir_rows(source, owner):
        return rows_of(source * rows + owner * own, own)

    def update(g, owner):
        sums = [jnp.zeros((8, LANES), f32), jnp.zeros((8, LANES), f32)]
        mine = rows_of(owner * own, own)
        for u in range(streams[g][0], sum(streams[g])):
            x, span = place(u)
            low = low_all[owner, u].astype(f32)
            first = 0.9 * moments[x][0, mine, span] + 0.1 * low
            second = 0.95 * moments[x][1, mine, span] + 0.05 * low * low
            new_moments[x][0, mine, span] = first
            new_moments[x][1, mine, span] = second
            normed = first / (jnp.sqrt(second) + 1e-08)
            directions[x][dir_rows(f, owner), span] = normed.astype(bf16)
            sums[x] = sums[x] + jnp.sum((normed * normed).reshape(own // 8, 8, LANES), axis=0)
        for x in range(2):
            part_squares[owner, g, x] = sums[x]

    def low_hop(g, slot):
        block = low_all.at[sent[slot], columns_of(g)]
        landed = low_r.at[g] if slot == g else low_end_r.at[0]
        return remote(block, block, low_s.at[0], landed, rep=targets[slot])

    def dir_blocks(g, source, owner):
        return [
            directions[x].at[dir_rows(source, owner), pl.ds(start, size)]
            for x, start, size in pieces(g)
        ]

    def dir_z(g, target):
        for block in dir_blocks(g, f, r):
            remote(block, block, dir_s.at[0], dir_r.at[g, f], fs=target).start()

    def dir_hop(g, slot, n):
        landed = dir_hop_r.at[n, g] if slot == g else dir_end_r.at[n]
        for block in dir_blocks(g, other(n), sent[slot]):
            remote(block, block, dir_hop_s.at[n], landed, rep=targets[slot]).start()

    def end_fs(g):
        arrived(slab_recv.at[pl.ds(0, fs - 1), columns_of(g)], slab_r.at[g])
        for u in range(streams[g][0], sum(streams[g])):
            value = slab_recv[0, u].astype(f32)
            for q in range(1, fs):
                value = value + slab_recv[q, u].astype(f32)
            low_all[r, u] = value.astype(bf16)
        for slot in (0, 1):
            low_hop(g, slot).start()
        update(g, r)
        for n in range(fs - 1, 0, -1):
            dir_z(g, other(n))

    end_fs(0)
    end_fs(1)

    def spread_dir(g, n):
        arrived(low_all.at[r, columns_of(g)], dir_r.at[g, other(n)])
        for slot in (0, 1):
            dir_hop(g, slot, n)

    def relay_dir(n):
        for g in range(2):
            arrived(low_all.at[r, columns_of(g)], dir_hop_r.at[n, g])
            dir_hop(g, g + 2, n)

    def finish_dir(n):
        arrived(low_all.at[pl.ds(0, 2)], dir_end_r.at[n])

    onward_all(key_z, 1, 1)
    for k in range(chunks):
        relay_weight(k, other(1))
    for g in range(2):
        arrived(low_all.at[r, columns_of(g)], low_r.at[g])
        low_hop(g, g + 2).start()
    spread_dir(0, 1)
    spread_dir(1, 1)
    for d in range(2, fs):
        spread_dir(0, d)
        spread_dir(1, d)
        relay_dir(d - 1)
    relay_dir(fs - 1)
    for k in range(chunks):
        relay_weight(k, other(2))
    for n in range(3, fs):
        for k in range(chunks):
            onward(query_z, n, k)
            spread(functools.partial(weight_hop, k), other(n))
    for d in range(2, fs - 1):
        onward_all(key_z, d, 1)
    arrived(low_all.at[pl.ds(0, 2)], low_end_r.at[0])
    for g in range(2):
        for j in range(1, rep):
            update(g, beside(j))
    for x in range(2):
        total = part_squares[0, 0, x] + part_squares[0, 1, x]
        for q in range(1, rep):
            total = total + (part_squares[q, 0, x] + part_squares[q, 1, x])
        squares[f, x] = total

    mine = squares.at[f]
    for n in range(1, fs):
        remote(mine, mine, squares_s.at[0], squares_r.at[0], fs=other(n)).start()
    arrived(squares.at[pl.ds(0, fs - 1)], squares_r.at[0])
    total = squares[0]
    for q in range(1, fs):
        total = total + squares[q]
    pair[c] = total
    total_copy, total_back = partner(pair.at[c], pair.at[1 - c], 2)
    total_copy.start()

    for d in range(1, fs):
        finish_dir(d)
    total_back.wait_recv()
    totals = pair[0] + pair[1]
    weights_all, copies = (weight_query_all, weight_key_all), (copy_query, copy_key)
    scales = [
        lax.rsqrt(jnp.sum(totals[x], keepdims=True) / (pair.shape[0] * rank * copies[x].shape[1]) + 1e-06)
        for x in range(2)
    ]

    def product(x, span, columns):
        return scales[x] * jnp.dot(
            basis_all[x, span], directions[x][:, columns], preferred_element_type=f32
        )

    def column_blocks(x):
        wide = copies[x].shape[1]
        width = 2 * LANES if wide % (2 * LANES) == 0 else LANES
        return [slice(n, n + width) for n in range(0, wide, width)]

    def copy_rows(x, start, size):
        span = rows_of(start, size)
        for columns in column_blocks(x):
            weight = weights_all[x][span, columns].astype(f32)
            copies[x][span, columns] = (weight - 0.02 * product(x, span, columns)).astype(bf16)

    swap_back.wait_recv()
    for x, weight, step_out, new_out in (
        (0, loaded_query, step_query, new_weight_query),
        (1, loaded_key, step_key, new_weight_key),
    ):
        for columns in column_blocks(x):
            step = product(x, own_block, columns)
            step_out[:, columns] = step
            new = weight[:, columns] - 0.02 * step
            new_out[:, columns] = new
            copies[x][own_block, columns] = new.astype(bf16)

    def relay_last(k):
        for n in range(3, fs):
            relay_weight(k, other(n))

    def finish_weight(n):
        arrived(weight_query_all.at[pl.ds(0, quarter)], query_end_r.at[other(n)])

    finish_weight(1)
    copy_rows(0, other(1) * height, height)
    relay_last(0)
    finish_weight(2)
    copy_rows(0, other(2) * height, height)
    relay_last(1)
    for n in (1, 2):
        copy_rows(1, other(n) * height, height)
    for n in range(3, fs):
        for owner in (r, near, far):
            copy_rows(0, other(n) * height + owner * quarter, quarter)
    for d in range(max(fs - 1, 3), fs):
        onward_all(key_z, d, 1)
    for n in range(3, fs):
        copy_rows(1, other(n) * height, height)
    for n in range(3, fs):
        finish_weight(n)
        copy_rows(0, other(n) * height + across * quarter, quarter)
    edge = (f == 0) | (f == fs - 1)
    hops = (fs - 1) * (rep - 1) * quarter
    for n, block in ((0, basis_all.at[c]), (1, weight_query_all)):
        departed(block.at[pl.ds(0, quarter)], line_s.at[n], edge)
        departed(block.at[pl.ds(0, (fs + 1) * quarter)], line_s.at[n], jnp.logical_not(edge))
        departed(block.at[pl.ds(0, hops)], hop_s.at[n])
    for n in range(fs):
        if n < fs - 1:
            departed(weight_key_all.at[pl.ds(0, (n + 1) * height)], key_s.at[1], f == n)
        if n > 0:
            departed(weight_key_all.at[pl.ds(0, (fs - n) * height)], key_s.at[0], f == n)
    departed(got_first, halve_s.at[0])
    departed(pair_sum, halve_s.at[1])
    departed(slab_recv.at[pl.ds(0, fs - 1)], slab_s.at[0])
    departed(low_all.at[pl.ds(0, rep - 1)], low_s.at[0])
    departed(slab_recv.at[pl.ds(0, fs - 1)], dir_s.at[0])
    for n in range(1, fs):
        departed(low_all.at[pl.ds(0, rep - 1)], dir_hop_s.at[n])
    departed(squares.at[pl.ds(0, fs - 1)], squares_s.at[0])
    for copy in (factor_copy, swap, total_copy):
        copy.wait_send()


def write_out(*refs):
    count = len(refs) // 2
    copies = [
        pltpu.make_async_copy(source, target, refs[-1].at[n])
        for n, (source, target) in enumerate(zip(refs[:count], refs[count : 2 * count]))
    ]
    for copy in copies:
        copy.start()
    for copy in copies:
        copy.wait()


def apply(
    count_query,
    count_key,
    totals,
    dir_query,
    dir_key,
    low_query,
    low_key,
    moments_query,
    moments_key,
    basis_all,
    weight_query_all,
    weight_key_all,
    basis_query,
    basis_key,
    weight_query,
    weight_key,
    step_query,
    step_key,
    new_weight_query,
    new_weight_key,
    copy_query,
    copy_key,
    new_moments_query,
    new_moments_key,
):
    parts = (
        (count_query, dir_query, weight_query_all, basis_query, weight_query),
        (count_key, dir_key, weight_key_all, basis_key, weight_key),
    )
    outs = (
        (step_query, new_weight_query, copy_query),
        (step_key, new_weight_key, copy_key),
    )
    for x in range(2):
        count, direction, weight_all, basis, weight = parts[x]
        step_out, new_weight_out, copy_out = outs[x]
        scale = lax.rsqrt(jnp.sum(totals[x], keepdims=True) / count + 1e-06)
        step = scale * jnp.dot(basis[...], direction[...], preferred_element_type=jnp.float32)
        step_out[...] = step
        new_weight_out[...] = weight[...] - 0.02 * step
        whole = scale * jnp.dot(
            basis_all[x], direction[...], preferred_element_type=jnp.float32
        )
        copy_out[...] = (weight_all[...].astype(jnp.float32) - 0.02 * whole).astype(jnp.bfloat16)

    @pl.when(pl.program_id(0) == 0)
    def moments_once():
        for moments, low_ref, out in (
            (moments_query, low_query, new_moments_query),
            (moments_key, low_key, new_moments_key),
        ):
            low = low_ref[...]
            out[0] = 0.9 * moments[0] + 0.1 * low
            out[1] = 0.95 * moments[1] + 0.05 * low * low


def on_device(
    inputs,
    cot_query,
    cot_key,
    basis_query,
    basis_key,
    weight_query,
    weight_key,
    moments_query,
    moments_key,
):
    fs, rep, tp = lax.axis_size("fs"), lax.axis_size("rep"), lax.axis_size("tp")
    assert tp == 2 and rep == 4
    height, rank = basis_query.shape
    rows = rank // fs
    tokens = inputs.shape[0]
    query_cols, key_cols = cot_query.shape[1], cot_key.shape[1]
    per = -(-((query_cols + key_cols) // LANES) // rep)
    vmem = pl.BlockSpec(memory_space=pltpu.VMEM)
    hbm = pl.BlockSpec(memory_space=pl.ANY)
    bf16, f32 = jnp.bfloat16, jnp.float32
    dma = pltpu.SemaphoreType.DMA
    shape = jax.ShapeDtypeStruct
    owned = tuple(
        shape((height, columns), f32) for columns in (query_cols, key_cols, query_cols, key_cols)
    )
    results = owned + (
        shape((height * fs, query_cols), bf16),
        shape((height * fs, key_cols), bf16),
        shape((2, rows, query_cols), f32),
        shape((2, rows, key_cols), f32),
    )
    own, units = rows // rep, (query_cols + key_cols) // LANES
    if own % 16 == 0 and fs % 2 == 0 and fs > 2 and units % 2 == 0:
        fresh = pl.pallas_call(
            functools.partial(exchange_grid, fs, rep),
            out_shape=results,
            in_specs=[pl.BlockSpec(memory_space=pltpu.HBM)] * 9,
            out_specs=(vmem,) * 8,
            scratch_shapes=[
                pltpu.VMEM((2, height * fs, rank), bf16),
                pltpu.VMEM((height * fs, query_cols), bf16),
                pltpu.VMEM((height * fs, key_cols), bf16),
                pltpu.VMEM((rank, query_cols), bf16),
                pltpu.VMEM((rank, key_cols), bf16),
                pltpu.VMEM((tokens, inputs.shape[1]), bf16),
                pltpu.VMEM((tokens, query_cols), bf16),
                pltpu.VMEM((tokens, key_cols), bf16),
                pltpu.VMEM((2, rows, query_cols), f32),
                pltpu.VMEM((2, rows, key_cols), f32),
                pltpu.VMEM((height, query_cols), f32),
                pltpu.VMEM((height, key_cols), f32),
                pltpu.VMEM((2, rank, tokens), bf16),
                pltpu.VMEM((units, rep, rows, LANES), bf16),
                pltpu.VMEM((2, 2, units, rows // 2, LANES), bf16),
                pltpu.VMEM((2, units, rows // 2, LANES), bf16),
                pltpu.VMEM((2, units, rows // 2, LANES), bf16),
                pltpu.VMEM((units, rows, LANES), bf16),
                pltpu.VMEM((fs, units, own, LANES), bf16),
                pltpu.VMEM((rep, units, own, LANES), bf16),
                pltpu.VMEM((rep, 2, 2, 8, LANES), f32),
                pltpu.VMEM((fs, 2, 8, LANES), f32),
                pltpu.VMEM((2, 2, 8, LANES), f32),
                dma((2,)),
                dma((2,)),
                dma((fs, 2)),
                dma((fs, 2)),
                dma((fs,)),
                dma((2,)),
                dma((fs, 2)),
                dma((fs, 2)),
                dma((1,)),
                dma((fs,)),
                dma((2,)),
                dma((2,)),
                dma((2,)),
                dma((1,)),
                dma((2,)),
                dma((1,)),
                dma((2,)),
                dma((1,)),
                dma((1,)),
                dma((2, fs)),
                dma((fs,)),
                dma((fs, 2)),
                dma((fs,)),
                dma((1,)),
                dma((1,)),
                dma((3,)),
                dma((3,)),
                dma((8,)),
            ],
            compiler_params=pltpu.CompilerParams(
                collective_id=0, has_side_effects=True, vmem_limit_bytes=40 * 1024 * 1024
            ),
        )(
            *(
                pltpu.with_memory_space_constraint(operand, pltpu.HBM)
                for operand in (
                    inputs,
                    cot_query,
                    cot_key,
                    basis_query,
                    basis_key,
                    weight_query,
                    weight_key,
                    moments_query,
                    moments_key,
                )
            )
        )
        return pl.pallas_call(
            write_out,
            out_shape=results,
            in_specs=[vmem] * 8,
            out_specs=(hbm,) * 8,
            scratch_shapes=[dma((8,))],
            compiler_params=pltpu.CompilerParams(vmem_limit_bytes=32 * 1024 * 1024),
        )(*fresh)

    (
        basis_all,
        weight_query_all,
        weight_key_all,
        dir_query,
        dir_key,
        low_query,
        low_key,
        totals,
    ) = pl.pallas_call(
        functools.partial(exchange, fs, rep),
        out_shape=(
            shape((2, height * fs, rank), bf16),
            shape((height * fs, query_cols), bf16),
            shape((height * fs, key_cols), bf16),
            shape((rank, query_cols), bf16),
            shape((rank, key_cols), bf16),
            shape((rows, query_cols), f32),
            shape((rows, key_cols), f32),
            shape((2, 8, LANES), f32),
        ),
        in_specs=[pl.BlockSpec(memory_space=pltpu.HBM)] * 9,
        out_specs=(vmem, hbm, hbm, vmem, vmem, vmem, vmem, vmem),
        scratch_shapes=[
            pltpu.VMEM((tokens, inputs.shape[1]), bf16),
            pltpu.VMEM((tokens, query_cols), bf16),
            pltpu.VMEM((tokens, key_cols), bf16),
            pltpu.VMEM((2, rows, query_cols), f32),
            pltpu.VMEM((2, rows, key_cols), f32),
            pltpu.VMEM((height, query_cols), f32),
            pltpu.VMEM((height, key_cols), f32),
            pltpu.VMEM((height, query_cols), bf16),
            pltpu.VMEM((height, key_cols), bf16),
            pltpu.VMEM((2, rank, tokens), bf16),
            pltpu.VMEM((per * rep, rank, LANES), bf16),
            pltpu.VMEM((rep, per, rank, LANES), bf16),
            pltpu.VMEM((per, rank, LANES), bf16),
            pltpu.VMEM((fs, per, rows, LANES), bf16),
            pltpu.VMEM((per * rep, rows, LANES), bf16),
            pltpu.VMEM((fs, 2, 8, LANES), f32),
            pltpu.VMEM((2, 2, 8, LANES), f32),
            dma((fs,)),
            dma((fs,)),
            dma((fs, rep)),
            dma((fs, rep)),
            dma((2, fs)),
            dma((2, fs)),
            dma((2, fs, rep)),
            dma((2, fs, rep)),
            dma((rep,)),
            dma((rep,)),
            dma((fs,)),
            dma((fs,)),
            dma((rep,)),
            dma((rep,)),
            dma((2, fs)),
            dma((2, fs)),
            dma((2, fs)),
            dma((fs,)),
            dma((fs,)),
            dma((3,)),
            dma((3,)),
            dma((10,)),
        ],
        compiler_params=pltpu.CompilerParams(
            collective_id=0, has_side_effects=True, vmem_limit_bytes=32 * 1024 * 1024
        ),
    )(
        *(
            pltpu.with_memory_space_constraint(operand, pltpu.HBM)
            for operand in (
                inputs,
                cot_query,
                cot_key,
                basis_query,
                basis_key,
                weight_query,
                weight_key,
                moments_query,
                moments_key,
            )
        )
    )

    steps = min(8, height // 16)
    tall, short = height * fs // steps, height // steps

    def fixed(*dims):
        return pl.BlockSpec(dims, lambda i: (0,) * len(dims))

    def banded(*dims):
        return pl.BlockSpec(dims, lambda i: (i, 0))

    owned_specs = tuple(
        banded(short, columns) for columns in (query_cols, key_cols, query_cols, key_cols)
    )
    return pl.pallas_call(
        functools.partial(
            apply, float(rank * query_cols * tp), float(rank * key_cols * tp)
        ),
        grid=(steps,),
        out_shape=results,
        in_specs=[
            fixed(2, 8, LANES),
            fixed(rank, query_cols),
            fixed(rank, key_cols),
            fixed(rows, query_cols),
            fixed(rows, key_cols),
            fixed(2, rows, query_cols),
            fixed(2, rows, key_cols),
            pl.BlockSpec((2, tall, rank), lambda i: (0, i, 0)),
            banded(tall, query_cols),
            banded(tall, key_cols),
            banded(short, rank),
            banded(short, rank),
            banded(short, query_cols),
            banded(short, key_cols),
        ],
        out_specs=owned_specs
        + (
            banded(tall, query_cols),
            banded(tall, key_cols),
            fixed(2, rows, query_cols),
            fixed(2, rows, key_cols),
        ),
        compiler_params=pltpu.CompilerParams(
            dimension_semantics=("arbitrary",), vmem_limit_bytes=32 * 1024 * 1024
        ),
    )(
        totals,
        dir_query,
        dir_key,
        low_query,
        low_key,
        moments_query,
        moments_key,
        basis_all,
        weight_query_all,
        weight_key_all,
        basis_query,
        basis_key,
        weight_query,
        weight_key,
    )


def solution(mesh):
    in_specs = (
        P(("fs", "rep"), None),
        P(("fs", "rep"), "tp"),
        P(("fs", "rep"), "tp"),
        P("fs", None),
        P("fs", None),
        P("fs", "tp"),
        P("fs", "tp"),
        P(None, "fs", "tp"),
        P(None, "fs", "tp"),
    )
    out_specs = (
        P("fs", "tp"),
        P("fs", "tp"),
        P("fs", "tp"),
        P("fs", "tp"),
        P(None, "tp"),
        P(None, "tp"),
        P(None, "fs", "tp"),
        P(None, "fs", "tp"),
    )
    return jax.shard_map(
        on_device, mesh=mesh, in_specs=in_specs, out_specs=out_specs, check_vma=False
    )
```

```python
import functools
import jax
import jax.numpy as jnp
from jax import lax
from jax.experimental import pallas as pl
from jax.experimental.pallas import tpu as pltpu
from jax.sharding import PartitionSpec as P

MESH = pl.DeviceIdType.MESH
LANES = 128


def each(start, stop, body):
    if stop - start <= 4:
        for i in range(start, stop):
            body(i)
    else:
        lax.fori_loop(start, stop, lambda i, carry: (body(i), carry)[1], 0)


def remote(src, dst, send_sem, recv_sem, **device):
    return pltpu.make_async_remote_copy(
        src_ref=src,
        dst_ref=dst,
        send_sem=send_sem,
        recv_sem=recv_sem,
        device_id=device,
        device_id_type=MESH,
    )


def exchange(
    fs,
    rep,
    inputs_far,
    cot_query_far,
    cot_key_far,
    basis_query,
    basis_key,
    full_query,
    full_key,
    moments_query_far,
    moments_key_far,
    basis_all,
    weight_query_all,
    weight_key_all,
    dir_query,
    dir_key,
    low_query,
    low_key,
    totals,
    inputs,
    cot_query,
    cot_key,
    moments_query,
    moments_key,
    loaded_query,
    loaded_key,
    wide_query,
    wide_key,
    factor,
    part_send,
    part_recv,
    slab,
    slab_recv,
    low_all,
    squares,
    pair,
    az_s,
    az_r,
    ap_s,
    ap_r,
    ez_s,
    ez_r,
    ep_s,
    ep_r,
    bp_s,
    bp_r,
    bz_s,
    bz_r,
    lp_s,
    lp_r,
    dr_s,
    dl_s,
    dz_r,
    qz_s,
    qz_r,
    pair_s,
    pair_r,
    local,
):
    f, r, c = lax.axis_index("fs"), lax.axis_index("rep"), lax.axis_index("tp")
    height = basis_query.shape[0]
    part = height // rep
    rank = basis_query.shape[1]
    rows = rank // fs
    tokens = inputs.shape[0]
    per = part_send.shape[0] // rep
    query_units = cot_query.shape[1] // LANES
    units = query_units + cot_key.shape[1] // LANES

    def ahead(i):
        return lax.rem(f + i, fs)

    def behind(i):
        return lax.rem(f + fs - i, fs)

    def beside(j):
        return lax.rem(r + j, rep)

    near = r + 1 - 2 * lax.rem(r, 2)
    far = r + 2 - 4 * (r // 2)
    across = 3 - r
    owners = (r, r, near, far)
    targets = (near, far, far, near)
    senders = (near, far, across, across)

    def span_of(slot, width):
        return (pl.ds(0, width), pl.ds(0, width), pl.ds(0, width // 2), pl.ds(width // 2, width // 2))[slot]

    def piece(source, owner):
        return pl.ds(pl.multiple_of(source * height + owner * part, part), part)

    own_part = pl.ds(pl.multiple_of(r * part, part), part)
    own_block = pl.ds(pl.multiple_of(f * height, height), height)

    def low_rows(source):
        return pl.ds(pl.multiple_of(source * rows, rows), rows)

    loads = [
        pltpu.make_async_copy(source, target, local.at[3 + n])
        for n, (source, target) in enumerate(
            (
                (full_query, loaded_query),
                (full_key, loaded_key),
                (inputs_far, inputs),
                (cot_query_far, cot_query),
                (cot_key_far, cot_key),
                (moments_query_far, moments_query),
                (moments_key_far, moments_key),
            )
        )
    ]
    barrier = pltpu.get_barrier_semaphore()

    def greet_fs(i):
        pl.semaphore_signal(barrier, inc=1, device_id={"fs": ahead(i)}, device_id_type=MESH)

    def greet_rep(j):
        pl.semaphore_signal(barrier, inc=1, device_id={"rep": beside(j)}, device_id_type=MESH)

    each(1, fs, greet_fs)
    each(1, rep, greet_rep)
    pl.semaphore_signal(barrier, inc=1, device_id={"tp": 1 - c}, device_id_type=MESH)
    pl.semaphore_wait(barrier, fs + rep - 1)

    bases = (basis_query, basis_key)
    weights = ((wide_query, weight_query_all), (wide_key, weight_key_all))

    def basis_fs(x, source, target):
        return remote(
            bases[x].at[own_part],
            basis_all.at[c, piece(source, r)],
            az_s.at[target],
            az_r.at[source],
            fs=target,
        )

    for x in range(2):

        @pl.when(c == x)
        def start_basis():
            each(1, fs, lambda i: basis_fs(x, f, ahead(i)).start())
            pltpu.make_async_copy(bases[x], basis_all.at[c, own_block], local.at[0]).start()

    for load in loads:
        load.start()
    own_basis = pltpu.make_async_copy(basis_query, basis_all.at[c, own_block], local.at[0])

    def basis_hop(source, slot, owner):
        block = basis_all.at[c, piece(source, owner), span_of(slot, rank)]
        return remote(
            block, block, ap_s.at[source, slot], ap_r.at[source, slot], rep=targets[slot]
        )

    def weight_fs(x, source, target):
        return remote(
            weights[x][0].at[own_part],
            weights[x][1].at[piece(source, r)],
            ez_s.at[x, target],
            ez_r.at[x, source],
            fs=target,
        )

    def weight_hop(x, source, slot, owner):
        block = weights[x][1].at[piece(source, owner), span_of(slot, weights[x][1].shape[1])]
        return remote(
            block, block, ep_s.at[x, source, slot], ep_r.at[x, source, slot], rep=targets[slot]
        )

    for load in loads[:2]:
        load.wait()
    wide_query[...] = loaded_query[...].astype(jnp.bfloat16)
    wide_key[...] = loaded_key[...].astype(jnp.bfloat16)

    def spread_basis(i):
        source = behind(i)
        basis_fs(0, source, source).wait_recv()
        for slot in (0, 1):
            basis_hop(source, slot, owners[slot]).start()

    each(1, fs, spread_basis)

    own_copies = [
        pltpu.make_async_copy(wide_query, weight_query_all.at[own_block], local.at[1]),
        pltpu.make_async_copy(wide_key, weight_key_all.at[own_block], local.at[2]),
    ]
    for copy in own_copies:
        copy.start()

    def start_weight(i):
        weight_fs(0, f, ahead(i)).start()
        weight_fs(1, f, ahead(i)).start()

    each(1, fs, start_weight)

    def relay_basis(i):
        source = behind(i)
        for slot in (0, 1):
            basis_hop(source, slot, senders[slot]).wait_recv()
            basis_hop(source, slot + 2, owners[slot + 2]).start()

    def all_basis(i):
        for slot in (2, 3):
            basis_hop(behind(i), slot, senders[slot]).wait_recv()

    each(1, fs, relay_basis)
    each(1, fs, all_basis)
    own_basis.wait()
    for load in loads[2:]:
        load.wait()

    for t in range(0, tokens, LANES):
        value = jnp.dot(
            inputs[t : t + LANES, :], basis_all[c], preferred_element_type=jnp.float32
        )
        factor[c, :, t : t + LANES] = value.T.astype(jnp.bfloat16)
    for u in range(units, per * rep):
        part_send[u] = jnp.zeros(part_send.shape[1:], jnp.bfloat16)
    factor_copy = remote(
        factor.at[c], factor.at[c], pair_s.at[0], pair_r.at[0], tp=1 - c
    )
    factor_back = remote(
        factor.at[1 - c], factor.at[1 - c], pair_s.at[0], pair_r.at[0], tp=1 - c
    )
    factor_copy.start()
    swap = remote(basis_all.at[c], basis_all.at[c], pair_s.at[1], pair_r.at[1], tp=1 - c)
    swap_back = remote(
        basis_all.at[1 - c], basis_all.at[1 - c], pair_s.at[1], pair_r.at[1], tp=1 - c
    )
    factor_back.wait_recv()
    swap.start()

    for x, cot in ((0, cot_query), (1, cot_key)):
        columns = cot.shape[1]
        width = 2 * LANES if columns % (2 * LANES) == 0 else LANES
        for n in range(0, columns, width):
            value = jnp.dot(
                factor[x], cot[:, n : n + width], preferred_element_type=jnp.float32
            ).astype(jnp.bfloat16)
            for k in range(0, width, LANES):
                part_send[x * query_units + (n + k) // LANES] = value[:, k : k + LANES]

    def group(owner):
        return pl.ds(owner * per, per)

    def part_rep(source, target):
        return remote(
            part_send.at[group(target)],
            part_recv.at[source],
            bp_s.at[target],
            bp_r.at[source],
            rep=target,
        )

    each(1, rep, lambda j: part_rep(r, beside(j)).start())
    part_recv[r] = part_send[group(r)]
    each(1, rep, lambda j: part_rep(beside(j), beside(j)).wait_recv())
    for p in range(per):
        value = part_recv[0, p].astype(jnp.float32)
        for q in range(1, rep):
            value = value + part_recv[q, p].astype(jnp.float32)
        slab[p] = value.astype(jnp.bfloat16)

    def slab_fs(source, target):
        return remote(
            slab.at[:, low_rows(target)],
            slab_recv.at[source],
            bz_s.at[target],
            bz_r.at[source],
            fs=target,
        )

    each(1, fs, lambda i: slab_fs(f, ahead(i)).start())

    def spread_weight(i):
        source = behind(i)
        for x in range(2):
            weight_fs(x, source, source).wait_recv()
            for slot in (0, 1):
                weight_hop(x, source, slot, owners[slot]).start()

    def relay_weight(i):
        source = behind(i)
        for slot in (0, 1):
            for x in range(2):
                weight_hop(x, source, slot, senders[slot]).wait_recv()
                weight_hop(x, source, slot + 2, owners[slot + 2]).start()

    spread_weight(1)
    slab_recv[f] = slab[:, low_rows(f), :]
    each(1, fs, lambda i: slab_fs(behind(i), behind(i)).wait_recv())
    for p in range(per):
        value = slab_recv[0, p].astype(jnp.float32)
        for q in range(1, fs):
            value = value + slab_recv[q, p].astype(jnp.float32)
        low_all[r * per + p] = value.astype(jnp.bfloat16)

    def low_rep(owner, target):
        block = low_all.at[group(owner)]
        return remote(block, block, lp_s.at[target], lp_r.at[owner], rep=target)

    each(1, rep, lambda j: low_rep(r, beside(j)).start())
    each(1, rep, lambda j: low_rep(beside(j), beside(j)).wait_recv())

    for x, moments, direction, low_out in (
        (0, moments_query, dir_query, low_query),
        (1, moments_key, dir_key, low_key),
    ):
        total = jnp.zeros((8, LANES), jnp.float32)
        for n in range(0, moments.shape[2], LANES):
            span = slice(n, n + LANES)
            low = low_all[x * query_units + n // LANES].astype(jnp.float32)
            low_out[:, span] = low
            first = 0.9 * moments[0, :, span] + 0.1 * low
            second = 0.95 * moments[1, :, span] + 0.05 * low * low
            normed = first / (jnp.sqrt(second) + 1e-08)
            direction[low_rows(f), span] = normed.astype(jnp.bfloat16)
            total = total + jnp.sum((normed * normed).reshape(rows // 8, 8, LANES), axis=0)
        squares[f, x] = total

    directions = (dir_query, dir_key)

    right, left = ahead(1), behind(1)

    def move_right(x, source):
        block = directions[x].at[low_rows(source)]
        return remote(block, block, dr_s.at[x, source], dz_r.at[x, source], fs=right)

    def move_left(x, source):
        block = directions[x].at[low_rows(source)]
        return remote(block, block, dl_s.at[x, source], dz_r.at[x, source], fs=left)

    def squares_fs(source, target):
        block = squares.at[source]
        return remote(block, block, qz_s.at[target], qz_r.at[source], fs=target)

    each(1, fs, lambda i: squares_fs(f, ahead(i)).start())

    @pl.when(f + 1 < fs)
    def start_right():
        for x in range(2):
            move_right(x, f).start()

    @pl.when(f > 0)
    def start_left():
        for x in range(2):
            move_left(x, f).start()

    each(2, fs, spread_weight)

    def relay_direction(k):
        @pl.when(f - k >= 0)
        def from_left():
            for x in range(2):
                move_right(x, f - k).wait_recv()

                @pl.when(f + 1 < fs)
                def onward():
                    move_right(x, f - k).start()

        @pl.when(f + k < fs)
        def from_right():
            for x in range(2):
                move_left(x, f + k).wait_recv()

                @pl.when(f > 0)
                def onward():
                    move_left(x, f + k).start()

    def relay_both(k):
        relay_weight(k)
        relay_direction(k)

    each(1, fs, relay_both)

    each(1, fs, lambda i: squares_fs(behind(i), behind(i)).wait_recv())
    total = squares[0]
    for q in range(1, fs):
        total = total + squares[q]
    pair[c] = total
    total_copy = remote(pair.at[c], pair.at[c], pair_s.at[2], pair_r.at[2], tp=1 - c)
    total_back = remote(pair.at[1 - c], pair.at[1 - c], pair_s.at[2], pair_r.at[2], tp=1 - c)
    total_copy.start()
    total_back.wait_recv()
    totals[...] = pair[0] + pair[1]

    def end_fs(i):
        source, target = behind(i), ahead(i)
        for x in range(2):
            for slot in (2, 3):
                weight_hop(x, source, slot, senders[slot]).wait_recv()
            for slot in range(4):
                weight_hop(x, source, slot, owners[slot]).wait_send()
            weight_fs(x, f, target).wait_send()
        for slot in range(4):
            basis_hop(source, slot, owners[slot]).wait_send()
        basis_fs(0, f, target).wait_send()
        slab_fs(f, target).wait_send()
        squares_fs(f, target).wait_send()

    def end_direction(k):
        @pl.when((f - k >= 0) & (f + 1 < fs))
        def end_right():
            for x in range(2):
                move_right(x, f - k).wait_send()

        @pl.when((f + k < fs) & (f > 0))
        def end_left():
            for x in range(2):
                move_left(x, f + k).wait_send()

    def end_rep(j):
        part_rep(r, beside(j)).wait_send()
        low_rep(r, beside(j)).wait_send()

    each(1, fs, end_fs)
    each(0, fs, end_direction)
    each(1, rep, end_rep)
    swap_back.wait_recv()
    factor_copy.wait_send()
    swap.wait_send()
    total_copy.wait_send()
    for copy in own_copies:
        copy.wait()


def exchange_grid(
    fs,
    rep,
    inputs_far,
    cot_query_far,
    cot_key_far,
    basis_query,
    basis_key,
    full_query,
    full_key,
    moments_query_far,
    moments_key_far,
    step_query,
    step_key,
    new_weight_query,
    new_weight_key,
    copy_query,
    copy_key,
    new_moments_query,
    new_moments_key,
    basis_all,
    weight_query_all,
    weight_key_all,
    dir_query,
    dir_key,
    inputs,
    cot_query,
    cot_key,
    moments_query,
    moments_key,
    loaded_query,
    loaded_key,
    factor,
    part,
    got_first,
    pair_sum,
    got_second,
    slab,
    slab_recv,
    low_all,
    part_squares,
    squares,
    pair,
    line_s,
    key_s,
    basis_line_r,
    query_line_r,
    key_line_r,
    hop_s,
    basis_hop_r,
    query_hop_r,
    basis_end_r,
    query_end_r,
    halve_s,
    first_r,
    second_r,
    slab_s,
    slab_r,
    low_s,
    low_r,
    low_end_r,
    dir_s,
    dir_r,
    dir_hop_s,
    dir_hop_r,
    dir_end_r,
    squares_s,
    squares_r,
    pair_s,
    pair_r,
    local,
):
    f, r, c = lax.axis_index("fs"), lax.axis_index("rep"), lax.axis_index("tp")
    height, rank = basis_query.shape
    quarter = height // rep
    rows = rank // fs
    own = rows // rep
    tokens = inputs.shape[0]
    query_units = cot_query.shape[1] // LANES
    units = query_units + cot_key.shape[1] // LANES
    streams = ((0, units // 2), (units // 2, units // 2))
    f32, bf16 = jnp.float32, jnp.bfloat16

    near = r + 1 - 2 * lax.rem(r, 2)
    far = r + 2 - 4 * (r // 2)
    across = 3 - r

    def when(conds, body):
        if not conds:
            body()
            return
        test = conds[0]
        for cond in conds[1:]:
            test = test & cond
        pl.when(test)(body)

    def send(make, *conds):
        when(conds, lambda: make().start())

    def arrived(block, sem, *conds):
        when(conds, lambda: remote(block, block, sem, sem, tp=1 - c).wait_recv())

    def departed(block, sem, *conds):
        when(conds, lambda: remote(block, block, sem, sem, tp=1 - c).wait_send())

    def sources(d):
        return ((f - d, f >= d), (f + d, f + d < fs))

    def beside(j):
        return lax.rem(r + j, rep)

    def rows_of(start, size):
        return pl.ds(pl.multiple_of(start, size), size)

    chunks = 2
    chunk = quarter // chunks
    fine = basis_line_r.shape[1]

    def piece(source, owner, k, parts=chunks):
        size = quarter // parts
        return rows_of(source * height + owner * quarter + k * size, size)

    mirror = f // (fs // 2)
    place_in_half = f + mirror * (fs - 1 - 2 * f)

    def other(n):
        low_side = n - 1 + (n + fs - 1 - place_in_half) // fs
        return low_side + mirror * (fs - 1 - 2 * low_side)

    own_block = rows_of(f * height, height)

    loads = [
        pltpu.make_async_copy(source, target, local.at[1 + n])
        for n, (source, target) in enumerate(
            (
                (full_query, loaded_query),
                (full_key, loaded_key),
                (inputs_far, inputs),
                (cot_query_far, cot_query),
                (cot_key_far, cot_key),
                (moments_query_far, moments_query),
                (moments_key_far, moments_key),
            )
        )
    ]
    bases = (basis_query, basis_key)
    for x in range(2):

        @pl.when(c == x)
        def load_basis():
            pltpu.make_async_copy(bases[x], basis_all.at[c, own_block], local.at[0]).start()

    for load in loads:
        load.start()
    own_basis = pltpu.make_async_copy(basis_query, basis_all.at[c, own_block], local.at[0])
    barrier = pltpu.get_barrier_semaphore()
    for i in range(1, fs):
        pl.semaphore_signal(
            barrier, inc=1, device_id={"fs": lax.rem(f + i, fs)}, device_id_type=MESH
        )
    for mate in (near, far):
        pl.semaphore_signal(barrier, inc=1, device_id={"rep": mate}, device_id_type=MESH)
    pl.semaphore_signal(barrier, inc=1, device_id={"tp": 1 - c}, device_id_type=MESH)
    pl.semaphore_wait(barrier, fs + 2)

    def basis_z(source, up, k):
        block = basis_all.at[c, piece(source, r, k, fine)]
        return remote(block, block, line_s.at[0], basis_line_r.at[source, k], fs=f + 2 * up - 1)

    ways = ((1, f + 1 < fs), (0, f > 0))
    edge = (f == 0) | (f == fs - 1)
    inner = (f > 0) & (f < fs - 1)
    def hop_span(slot, width):
        return (pl.ds(0, width), pl.ds(0, width), pl.ds(0, width // 2), pl.ds(width // 2, width // 2))[slot]

    targets = (near, far, far, near)
    sent = (r, r, near, far)

    def basis_hop(k, source, slot):
        block = basis_all.at[c, piece(source, sent[slot], k, fine), hop_span(slot, rank)]
        landed = basis_hop_r.at[source, k] if slot < 2 else basis_end_r.at[0]
        return remote(block, block, hop_s.at[0], landed, rep=targets[slot])

    def weight_hop(k, source, slot):
        width = weight_query_all.shape[1]
        block = weight_query_all.at[piece(source, sent[slot], k), hop_span(slot, width)]
        landed = query_hop_r.at[source, k] if slot < 2 else query_end_r.at[source]
        return remote(block, block, hop_s.at[1], landed, rep=targets[slot])

    def spread(hop, source, *there):
        for slot in (0, 1):
            send(functools.partial(hop, source, slot), *there)

    def relay(hop, both, sem, source, *there):
        arrived(both, sem, *there)
        for slot in (2, 3):
            send(functools.partial(hop, source, slot), *there)

    def relay_basis(k, source, *there):
        both = basis_all.at[c, pl.ds(0, 2 * (quarter // fine))]
        relay(functools.partial(basis_hop, k), both, basis_hop_r.at[source, k], source, *there)

    def relay_weight(k, source):
        both = weight_query_all.at[pl.ds(0, 2 * chunk)]
        relay(functools.partial(weight_hop, k), both, query_hop_r.at[source, k], source)

    def query_z(source, up, k):
        block = weight_query_all.at[piece(source, r, k)]
        return remote(block, block, line_s.at[1], query_line_r.at[source, k], fs=f + 2 * up - 1)

    def key_z(source, up, k):
        block = weight_key_all.at[rows_of(source * height, height)]
        return remote(block, block, key_s.at[up], key_line_r.at[source], fs=f + 2 * up - 1)

    def launch(line, parts=chunks):
        for k in range(parts):
            for up, there in ways:
                send(functools.partial(line, f, up, k), there)

    def onward(line, d, k, *conds):
        for source, there, up, more in (
            (f - d, f >= d, 1, f + 1 < fs),
            (f + d, f + d < fs, 0, f > 0),
        ):
            when((there, *conds), lambda: line(source, up, k).wait_recv())
            if d + 1 < fs:
                send(functools.partial(line, source, up, k), there, more, *conds)

    def onward_all(line, d, parts=chunks):
        for k in range(parts):
            onward(line, d, k)

    own_basis.wait()
    launch(basis_z, fine)
    for load in loads[:2]:
        load.wait()
    weight_query_all[own_block, :] = loaded_query[...].astype(bf16)
    weight_key_all[own_block, :] = loaded_key[...].astype(bf16)

    steps = [(d, k) for d in range(1, fs) for k in range(fine)]
    for n, (d, k) in enumerate(steps):
        onward(basis_z, d, k)
        for source, there in sources(d):
            spread(functools.partial(basis_hop, k), source, there)
        if (d, k) == (max(fs - 2, 1), fine - 1):
            launch(query_z)
        if n >= 6:
            before, j = steps[n - 6]
            for source, there in sources(before):
                relay_basis(j, source, there)
    for d, k in steps[-6:]:
        for source, there in sources(d):
            relay_basis(k, source, there)
    onward_all(query_z, 1)
    launch(key_z, 1)
    spread(functools.partial(weight_hop, 0), other(1))
    arrived(basis_all.at[c, pl.ds(0, (fs - 1) * quarter)], basis_end_r.at[0])
    for load in loads[2:]:
        load.wait()

    for t in range(0, tokens, LANES):
        value = jnp.dot(inputs[t : t + LANES, :], basis_all[c], preferred_element_type=f32)
        factor[c, :, t : t + LANES] = value.T.astype(bf16)

    def partner(block, back, n):
        return (
            remote(block, block, pair_s.at[n], pair_r.at[n], tp=1 - c),
            remote(back, back, pair_s.at[n], pair_r.at[n], tp=1 - c),
        )

    factor_copy, factor_back = partner(factor.at[c], factor.at[1 - c], 0)
    swap, swap_back = partner(basis_all.at[c], basis_all.at[1 - c], 1)
    factor_copy.start()
    factor_back.wait_recv()
    swap.start()

    for x, cot in ((0, cot_query), (1, cot_key)):
        columns = cot.shape[1]
        width = 2 * LANES if columns % (2 * LANES) == 0 else LANES
        for n in range(0, columns, width):
            value = jnp.dot(
                factor[x], cot[:, n : n + width], preferred_element_type=f32
            ).astype(bf16)
            for k in range(0, width, LANES):
                for q in range(rep):
                    for s in range(fs):
                        part[x * query_units + (n + k) // LANES, q, s * own : (s + 1) * own] = value[
                            s * rows + q * own : s * rows + (q + 1) * own, k : k + LANES
                        ]

    half = rows // 2
    spans = (slice(0, half), slice(half, rows))
    mates = ((near, far), (far, near))

    def columns_of(g):
        return pl.ds(streams[g][0], streams[g][1])

    def first_hop(h, g, w):
        owner = (across, mates[h][0])[w]
        return remote(
            part.at[columns_of(g), owner, pl.ds(h * half, half)],
            got_first.at[h, w, columns_of(g)],
            halve_s.at[0],
            (first_r, second_r)[w].at[g],
            rep=mates[h][0],
        )

    def second_hop(h, g):
        return remote(
            pair_sum.at[h, columns_of(g)],
            got_second.at[h, columns_of(g)],
            halve_s.at[1],
            second_r.at[g],
            rep=mates[h][1],
        )

    def start_first(g, w):
        for h in range(2):
            first_hop(h, g, w).start()

    def start_second(g):
        arrived(got_first.at[:, 0, columns_of(g)], first_r.at[g])
        for h in range(2):
            for u in range(streams[g][0], sum(streams[g])):
                pair_sum[h, u] = (
                    part[u, mates[h][1], spans[h]].astype(f32) + got_first[h, 0, u].astype(f32)
                ).astype(bf16)
            second_hop(h, g).start()

    def slab_z(g, source, target):
        return remote(
            slab.at[columns_of(g), rows_of(target * own, own)],
            slab_recv.at[source, columns_of(g)],
            slab_s.at[0],
            slab_r.at[g],
            fs=target,
        )

    def end_rep(g):
        arrived(got_first.at[:, :, columns_of(g)], second_r.at[g])
        for h in range(2):
            for u in range(streams[g][0], sum(streams[g])):
                slab[u, spans[h]] = (
                    part[u, r, spans[h]].astype(f32)
                    + got_first[h, 1, u].astype(f32)
                    + got_second[h, u].astype(f32)
                ).astype(bf16)
        for n in range(fs - 1, 0, -1):
            slab_z(g, f, other(n)).start()
        for u in range(streams[g][0], sum(streams[g])):
            slab_recv[f, u] = slab[u, rows_of(f * own, own)]

    start_first(0, 0)
    start_first(0, 1)
    start_first(1, 0)
    start_second(0)
    start_first(1, 1)
    start_second(1)
    for k in range(1, chunks):
        spread(functools.partial(weight_hop, k), other(1))
    end_rep(0)
    end_rep(1)
    for k in range(chunks):
        when((edge,), lambda: query_z(other(2), 1, k).wait_recv())
        spread(functools.partial(weight_hop, k), other(2))

    directions, new_moments = (dir_query, dir_key), (new_moments_query, new_moments_key)
    moments = (moments_query, moments_key)

    def place(u):
        x = 0 if u < query_units else 1
        n = (u - x * query_units) * LANES
        return x, slice(n, n + LANES)

    def pieces(g):
        first, last = streams[g][0], sum(streams[g])
        found = []
        if first < query_units:
            found.append((0, first * LANES, (min(last, query_units) - first) * LANES))
        if last > query_units:
            start = max(first, query_units)
            found.append((1, (start - query_units) * LANES, (last - start) * LANES))
        return found

    def dir_rows(source, owner):
        return rows_of(source * rows + owner * own, own)

    def update(g, owner):
        sums = [jnp.zeros((8, LANES), f32), jnp.zeros((8, LANES), f32)]
        mine = rows_of(owner * own, own)
        for u in range(streams[g][0], sum(streams[g])):
            x, span = place(u)
            low = low_all[owner, u].astype(f32)
            first = 0.9 * moments[x][0, mine, span] + 0.1 * low
            second = 0.95 * moments[x][1, mine, span] + 0.05 * low * low
            new_moments[x][0, mine, span] = first
            new_moments[x][1, mine, span] = second
            normed = first / (jnp.sqrt(second) + 1e-08)
            directions[x][dir_rows(f, owner), span] = normed.astype(bf16)
            sums[x] = sums[x] + jnp.sum((normed * normed).reshape(own // 8, 8, LANES), axis=0)
        for x in range(2):
            part_squares[owner, g, x] = sums[x]

    def low_hop(g, slot):
        block = low_all.at[sent[slot], columns_of(g)]
        landed = low_r.at[g] if slot == g else low_end_r.at[0]
        return remote(block, block, low_s.at[0], landed, rep=targets[slot])

    def dir_blocks(g, source, owner):
        return [
            (x, directions[x].at[dir_rows(source, owner), pl.ds(start, size)])
            for x, start, size in pieces(g)
        ]

    def dir_line(g, source, up):
        for x, block in dir_blocks(g, source, r):
            remote(block, block, dir_s.at[x], dir_r.at[g, source], fs=f + 2 * up - 1).start()

    def dir_hop(g, slot, n):
        landed = dir_hop_r.at[n, g] if slot == g else dir_end_r.at[n]
        for x, block in dir_blocks(g, other(n), sent[slot]):
            remote(block, block, dir_hop_s.at[n], landed, rep=targets[slot]).start()

    def end_fs(g):
        arrived(slab_recv.at[pl.ds(0, fs - 1), columns_of(g)], slab_r.at[g])
        for u in range(streams[g][0], sum(streams[g])):
            value = slab_recv[0, u].astype(f32)
            for q in range(1, fs):
                value = value + slab_recv[q, u].astype(f32)
            low_all[r, u] = value.astype(bf16)
        for slot in (0, 1):
            low_hop(g, slot).start()
        update(g, r)
        for up, there in ways:
            when((there,), lambda: dir_line(g, f, up))

    end_fs(0)
    end_fs(1)

    def onward_dir(d):
        for g in range(2):
            for source, there, up, more in (
                (f - d, f >= d, 1, f + 1 < fs),
                (f + d, f + d < fs, 0, f > 0),
            ):
                arrived(low_all.at[r, columns_of(g)], dir_r.at[g, source], there)
                if d + 1 < fs:
                    when((there, more), lambda: dir_line(g, source, up))

    def spread_dir(n, *conds):
        for g in range(2):
            for slot in (0, 1):
                when(conds, lambda: dir_hop(g, slot, n))

    def relay_dir(n):
        for g in range(2):
            arrived(low_all.at[r, columns_of(g)], dir_hop_r.at[n, g])
            dir_hop(g, g + 2, n)

    def finish_dir(n):
        arrived(low_all.at[pl.ds(0, 2)], dir_end_r.at[n])

    for k in range(chunks):
        relay_weight(k, other(1))
    onward_dir(1)
    spread_dir(1)
    spread_dir(2, inner)
    for g in range(2):
        arrived(low_all.at[r, columns_of(g)], low_r.at[g])
        low_hop(g, g + 2).start()
    onward_dir(2)
    spread_dir(2, edge)
    spread_dir(3, inner)
    for k in range(chunks):
        onward(query_z, 2, k, inner)
    relay_dir(1)
    onward_dir(3)
    spread_dir(3, edge)
    arrived(low_all.at[pl.ds(0, 2)], low_end_r.at[0])
    for g in range(2):
        for j in range(1, rep):
            update(g, beside(j))
    for x in range(2):
        total = part_squares[0, 0, x] + part_squares[0, 1, x]
        for q in range(1, rep):
            total = total + (part_squares[q, 0, x] + part_squares[q, 1, x])
        squares[f, x] = total

    mine = squares.at[f]
    for n in range(1, fs):
        remote(mine, mine, squares_s.at[0], squares_r.at[0], fs=other(n)).start()
    onward_all(key_z, 1, 1)
    relay_dir(2)
    relay_dir(3)
    for n in range(3, fs):
        for k in range(chunks):
            onward(query_z, n, k)
            spread(functools.partial(weight_hop, k), other(n))
    for k in range(chunks):
        relay_weight(k, other(2))
    def relay_last(k):
        for n in range(3, fs):
            relay_weight(k, other(n))

    def finish_weight(n):
        arrived(weight_query_all.at[pl.ds(0, quarter)], query_end_r.at[other(n)])

    arrived(squares.at[pl.ds(0, fs - 1)], squares_r.at[0])
    total = squares[0]
    for q in range(1, fs):
        total = total + squares[q]
    pair[c] = total
    total_copy, total_back = partner(pair.at[c], pair.at[1 - c], 2)
    total_copy.start()
    for d in range(1, fs):
        finish_dir(d)
    total_back.wait_recv()
    totals = pair[0] + pair[1]
    weights_all, copies = (weight_query_all, weight_key_all), (copy_query, copy_key)
    scales = [
        lax.rsqrt(jnp.sum(totals[x], keepdims=True) / (pair.shape[0] * rank * copies[x].shape[1]) + 1e-06)
        for x in range(2)
    ]

    def product(x, span, columns):
        return scales[x] * jnp.dot(
            basis_all[x, span], directions[x][:, columns], preferred_element_type=f32
        )

    def column_blocks(x):
        wide = copies[x].shape[1]
        width = 2 * LANES if wide % (2 * LANES) == 0 else LANES
        return [slice(n, n + width) for n in range(0, wide, width)]

    def copy_rows(x, start, size):
        span = rows_of(start, size)
        for columns in column_blocks(x):
            weight = weights_all[x][span, columns].astype(f32)
            copies[x][span, columns] = (weight - 0.02 * product(x, span, columns)).astype(bf16)

    swap_back.wait_recv()
    for x, weight, step_out, new_out in (
        (0, loaded_query, step_query, new_weight_query),
        (1, loaded_key, step_key, new_weight_key),
    ):
        for columns in column_blocks(x):
            step = product(x, own_block, columns)
            step_out[:, columns] = step
            new = weight[:, columns] - 0.02 * step
            new_out[:, columns] = new
            copies[x][own_block, columns] = new.astype(bf16)

    finish_weight(1)
    copy_rows(0, other(1) * height, height)
    relay_last(0)
    for d in range(2, fs - 1):
        onward_all(key_z, d, 1)
    for n in (1, 2):
        copy_rows(1, other(n) * height, height)
    relay_last(1)
    finish_weight(2)
    copy_rows(0, other(2) * height, height)
    for n in range(3, fs):
        for owner in (r, near, far):
            copy_rows(0, other(n) * height + owner * quarter, quarter)
    for d in range(max(fs - 1, 3), fs):
        onward_all(key_z, d, 1)
    for n in range(3, fs):
        copy_rows(1, other(n) * height, height)
    for n in range(3, fs):
        finish_weight(n)
        copy_rows(0, other(n) * height + across * quarter, quarter)
    hops = (fs - 1) * (rep - 1) * quarter
    for n, block in ((0, basis_all.at[c]), (1, weight_query_all)):
        departed(block.at[pl.ds(0, quarter)], line_s.at[n], edge)
        departed(block.at[pl.ds(0, (fs + 1) * quarter)], line_s.at[n], inner)
        departed(block.at[pl.ds(0, hops)], hop_s.at[n])
    for n in range(fs):
        if n < fs - 1:
            departed(weight_key_all.at[pl.ds(0, (n + 1) * height)], key_s.at[1], f == n)
        if n > 0:
            departed(weight_key_all.at[pl.ds(0, (fs - n) * height)], key_s.at[0], f == n)
    departed(got_first, halve_s.at[0])
    departed(pair_sum, halve_s.at[1])
    departed(slab_recv.at[pl.ds(0, fs - 1)], slab_s.at[0])
    departed(low_all.at[pl.ds(0, rep - 1)], low_s.at[0])
    for x in range(2):
        departed(directions[x].at[pl.ds(0, own)], dir_s.at[x], edge)
        departed(directions[x].at[pl.ds(0, (fs + 1) * own)], dir_s.at[x], inner)
    for n in range(1, fs):
        departed(low_all.at[pl.ds(0, rep - 1)], dir_hop_s.at[n])
    departed(squares.at[pl.ds(0, fs - 1)], squares_s.at[0])
    for copy in (factor_copy, swap, total_copy):
        copy.wait_send()


def write_out(*refs):
    count = len(refs) // 2
    copies, starts = [], []
    for n, (source, target) in enumerate(zip(refs[:count], refs[count : 2 * count])):
        copies.append(pltpu.make_async_copy(source, target, refs[-1].at[n]))
        size = source.shape[0] // 4 if source.ndim == 2 else 1
        for start in range(0, source.shape[0], size):
            span = pl.ds(start, size)
            starts.append(pltpu.make_async_copy(source.at[span], target.at[span], refs[-1].at[n]))
    for copy in starts:
        copy.start()
    for copy in copies:
        copy.wait()


def apply(
    count_query,
    count_key,
    totals,
    dir_query,
    dir_key,
    low_query,
    low_key,
    moments_query,
    moments_key,
    basis_all,
    weight_query_all,
    weight_key_all,
    basis_query,
    basis_key,
    weight_query,
    weight_key,
    step_query,
    step_key,
    new_weight_query,
    new_weight_key,
    copy_query,
    copy_key,
    new_moments_query,
    new_moments_key,
):
    parts = (
        (count_query, dir_query, weight_query_all, basis_query, weight_query),
        (count_key, dir_key, weight_key_all, basis_key, weight_key),
    )
    outs = (
        (step_query, new_weight_query, copy_query),
        (step_key, new_weight_key, copy_key),
    )
    for x in range(2):
        count, direction, weight_all, basis, weight = parts[x]
        step_out, new_weight_out, copy_out = outs[x]
        scale = lax.rsqrt(jnp.sum(totals[x], keepdims=True) / count + 1e-06)
        step = scale * jnp.dot(basis[...], direction[...], preferred_element_type=jnp.float32)
        step_out[...] = step
        new_weight_out[...] = weight[...] - 0.02 * step
        whole = scale * jnp.dot(
            basis_all[x], direction[...], preferred_element_type=jnp.float32
        )
        copy_out[...] = (weight_all[...].astype(jnp.float32) - 0.02 * whole).astype(jnp.bfloat16)

    @pl.when(pl.program_id(0) == 0)
    def moments_once():
        for moments, low_ref, out in (
            (moments_query, low_query, new_moments_query),
            (moments_key, low_key, new_moments_key),
        ):
            low = low_ref[...]
            out[0] = 0.9 * moments[0] + 0.1 * low
            out[1] = 0.95 * moments[1] + 0.05 * low * low


def on_device(
    inputs,
    cot_query,
    cot_key,
    basis_query,
    basis_key,
    weight_query,
    weight_key,
    moments_query,
    moments_key,
):
    fs, rep, tp = lax.axis_size("fs"), lax.axis_size("rep"), lax.axis_size("tp")
    assert tp == 2 and rep == 4
    height, rank = basis_query.shape
    rows = rank // fs
    tokens = inputs.shape[0]
    query_cols, key_cols = cot_query.shape[1], cot_key.shape[1]
    per = -(-((query_cols + key_cols) // LANES) // rep)
    vmem = pl.BlockSpec(memory_space=pltpu.VMEM)
    hbm = pl.BlockSpec(memory_space=pl.ANY)
    bf16, f32 = jnp.bfloat16, jnp.float32
    dma = pltpu.SemaphoreType.DMA
    shape = jax.ShapeDtypeStruct
    owned = tuple(
        shape((height, columns), f32) for columns in (query_cols, key_cols, query_cols, key_cols)
    )
    results = owned + (
        shape((height * fs, query_cols), bf16),
        shape((height * fs, key_cols), bf16),
        shape((2, rows, query_cols), f32),
        shape((2, rows, key_cols), f32),
    )
    own, units = rows // rep, (query_cols + key_cols) // LANES
    if own % 16 == 0 and fs == 4 and units % 2 == 0:
        fresh = pl.pallas_call(
            functools.partial(exchange_grid, fs, rep),
            out_shape=results,
            in_specs=[pl.BlockSpec(memory_space=pltpu.HBM)] * 9,
            out_specs=(vmem,) * 8,
            scratch_shapes=[
                pltpu.VMEM((2, height * fs, rank), bf16),
                pltpu.VMEM((height * fs, query_cols), bf16),
                pltpu.VMEM((height * fs, key_cols), bf16),
                pltpu.VMEM((rank, query_cols), bf16),
                pltpu.VMEM((rank, key_cols), bf16),
                pltpu.VMEM((tokens, inputs.shape[1]), bf16),
                pltpu.VMEM((tokens, query_cols), bf16),
                pltpu.VMEM((tokens, key_cols), bf16),
                pltpu.VMEM((2, rows, query_cols), f32),
                pltpu.VMEM((2, rows, key_cols), f32),
                pltpu.VMEM((height, query_cols), f32),
                pltpu.VMEM((height, key_cols), f32),
                pltpu.VMEM((2, rank, tokens), bf16),
                pltpu.VMEM((units, rep, rows, LANES), bf16),
                pltpu.VMEM((2, 2, units, rows // 2, LANES), bf16),
                pltpu.VMEM((2, units, rows // 2, LANES), bf16),
                pltpu.VMEM((2, units, rows // 2, LANES), bf16),
                pltpu.VMEM((units, rows, LANES), bf16),
                pltpu.VMEM((fs, units, own, LANES), bf16),
                pltpu.VMEM((rep, units, own, LANES), bf16),
                pltpu.VMEM((rep, 2, 2, 8, LANES), f32),
                pltpu.VMEM((fs, 2, 8, LANES), f32),
                pltpu.VMEM((2, 2, 8, LANES), f32),
                dma((2,)),
                dma((2,)),
                dma((fs, 4)),
                dma((fs, 2)),
                dma((fs,)),
                dma((2,)),
                dma((fs, 4)),
                dma((fs, 2)),
                dma((1,)),
                dma((fs,)),
                dma((2,)),
                dma((2,)),
                dma((2,)),
                dma((1,)),
                dma((2,)),
                dma((1,)),
                dma((2,)),
                dma((1,)),
                dma((2,)),
                dma((2, fs)),
                dma((fs,)),
                dma((fs, 2)),
                dma((fs,)),
                dma((1,)),
                dma((1,)),
                dma((3,)),
                dma((3,)),
                dma((8,)),
            ],
            compiler_params=pltpu.CompilerParams(
                collective_id=0, has_side_effects=True, vmem_limit_bytes=40 * 1024 * 1024
            ),
        )(
            *(
                pltpu.with_memory_space_constraint(operand, pltpu.HBM)
                for operand in (
                    inputs,
                    cot_query,
                    cot_key,
                    basis_query,
                    basis_key,
                    weight_query,
                    weight_key,
                    moments_query,
                    moments_key,
                )
            )
        )
        return pl.pallas_call(
            write_out,
            out_shape=results,
            in_specs=[vmem] * 8,
            out_specs=(hbm,) * 8,
            scratch_shapes=[dma((8,))],
            compiler_params=pltpu.CompilerParams(vmem_limit_bytes=32 * 1024 * 1024),
        )(*fresh)

    (
        basis_all,
        weight_query_all,
        weight_key_all,
        dir_query,
        dir_key,
        low_query,
        low_key,
        totals,
    ) = pl.pallas_call(
        functools.partial(exchange, fs, rep),
        out_shape=(
            shape((2, height * fs, rank), bf16),
            shape((height * fs, query_cols), bf16),
            shape((height * fs, key_cols), bf16),
            shape((rank, query_cols), bf16),
            shape((rank, key_cols), bf16),
            shape((rows, query_cols), f32),
            shape((rows, key_cols), f32),
            shape((2, 8, LANES), f32),
        ),
        in_specs=[pl.BlockSpec(memory_space=pltpu.HBM)] * 9,
        out_specs=(vmem, hbm, hbm, vmem, vmem, vmem, vmem, vmem),
        scratch_shapes=[
            pltpu.VMEM((tokens, inputs.shape[1]), bf16),
            pltpu.VMEM((tokens, query_cols), bf16),
            pltpu.VMEM((tokens, key_cols), bf16),
            pltpu.VMEM((2, rows, query_cols), f32),
            pltpu.VMEM((2, rows, key_cols), f32),
            pltpu.VMEM((height, query_cols), f32),
            pltpu.VMEM((height, key_cols), f32),
            pltpu.VMEM((height, query_cols), bf16),
            pltpu.VMEM((height, key_cols), bf16),
            pltpu.VMEM((2, rank, tokens), bf16),
            pltpu.VMEM((per * rep, rank, LANES), bf16),
            pltpu.VMEM((rep, per, rank, LANES), bf16),
            pltpu.VMEM((per, rank, LANES), bf16),
            pltpu.VMEM((fs, per, rows, LANES), bf16),
            pltpu.VMEM((per * rep, rows, LANES), bf16),
            pltpu.VMEM((fs, 2, 8, LANES), f32),
            pltpu.VMEM((2, 2, 8, LANES), f32),
            dma((fs,)),
            dma((fs,)),
            dma((fs, rep)),
            dma((fs, rep)),
            dma((2, fs)),
            dma((2, fs)),
            dma((2, fs, rep)),
            dma((2, fs, rep)),
            dma((rep,)),
            dma((rep,)),
            dma((fs,)),
            dma((fs,)),
            dma((rep,)),
            dma((rep,)),
            dma((2, fs)),
            dma((2, fs)),
            dma((2, fs)),
            dma((fs,)),
            dma((fs,)),
            dma((3,)),
            dma((3,)),
            dma((10,)),
        ],
        compiler_params=pltpu.CompilerParams(
            collective_id=0, has_side_effects=True, vmem_limit_bytes=32 * 1024 * 1024
        ),
    )(
        *(
            pltpu.with_memory_space_constraint(operand, pltpu.HBM)
            for operand in (
                inputs,
                cot_query,
                cot_key,
                basis_query,
                basis_key,
                weight_query,
                weight_key,
                moments_query,
                moments_key,
            )
        )
    )

    steps = min(8, height // 16)
    tall, short = height * fs // steps, height // steps

    def fixed(*dims):
        return pl.BlockSpec(dims, lambda i: (0,) * len(dims))

    def banded(*dims):
        return pl.BlockSpec(dims, lambda i: (i, 0))

    owned_specs = tuple(
        banded(short, columns) for columns in (query_cols, key_cols, query_cols, key_cols)
    )
    return pl.pallas_call(
        functools.partial(
            apply, float(rank * query_cols * tp), float(rank * key_cols * tp)
        ),
        grid=(steps,),
        out_shape=results,
        in_specs=[
            fixed(2, 8, LANES),
            fixed(rank, query_cols),
            fixed(rank, key_cols),
            fixed(rows, query_cols),
            fixed(rows, key_cols),
            fixed(2, rows, query_cols),
            fixed(2, rows, key_cols),
            pl.BlockSpec((2, tall, rank), lambda i: (0, i, 0)),
            banded(tall, query_cols),
            banded(tall, key_cols),
            banded(short, rank),
            banded(short, rank),
            banded(short, query_cols),
            banded(short, key_cols),
        ],
        out_specs=owned_specs
        + (
            banded(tall, query_cols),
            banded(tall, key_cols),
            fixed(2, rows, query_cols),
            fixed(2, rows, key_cols),
        ),
        compiler_params=pltpu.CompilerParams(
            dimension_semantics=("arbitrary",), vmem_limit_bytes=32 * 1024 * 1024
        ),
    )(
        totals,
        dir_query,
        dir_key,
        low_query,
        low_key,
        moments_query,
        moments_key,
        basis_all,
        weight_query_all,
        weight_key_all,
        basis_query,
        basis_key,
        weight_query,
        weight_key,
    )


def solution(mesh):
    in_specs = (
        P(("fs", "rep"), None),
        P(("fs", "rep"), "tp"),
        P(("fs", "rep"), "tp"),
        P("fs", None),
        P("fs", None),
        P("fs", "tp"),
        P("fs", "tp"),
        P(None, "fs", "tp"),
        P(None, "fs", "tp"),
    )
    out_specs = (
        P("fs", "tp"),
        P("fs", "tp"),
        P("fs", "tp"),
        P("fs", "tp"),
        P(None, "tp"),
        P(None, "tp"),
        P(None, "fs", "tp"),
        P(None, "fs", "tp"),
    )
    return jax.shard_map(
        on_device, mesh=mesh, in_specs=in_specs, out_specs=out_specs, check_vma=False
    )
```

```python
import functools
import jax
import jax.numpy as jnp
from jax import lax
from jax.experimental import pallas as pl
from jax.experimental.pallas import tpu as pltpu
from jax.sharding import PartitionSpec as P

MESH = pl.DeviceIdType.MESH
LANES = 128


def each(start, stop, body):
    if stop - start <= 4:
        for i in range(start, stop):
            body(i)
    else:
        lax.fori_loop(start, stop, lambda i, carry: (body(i), carry)[1], 0)


def remote(src, dst, send_sem, recv_sem, **device):
    return pltpu.make_async_remote_copy(
        src_ref=src,
        dst_ref=dst,
        send_sem=send_sem,
        recv_sem=recv_sem,
        device_id=device,
        device_id_type=MESH,
    )


def exchange(
    fs,
    rep,
    inputs_far,
    cot_query_far,
    cot_key_far,
    basis_query,
    basis_key,
    full_query,
    full_key,
    moments_query_far,
    moments_key_far,
    basis_all,
    weight_query_all,
    weight_key_all,
    dir_query,
    dir_key,
    low_query,
    low_key,
    totals,
    inputs,
    cot_query,
    cot_key,
    moments_query,
    moments_key,
    loaded_query,
    loaded_key,
    wide_query,
    wide_key,
    factor,
    part_send,
    part_recv,
    slab,
    slab_recv,
    low_all,
    squares,
    pair,
    az_s,
    az_r,
    ap_s,
    ap_r,
    ez_s,
    ez_r,
    ep_s,
    ep_r,
    bp_s,
    bp_r,
    bz_s,
    bz_r,
    lp_s,
    lp_r,
    dr_s,
    dl_s,
    dz_r,
    qz_s,
    qz_r,
    pair_s,
    pair_r,
    local,
):
    f, r, c = lax.axis_index("fs"), lax.axis_index("rep"), lax.axis_index("tp")
    height = basis_query.shape[0]
    part = height // rep
    rank = basis_query.shape[1]
    rows = rank // fs
    tokens = inputs.shape[0]
    per = part_send.shape[0] // rep
    query_units = cot_query.shape[1] // LANES
    units = query_units + cot_key.shape[1] // LANES

    def ahead(i):
        return lax.rem(f + i, fs)

    def behind(i):
        return lax.rem(f + fs - i, fs)

    def beside(j):
        return lax.rem(r + j, rep)

    near = r + 1 - 2 * lax.rem(r, 2)
    far = r + 2 - 4 * (r // 2)
    across = 3 - r
    owners = (r, r, near, far)
    targets = (near, far, far, near)
    senders = (near, far, across, across)

    def span_of(slot, width):
        return (pl.ds(0, width), pl.ds(0, width), pl.ds(0, width // 2), pl.ds(width // 2, width // 2))[slot]

    def piece(source, owner):
        return pl.ds(pl.multiple_of(source * height + owner * part, part), part)

    own_part = pl.ds(pl.multiple_of(r * part, part), part)
    own_block = pl.ds(pl.multiple_of(f * height, height), height)

    def low_rows(source):
        return pl.ds(pl.multiple_of(source * rows, rows), rows)

    loads = [
        pltpu.make_async_copy(source, target, local.at[3 + n])
        for n, (source, target) in enumerate(
            (
                (full_query, loaded_query),
                (full_key, loaded_key),
                (inputs_far, inputs),
                (cot_query_far, cot_query),
                (cot_key_far, cot_key),
                (moments_query_far, moments_query),
                (moments_key_far, moments_key),
            )
        )
    ]
    barrier = pltpu.get_barrier_semaphore()

    def greet_fs(i):
        pl.semaphore_signal(barrier, inc=1, device_id={"fs": ahead(i)}, device_id_type=MESH)

    def greet_rep(j):
        pl.semaphore_signal(barrier, inc=1, device_id={"rep": beside(j)}, device_id_type=MESH)

    each(1, fs, greet_fs)
    each(1, rep, greet_rep)
    pl.semaphore_signal(barrier, inc=1, device_id={"tp": 1 - c}, device_id_type=MESH)
    pl.semaphore_wait(barrier, fs + rep - 1)

    bases = (basis_query, basis_key)
    weights = ((wide_query, weight_query_all), (wide_key, weight_key_all))

    def basis_fs(x, source, target):
        return remote(
            bases[x].at[own_part],
            basis_all.at[c, piece(source, r)],
            az_s.at[target],
            az_r.at[source],
            fs=target,
        )

    for x in range(2):

        @pl.when(c == x)
        def start_basis():
            each(1, fs, lambda i: basis_fs(x, f, ahead(i)).start())
            pltpu.make_async_copy(bases[x], basis_all.at[c, own_block], local.at[0]).start()

    for load in loads:
        load.start()
    own_basis = pltpu.make_async_copy(basis_query, basis_all.at[c, own_block], local.at[0])

    def basis_hop(source, slot, owner):
        block = basis_all.at[c, piece(source, owner), span_of(slot, rank)]
        return remote(
            block, block, ap_s.at[source, slot], ap_r.at[source, slot], rep=targets[slot]
        )

    def weight_fs(x, source, target):
        return remote(
            weights[x][0].at[own_part],
            weights[x][1].at[piece(source, r)],
            ez_s.at[x, target],
            ez_r.at[x, source],
            fs=target,
        )

    def weight_hop(x, source, slot, owner):
        block = weights[x][1].at[piece(source, owner), span_of(slot, weights[x][1].shape[1])]
        return remote(
            block, block, ep_s.at[x, source, slot], ep_r.at[x, source, slot], rep=targets[slot]
        )

    for load in loads[:2]:
        load.wait()
    wide_query[...] = loaded_query[...].astype(jnp.bfloat16)
    wide_key[...] = loaded_key[...].astype(jnp.bfloat16)

    def spread_basis(i):
        source = behind(i)
        basis_fs(0, source, source).wait_recv()
        for slot in (0, 1):
            basis_hop(source, slot, owners[slot]).start()

    each(1, fs, spread_basis)

    own_copies = [
        pltpu.make_async_copy(wide_query, weight_query_all.at[own_block], local.at[1]),
        pltpu.make_async_copy(wide_key, weight_key_all.at[own_block], local.at[2]),
    ]
    for copy in own_copies:
        copy.start()

    def start_weight(i):
        weight_fs(0, f, ahead(i)).start()
        weight_fs(1, f, ahead(i)).start()

    each(1, fs, start_weight)

    def relay_basis(i):
        source = behind(i)
        for slot in (0, 1):
            basis_hop(source, slot, senders[slot]).wait_recv()
            basis_hop(source, slot + 2, owners[slot + 2]).start()

    def all_basis(i):
        for slot in (2, 3):
            basis_hop(behind(i), slot, senders[slot]).wait_recv()

    each(1, fs, relay_basis)
    each(1, fs, all_basis)
    own_basis.wait()
    for load in loads[2:]:
        load.wait()

    for t in range(0, tokens, LANES):
        value = jnp.dot(
            inputs[t : t + LANES, :], basis_all[c], preferred_element_type=jnp.float32
        )
        factor[c, :, t : t + LANES] = value.T.astype(jnp.bfloat16)
    for u in range(units, per * rep):
        part_send[u] = jnp.zeros(part_send.shape[1:], jnp.bfloat16)
    factor_copy = remote(
        factor.at[c], factor.at[c], pair_s.at[0], pair_r.at[0], tp=1 - c
    )
    factor_back = remote(
        factor.at[1 - c], factor.at[1 - c], pair_s.at[0], pair_r.at[0], tp=1 - c
    )
    factor_copy.start()
    swap = remote(basis_all.at[c], basis_all.at[c], pair_s.at[1], pair_r.at[1], tp=1 - c)
    swap_back = remote(
        basis_all.at[1 - c], basis_all.at[1 - c], pair_s.at[1], pair_r.at[1], tp=1 - c
    )
    factor_back.wait_recv()
    swap.start()

    for x, cot in ((0, cot_query), (1, cot_key)):
        columns = cot.shape[1]
        width = 2 * LANES if columns % (2 * LANES) == 0 else LANES
        for n in range(0, columns, width):
            value = jnp.dot(
                factor[x], cot[:, n : n + width], preferred_element_type=jnp.float32
            ).astype(jnp.bfloat16)
            for k in range(0, width, LANES):
                part_send[x * query_units + (n + k) // LANES] = value[:, k : k + LANES]

    def group(owner):
        return pl.ds(owner * per, per)

    def part_rep(source, target):
        return remote(
            part_send.at[group(target)],
            part_recv.at[source],
            bp_s.at[target],
            bp_r.at[source],
            rep=target,
        )

    each(1, rep, lambda j: part_rep(r, beside(j)).start())
    part_recv[r] = part_send[group(r)]
    each(1, rep, lambda j: part_rep(beside(j), beside(j)).wait_recv())
    for p in range(per):
        value = part_recv[0, p].astype(jnp.float32)
        for q in range(1, rep):
            value = value + part_recv[q, p].astype(jnp.float32)
        slab[p] = value.astype(jnp.bfloat16)

    def slab_fs(source, target):
        return remote(
            slab.at[:, low_rows(target)],
            slab_recv.at[source],
            bz_s.at[target],
            bz_r.at[source],
            fs=target,
        )

    each(1, fs, lambda i: slab_fs(f, ahead(i)).start())

    def spread_weight(i):
        source = behind(i)
        for x in range(2):
            weight_fs(x, source, source).wait_recv()
            for slot in (0, 1):
                weight_hop(x, source, slot, owners[slot]).start()

    def relay_weight(i):
        source = behind(i)
        for slot in (0, 1):
            for x in range(2):
                weight_hop(x, source, slot, senders[slot]).wait_recv()
                weight_hop(x, source, slot + 2, owners[slot + 2]).start()

    spread_weight(1)
    slab_recv[f] = slab[:, low_rows(f), :]
    each(1, fs, lambda i: slab_fs(behind(i), behind(i)).wait_recv())
    for p in range(per):
        value = slab_recv[0, p].astype(jnp.float32)
        for q in range(1, fs):
            value = value + slab_recv[q, p].astype(jnp.float32)
        low_all[r * per + p] = value.astype(jnp.bfloat16)

    def low_rep(owner, target):
        block = low_all.at[group(owner)]
        return remote(block, block, lp_s.at[target], lp_r.at[owner], rep=target)

    each(1, rep, lambda j: low_rep(r, beside(j)).start())
    each(1, rep, lambda j: low_rep(beside(j), beside(j)).wait_recv())

    for x, moments, direction, low_out in (
        (0, moments_query, dir_query, low_query),
        (1, moments_key, dir_key, low_key),
    ):
        total = jnp.zeros((8, LANES), jnp.float32)
        for n in range(0, moments.shape[2], LANES):
            span = slice(n, n + LANES)
            low = low_all[x * query_units + n // LANES].astype(jnp.float32)
            low_out[:, span] = low
            first = 0.9 * moments[0, :, span] + 0.1 * low
            second = 0.95 * moments[1, :, span] + 0.05 * low * low
            normed = first / (jnp.sqrt(second) + 1e-08)
            direction[low_rows(f), span] = normed.astype(jnp.bfloat16)
            total = total + jnp.sum((normed * normed).reshape(rows // 8, 8, LANES), axis=0)
        squares[f, x] = total

    directions = (dir_query, dir_key)

    right, left = ahead(1), behind(1)

    def move_right(x, source):
        block = directions[x].at[low_rows(source)]
        return remote(block, block, dr_s.at[x, source], dz_r.at[x, source], fs=right)

    def move_left(x, source):
        block = directions[x].at[low_rows(source)]
        return remote(block, block, dl_s.at[x, source], dz_r.at[x, source], fs=left)

    def squares_fs(source, target):
        block = squares.at[source]
        return remote(block, block, qz_s.at[target], qz_r.at[source], fs=target)

    each(1, fs, lambda i: squares_fs(f, ahead(i)).start())

    @pl.when(f + 1 < fs)
    def start_right():
        for x in range(2):
            move_right(x, f).start()

    @pl.when(f > 0)
    def start_left():
        for x in range(2):
            move_left(x, f).start()

    each(2, fs, spread_weight)

    def relay_direction(k):
        @pl.when(f - k >= 0)
        def from_left():
            for x in range(2):
                move_right(x, f - k).wait_recv()

                @pl.when(f + 1 < fs)
                def onward():
                    move_right(x, f - k).start()

        @pl.when(f + k < fs)
        def from_right():
            for x in range(2):
                move_left(x, f + k).wait_recv()

                @pl.when(f > 0)
                def onward():
                    move_left(x, f + k).start()

    def relay_both(k):
        relay_weight(k)
        relay_direction(k)

    each(1, fs, relay_both)

    each(1, fs, lambda i: squares_fs(behind(i), behind(i)).wait_recv())
    total = squares[0]
    for q in range(1, fs):
        total = total + squares[q]
    pair[c] = total
    total_copy = remote(pair.at[c], pair.at[c], pair_s.at[2], pair_r.at[2], tp=1 - c)
    total_back = remote(pair.at[1 - c], pair.at[1 - c], pair_s.at[2], pair_r.at[2], tp=1 - c)
    total_copy.start()
    total_back.wait_recv()
    totals[...] = pair[0] + pair[1]

    def end_fs(i):
        source, target = behind(i), ahead(i)
        for x in range(2):
            for slot in (2, 3):
                weight_hop(x, source, slot, senders[slot]).wait_recv()
            for slot in range(4):
                weight_hop(x, source, slot, owners[slot]).wait_send()
            weight_fs(x, f, target).wait_send()
        for slot in range(4):
            basis_hop(source, slot, owners[slot]).wait_send()
        basis_fs(0, f, target).wait_send()
        slab_fs(f, target).wait_send()
        squares_fs(f, target).wait_send()

    def end_direction(k):
        @pl.when((f - k >= 0) & (f + 1 < fs))
        def end_right():
            for x in range(2):
                move_right(x, f - k).wait_send()

        @pl.when((f + k < fs) & (f > 0))
        def end_left():
            for x in range(2):
                move_left(x, f + k).wait_send()

    def end_rep(j):
        part_rep(r, beside(j)).wait_send()
        low_rep(r, beside(j)).wait_send()

    each(1, fs, end_fs)
    each(0, fs, end_direction)
    each(1, rep, end_rep)
    swap_back.wait_recv()
    factor_copy.wait_send()
    swap.wait_send()
    total_copy.wait_send()
    for copy in own_copies:
        copy.wait()


def exchange_grid(
    fs,
    rep,
    inputs_far,
    cot_query_far,
    cot_key_far,
    basis_query,
    basis_key,
    full_query,
    full_key,
    moments_query_far,
    moments_key_far,
    step_query,
    step_key,
    new_weight_query,
    new_weight_key,
    copy_query,
    copy_key,
    new_moments_query,
    new_moments_key,
    basis_all,
    weight_query_all,
    weight_key_all,
    dir_query,
    dir_key,
    inputs,
    cot_query,
    cot_key,
    moments_query,
    moments_key,
    loaded_query,
    loaded_key,
    factor,
    part,
    got_first,
    pair_sum,
    got_second,
    slab,
    slab_recv,
    low_all,
    part_squares,
    squares,
    pair,
    late_query,
    late_key,
    line_s,
    key_s,
    basis_line_r,
    query_line_r,
    key_line_r,
    hop_s,
    basis_hop_r,
    query_hop_r,
    basis_end_r,
    query_end_r,
    halve_s,
    first_r,
    second_r,
    slab_s,
    slab_r,
    low_s,
    low_r,
    low_end_r,
    dir_s,
    dir_r,
    dir_hop_s,
    dir_hop_r,
    dir_end_r,
    squares_s,
    squares_r,
    pair_s,
    pair_r,
    local,
):
    f, r, c = lax.axis_index("fs"), lax.axis_index("rep"), lax.axis_index("tp")
    height, rank = basis_query.shape
    quarter = height // rep
    rows = rank // fs
    own = rows // rep
    tokens = inputs.shape[0]
    query_units = cot_query.shape[1] // LANES
    units = query_units + cot_key.shape[1] // LANES
    streams = ((0, units // 2), (units // 2, units // 2))
    f32, bf16 = jnp.float32, jnp.bfloat16

    near = r + 1 - 2 * lax.rem(r, 2)
    far = r + 2 - 4 * (r // 2)
    across = 3 - r

    def when(conds, body):
        if not conds:
            body()
            return
        test = conds[0]
        for cond in conds[1:]:
            test = test & cond
        pl.when(test)(body)

    def send(make, *conds):
        when(conds, lambda: make().start())

    def arrived(block, sem, *conds):
        when(conds, lambda: remote(block, block, sem, sem, tp=1 - c).wait_recv())

    def departed(block, sem, *conds):
        when(conds, lambda: remote(block, block, sem, sem, tp=1 - c).wait_send())

    def sources(d):
        return ((f - d, f >= d), (f + d, f + d < fs))

    def beside(j):
        return lax.rem(r + j, rep)

    def rows_of(start, size):
        return pl.ds(pl.multiple_of(start, size), size)

    chunks = 2
    chunk = quarter // chunks
    fine = basis_line_r.shape[1]

    def piece(source, owner, k, parts=chunks):
        size = quarter // parts
        return rows_of(source * height + owner * quarter + k * size, size)

    mirror = f // (fs // 2)
    place_in_half = f + mirror * (fs - 1 - 2 * f)

    def other(n):
        low_side = n - 1 + (n + fs - 1 - place_in_half) // fs
        return low_side + mirror * (fs - 1 - 2 * low_side)

    own_block = rows_of(f * height, height)

    loads = [
        pltpu.make_async_copy(source, target, local.at[1 + n])
        for n, (source, target) in enumerate(
            (
                (full_query, loaded_query),
                (full_key, loaded_key),
                (inputs_far, inputs),
                (cot_query_far, cot_query),
                (cot_key_far, cot_key),
                (moments_query_far, moments_query),
                (moments_key_far, moments_key),
            )
        )
    ]
    bases = (basis_query, basis_key)
    for x in range(2):

        @pl.when(c == x)
        def load_basis():
            pltpu.make_async_copy(bases[x], basis_all.at[c, own_block], local.at[0]).start()

    for load in loads:
        load.start()
    own_basis = pltpu.make_async_copy(basis_query, basis_all.at[c, own_block], local.at[0])
    barrier = pltpu.get_barrier_semaphore()
    for i in range(1, fs):
        pl.semaphore_signal(
            barrier, inc=1, device_id={"fs": lax.rem(f + i, fs)}, device_id_type=MESH
        )
    for mate in (near, far):
        pl.semaphore_signal(barrier, inc=1, device_id={"rep": mate}, device_id_type=MESH)
    pl.semaphore_signal(barrier, inc=1, device_id={"tp": 1 - c}, device_id_type=MESH)
    pl.semaphore_wait(barrier, fs + 2)

    def basis_z(source, up, k):
        block = basis_all.at[c, piece(source, r, k, fine)]
        return remote(block, block, line_s.at[0], basis_line_r.at[source, k], fs=f + 2 * up - 1)

    ways = ((1, f + 1 < fs), (0, f > 0))
    edge = (f == 0) | (f == fs - 1)
    inner = (f > 0) & (f < fs - 1)
    def hop_span(slot, width):
        return (pl.ds(0, width), pl.ds(0, width), pl.ds(0, width // 2), pl.ds(width // 2, width // 2))[slot]

    targets = (near, far, far, near)
    sent = (r, r, near, far)

    def basis_hop(k, source, slot):
        block = basis_all.at[c, piece(source, sent[slot], k, fine), hop_span(slot, rank)]
        landed = basis_hop_r.at[source, k] if slot < 2 else basis_end_r.at[0]
        return remote(block, block, hop_s.at[0], landed, rep=targets[slot])

    def weight_hop(k, source, slot):
        width = weight_query_all.shape[1]
        block = weight_query_all.at[piece(source, sent[slot], k), hop_span(slot, width)]
        landed = query_hop_r.at[source, k] if slot < 2 else query_end_r.at[source]
        return remote(block, block, hop_s.at[1], landed, rep=targets[slot])

    def spread(hop, source, *there):
        for slot in (0, 1):
            send(functools.partial(hop, source, slot), *there)

    def relay(hop, both, sem, source, *there):
        arrived(both, sem, *there)
        for slot in (2, 3):
            send(functools.partial(hop, source, slot), *there)

    def relay_basis(k, source, *there):
        both = basis_all.at[c, pl.ds(0, 2 * (quarter // fine))]
        relay(functools.partial(basis_hop, k), both, basis_hop_r.at[source, k], source, *there)

    def relay_weight(k, source):
        both = weight_query_all.at[pl.ds(0, 2 * chunk)]
        relay(functools.partial(weight_hop, k), both, query_hop_r.at[source, k], source)

    def query_z(source, up, k):
        block = weight_query_all.at[piece(source, r, k)]
        return remote(block, block, line_s.at[1], query_line_r.at[source, k], fs=f + 2 * up - 1)

    def key_z(source, up, k):
        size = height // chunks
        block = weight_key_all.at[rows_of(source * height + k * size, size)]
        return remote(block, block, key_s.at[up], key_line_r.at[source, k], fs=f + 2 * up - 1)

    def launch(line, parts=chunks):
        for k in range(parts):
            for up, there in ways:
                send(functools.partial(line, f, up, k), there)

    def onward(line, d, k, *conds):
        for source, there, up, more in (
            (f - d, f >= d, 1, f + 1 < fs),
            (f + d, f + d < fs, 0, f > 0),
        ):
            when((there, *conds), lambda: line(source, up, k).wait_recv())
            if d + 1 < fs:
                send(functools.partial(line, source, up, k), there, more, *conds)

    def onward_all(line, d, parts=chunks):
        for k in range(parts):
            onward(line, d, k)

    own_basis.wait()
    launch(basis_z, fine)
    for load in loads[:2]:
        load.wait()
    weight_query_all[own_block, :] = loaded_query[...].astype(bf16)
    weight_key_all[own_block, :] = loaded_key[...].astype(bf16)

    steps = [(d, k) for d in range(1, fs) for k in range(fine)]
    for n, (d, k) in enumerate(steps):
        onward(basis_z, d, k)
        for source, there in sources(d):
            spread(functools.partial(basis_hop, k), source, there)
        if (d, k) == (max(fs - 2, 1), fine - 1):
            launch(query_z)
        if n >= 6:
            before, j = steps[n - 6]
            for source, there in sources(before):
                relay_basis(j, source, there)
    for d, k in steps[-6:]:
        for source, there in sources(d):
            relay_basis(k, source, there)
    onward_all(query_z, 1)
    launch(key_z)
    spread(functools.partial(weight_hop, 0), other(1))
    spread(functools.partial(weight_hop, 1), other(1), c == 1)
    arrived(basis_all.at[c, pl.ds(0, (fs - 1) * quarter)], basis_end_r.at[0])
    for load in loads[2:]:
        load.wait()

    for t in range(0, tokens, LANES):
        value = jnp.dot(inputs[t : t + LANES, :], basis_all[c], preferred_element_type=f32)
        factor[c, :, t : t + LANES] = value.T.astype(bf16)

    def partner(block, back, n):
        return (
            remote(block, block, pair_s.at[n], pair_r.at[n], tp=1 - c),
            remote(back, back, pair_s.at[n], pair_r.at[n], tp=1 - c),
        )

    factor_copy, factor_back = partner(factor.at[c], factor.at[1 - c], 0)
    swap, swap_back = partner(basis_all.at[c], basis_all.at[1 - c], 1)
    factor_copy.start()
    factor_back.wait_recv()
    swap.start()

    for x, cot in ((0, cot_query), (1, cot_key)):
        columns = cot.shape[1]
        width = 2 * LANES if columns % (2 * LANES) == 0 else LANES
        for n in range(0, columns, width):
            value = jnp.dot(
                factor[x], cot[:, n : n + width], preferred_element_type=f32
            ).astype(bf16)
            for k in range(0, width, LANES):
                for q in range(rep):
                    for s in range(fs):
                        part[x * query_units + (n + k) // LANES, q, s * own : (s + 1) * own] = value[
                            s * rows + q * own : s * rows + (q + 1) * own, k : k + LANES
                        ]

    half = rows // 2
    spans = (slice(0, half), slice(half, rows))
    mates = ((near, far), (far, near))

    def columns_of(g):
        return pl.ds(streams[g][0], streams[g][1])

    def first_hop(h, g, w):
        owner = (across, mates[h][0])[w]
        return remote(
            part.at[columns_of(g), owner, pl.ds(h * half, half)],
            got_first.at[h, w, columns_of(g)],
            halve_s.at[0],
            (first_r, second_r)[w].at[g],
            rep=mates[h][0],
        )

    def second_hop(h, g):
        return remote(
            pair_sum.at[h, columns_of(g)],
            got_second.at[h, columns_of(g)],
            halve_s.at[1],
            second_r.at[g],
            rep=mates[h][1],
        )

    def start_first(g, w):
        for h in range(2):
            first_hop(h, g, w).start()

    def start_second(g):
        arrived(got_first.at[:, 0, columns_of(g)], first_r.at[g])
        for h in range(2):
            for u in range(streams[g][0], sum(streams[g])):
                pair_sum[h, u] = (
                    part[u, mates[h][1], spans[h]].astype(f32) + got_first[h, 0, u].astype(f32)
                ).astype(bf16)
            second_hop(h, g).start()

    def slab_z(g, source, target):
        return remote(
            slab.at[columns_of(g), rows_of(target * own, own)],
            slab_recv.at[source, columns_of(g)],
            slab_s.at[0],
            slab_r.at[g],
            fs=target,
        )

    def end_rep(g):
        arrived(got_first.at[:, :, columns_of(g)], second_r.at[g])
        for h in range(2):
            for u in range(streams[g][0], sum(streams[g])):
                slab[u, spans[h]] = (
                    part[u, r, spans[h]].astype(f32)
                    + got_first[h, 1, u].astype(f32)
                    + got_second[h, u].astype(f32)
                ).astype(bf16)
        for n in range(fs - 1, 0, -1):
            slab_z(g, f, other(n)).start()
        for u in range(streams[g][0], sum(streams[g])):
            slab_recv[f, u] = slab[u, rows_of(f * own, own)]

    start_first(0, 0)
    start_first(0, 1)
    start_first(1, 0)
    start_second(0)
    start_first(1, 1)
    start_second(1)
    spread(functools.partial(weight_hop, 1), other(1), c == 0)
    end_rep(0)
    end_rep(1)
    for k in range(chunks):
        when((edge,), lambda: query_z(other(2), 1, k).wait_recv())
        spread(functools.partial(weight_hop, k), other(2))

    directions, new_moments = (dir_query, dir_key), (new_moments_query, new_moments_key)
    moments = (moments_query, moments_key)

    def place(u):
        x = 0 if u < query_units else 1
        n = (u - x * query_units) * LANES
        return x, slice(n, n + LANES)

    def pieces(g):
        first, last = streams[g][0], sum(streams[g])
        found = []
        if first < query_units:
            found.append((0, first * LANES, (min(last, query_units) - first) * LANES))
        if last > query_units:
            start = max(first, query_units)
            found.append((1, (start - query_units) * LANES, (last - start) * LANES))
        return found

    def dir_rows(source, owner):
        return rows_of(source * rows + owner * own, own)

    def update(g, owner):
        sums = [jnp.zeros((8, LANES), f32), jnp.zeros((8, LANES), f32)]
        mine = rows_of(owner * own, own)
        for u in range(streams[g][0], sum(streams[g])):
            x, span = place(u)
            low = low_all[owner, u].astype(f32)
            first = 0.9 * moments[x][0, mine, span] + 0.1 * low
            second = 0.95 * moments[x][1, mine, span] + 0.05 * low * low
            new_moments[x][0, mine, span] = first
            new_moments[x][1, mine, span] = second
            normed = first / (jnp.sqrt(second) + 1e-08)
            directions[x][dir_rows(f, owner), span] = normed.astype(bf16)
            sums[x] = sums[x] + jnp.sum((normed * normed).reshape(own // 8, 8, LANES), axis=0)
        for x in range(2):
            part_squares[owner, g, x] = sums[x]

    def low_hop(g, slot):
        block = low_all.at[sent[slot], columns_of(g)]
        landed = low_r.at[g] if slot == g else low_end_r.at[0]
        return remote(block, block, low_s.at[0], landed, rep=targets[slot])

    def dir_blocks(g, source, owner):
        return [
            (x, directions[x].at[dir_rows(source, owner), pl.ds(start, size)])
            for x, start, size in pieces(g)
        ]

    def dir_line(g, source, up):
        for x, block in dir_blocks(g, source, r):
            remote(block, block, dir_s.at[x], dir_r.at[g, source], fs=f + 2 * up - 1).start()

    def dir_hop(g, slot, n):
        landed = dir_hop_r.at[n, g] if slot == g else dir_end_r.at[n]
        for x, block in dir_blocks(g, other(n), sent[slot]):
            remote(block, block, dir_hop_s.at[n], landed, rep=targets[slot]).start()

    def end_fs(g):
        arrived(slab_recv.at[pl.ds(0, fs - 1), columns_of(g)], slab_r.at[g])
        for u in range(streams[g][0], sum(streams[g])):
            value = slab_recv[0, u].astype(f32)
            for q in range(1, fs):
                value = value + slab_recv[q, u].astype(f32)
            low_all[r, u] = value.astype(bf16)
        for slot in (0, 1):
            low_hop(g, slot).start()
        update(g, r)
        for up, there in ways:
            when((there,), lambda: dir_line(g, f, up))

    end_fs(0)
    end_fs(1)

    def onward_dir(d):
        for g in range(2):
            for source, there, up, more in (
                (f - d, f >= d, 1, f + 1 < fs),
                (f + d, f + d < fs, 0, f > 0),
            ):
                arrived(low_all.at[r, columns_of(g)], dir_r.at[g, source], there)
                if d + 1 < fs:
                    when((there, more), lambda: dir_line(g, source, up))

    def spread_dir(n, *conds):
        for g in range(2):
            for slot in (0, 1):
                when(conds, lambda: dir_hop(g, slot, n))

    def relay_dir(n):
        for g in range(2):
            arrived(low_all.at[r, columns_of(g)], dir_hop_r.at[n, g])
            dir_hop(g, g + 2, n)

    def finish_dir(n):
        arrived(low_all.at[pl.ds(0, 2)], dir_end_r.at[n])

    for k in range(chunks):
        relay_weight(k, other(1))
    onward_dir(1)
    spread_dir(1)
    spread_dir(2, inner)
    for g in range(2):
        arrived(low_all.at[r, columns_of(g)], low_r.at[g])
        low_hop(g, g + 2).start()
    onward_dir(2)
    spread_dir(2, edge)
    spread_dir(3, inner)
    for k in range(chunks):
        onward(query_z, 2, k, inner)
    relay_dir(1)
    onward_dir(3)
    spread_dir(3, edge)
    arrived(low_all.at[pl.ds(0, 2)], low_end_r.at[0])
    for g in range(2):
        for j in range(1, rep):
            update(g, beside(j))
    for x in range(2):
        total = part_squares[0, 0, x] + part_squares[0, 1, x]
        for q in range(1, rep):
            total = total + (part_squares[q, 0, x] + part_squares[q, 1, x])
        squares[f, x] = total

    mine = squares.at[f]
    for n in range(1, fs):
        remote(mine, mine, squares_s.at[0], squares_r.at[0], fs=other(n)).start()
    onward_all(key_z, 1)
    relay_dir(2)
    relay_dir(3)
    for n in range(3, fs):
        for k in range(chunks):
            onward(query_z, n, k)
            spread(functools.partial(weight_hop, k), other(n))
    for k in range(chunks):
        relay_weight(k, other(2))
    def relay_last(k):
        for n in range(3, fs):
            relay_weight(k, other(n))

    def finish_weight(n):
        arrived(weight_query_all.at[pl.ds(0, quarter)], query_end_r.at[other(n)])

    arrived(squares.at[pl.ds(0, fs - 1)], squares_r.at[0])
    total = squares[0]
    for q in range(1, fs):
        total = total + squares[q]
    pair[c] = total
    total_copy, total_back = partner(pair.at[c], pair.at[1 - c], 2)
    total_copy.start()
    for d in range(1, fs):
        finish_dir(d)
    total_back.wait_recv()
    totals = pair[0] + pair[1]
    onward(key_z, 2, 0)
    weights_all, copies = (weight_query_all, weight_key_all), (copy_query, copy_key)
    scales = [
        lax.rsqrt(jnp.sum(totals[x], keepdims=True) / (pair.shape[0] * rank * copies[x].shape[1]) + 1e-06)
        for x in range(2)
    ]

    def product(x, span, columns):
        return scales[x] * jnp.dot(
            basis_all[x, span], directions[x][:, columns], preferred_element_type=f32
        )

    def column_blocks(x):
        wide = copies[x].shape[1]
        width = 2 * LANES if wide % (2 * LANES) == 0 else LANES
        return [slice(n, n + width) for n in range(0, wide, width)]

    def ahead_rows(x, start, size, held):
        for columns in column_blocks(x):
            held[pl.ds(0, size), columns] = 0.02 * product(x, rows_of(start, size), columns)

    def late_rows(x, start, size, held):
        span = rows_of(start, size)
        weight = weights_all[x][span].astype(f32)
        copies[x][span] = (weight - held[pl.ds(0, size)]).astype(bf16)

    def copy_rows(x, start, size):
        span = rows_of(start, size)
        for columns in column_blocks(x):
            weight = weights_all[x][span, columns].astype(f32)
            copies[x][span, columns] = (weight - 0.02 * product(x, span, columns)).astype(bf16)

    swap_back.wait_recv()
    for x, weight, step_out, new_out in (
        (0, loaded_query, step_query, new_weight_query),
        (1, loaded_key, step_key, new_weight_key),
    ):
        for columns in column_blocks(x):
            step = product(x, own_block, columns)
            step_out[:, columns] = step
            new = weight[:, columns] - 0.02 * step
            new_out[:, columns] = new
            copies[x][own_block, columns] = new.astype(bf16)

    finish_weight(1)
    copy_rows(0, other(1) * height, height)
    relay_last(0)
    onward(key_z, 2, 1)
    for n in (1, 2):
        copy_rows(1, other(n) * height, height)
    relay_last(1)
    for n in range(3, fs):
        for owner in (r, near, far):
            copy_rows(0, other(n) * height + owner * quarter, quarter)
    for n in range(3, fs):
        ahead_rows(0, other(n) * height + across * quarter, quarter, late_query)
        ahead_rows(1, other(n) * height, height, late_key)
    finish_weight(2)
    copy_rows(0, other(2) * height, height)
    for d in range(3, fs):
        onward_all(key_z, d)
    for n in range(3, fs):
        late_rows(1, other(n) * height, height, late_key)
    for n in range(3, fs):
        finish_weight(n)
        late_rows(0, other(n) * height + across * quarter, quarter, late_query)
    hops = (fs - 1) * (rep - 1) * quarter
    for n, block in ((0, basis_all.at[c]), (1, weight_query_all)):
        departed(block.at[pl.ds(0, quarter)], line_s.at[n], edge)
        departed(block.at[pl.ds(0, (fs + 1) * quarter)], line_s.at[n], inner)
        departed(block.at[pl.ds(0, hops)], hop_s.at[n])
    for n in range(fs):
        if n < fs - 1:
            departed(weight_key_all.at[pl.ds(0, (n + 1) * height)], key_s.at[1], f == n)
        if n > 0:
            departed(weight_key_all.at[pl.ds(0, (fs - n) * height)], key_s.at[0], f == n)
    departed(got_first, halve_s.at[0])
    departed(pair_sum, halve_s.at[1])
    departed(slab_recv.at[pl.ds(0, fs - 1)], slab_s.at[0])
    departed(low_all.at[pl.ds(0, rep - 1)], low_s.at[0])
    for x in range(2):
        departed(directions[x].at[pl.ds(0, own)], dir_s.at[x], edge)
        departed(directions[x].at[pl.ds(0, (fs + 1) * own)], dir_s.at[x], inner)
    for n in range(1, fs):
        departed(low_all.at[pl.ds(0, rep - 1)], dir_hop_s.at[n])
    departed(squares.at[pl.ds(0, fs - 1)], squares_s.at[0])
    for copy in (factor_copy, swap, total_copy):
        copy.wait_send()


def write_out(*refs):
    count = len(refs) // 2
    copies, starts = [], []
    for n, (source, target) in enumerate(zip(refs[:count], refs[count : 2 * count])):
        copies.append(pltpu.make_async_copy(source, target, refs[-1].at[n]))
        size = source.shape[0] // 4 if source.ndim == 2 else 1
        for start in range(0, source.shape[0], size):
            span = pl.ds(start, size)
            starts.append(pltpu.make_async_copy(source.at[span], target.at[span], refs[-1].at[n]))
    for copy in starts:
        copy.start()
    for copy in copies:
        copy.wait()


def apply(
    count_query,
    count_key,
    totals,
    dir_query,
    dir_key,
    low_query,
    low_key,
    moments_query,
    moments_key,
    basis_all,
    weight_query_all,
    weight_key_all,
    basis_query,
    basis_key,
    weight_query,
    weight_key,
    step_query,
    step_key,
    new_weight_query,
    new_weight_key,
    copy_query,
    copy_key,
    new_moments_query,
    new_moments_key,
):
    parts = (
        (count_query, dir_query, weight_query_all, basis_query, weight_query),
        (count_key, dir_key, weight_key_all, basis_key, weight_key),
    )
    outs = (
        (step_query, new_weight_query, copy_query),
        (step_key, new_weight_key, copy_key),
    )
    for x in range(2):
        count, direction, weight_all, basis, weight = parts[x]
        step_out, new_weight_out, copy_out = outs[x]
        scale = lax.rsqrt(jnp.sum(totals[x], keepdims=True) / count + 1e-06)
        step = scale * jnp.dot(basis[...], direction[...], preferred_element_type=jnp.float32)
        step_out[...] = step
        new_weight_out[...] = weight[...] - 0.02 * step
        whole = scale * jnp.dot(
            basis_all[x], direction[...], preferred_element_type=jnp.float32
        )
        copy_out[...] = (weight_all[...].astype(jnp.float32) - 0.02 * whole).astype(jnp.bfloat16)

    @pl.when(pl.program_id(0) == 0)
    def moments_once():
        for moments, low_ref, out in (
            (moments_query, low_query, new_moments_query),
            (moments_key, low_key, new_moments_key),
        ):
            low = low_ref[...]
            out[0] = 0.9 * moments[0] + 0.1 * low
            out[1] = 0.95 * moments[1] + 0.05 * low * low


def on_device(
    inputs,
    cot_query,
    cot_key,
    basis_query,
    basis_key,
    weight_query,
    weight_key,
    moments_query,
    moments_key,
):
    fs, rep, tp = lax.axis_size("fs"), lax.axis_size("rep"), lax.axis_size("tp")
    assert tp == 2 and rep == 4
    height, rank = basis_query.shape
    rows = rank // fs
    tokens = inputs.shape[0]
    query_cols, key_cols = cot_query.shape[1], cot_key.shape[1]
    per = -(-((query_cols + key_cols) // LANES) // rep)
    vmem = pl.BlockSpec(memory_space=pltpu.VMEM)
    hbm = pl.BlockSpec(memory_space=pl.ANY)
    bf16, f32 = jnp.bfloat16, jnp.float32
    dma = pltpu.SemaphoreType.DMA
    shape = jax.ShapeDtypeStruct
    owned = tuple(
        shape((height, columns), f32) for columns in (query_cols, key_cols, query_cols, key_cols)
    )
    results = owned + (
        shape((height * fs, query_cols), bf16),
        shape((height * fs, key_cols), bf16),
        shape((2, rows, query_cols), f32),
        shape((2, rows, key_cols), f32),
    )
    own, units = rows // rep, (query_cols + key_cols) // LANES
    if own % 16 == 0 and fs == 4 and units % 2 == 0:
        fresh = pl.pallas_call(
            functools.partial(exchange_grid, fs, rep),
            out_shape=results,
            in_specs=[pl.BlockSpec(memory_space=pltpu.HBM)] * 9,
            out_specs=(vmem,) * 8,
            scratch_shapes=[
                pltpu.VMEM((2, height * fs, rank), bf16),
                pltpu.VMEM((height * fs, query_cols), bf16),
                pltpu.VMEM((height * fs, key_cols), bf16),
                pltpu.VMEM((rank, query_cols), bf16),
                pltpu.VMEM((rank, key_cols), bf16),
                pltpu.VMEM((tokens, inputs.shape[1]), bf16),
                pltpu.VMEM((tokens, query_cols), bf16),
                pltpu.VMEM((tokens, key_cols), bf16),
                pltpu.VMEM((2, rows, query_cols), f32),
                pltpu.VMEM((2, rows, key_cols), f32),
                pltpu.VMEM((height, query_cols), f32),
                pltpu.VMEM((height, key_cols), f32),
                pltpu.VMEM((2, rank, tokens), bf16),
                pltpu.VMEM((units, rep, rows, LANES), bf16),
                pltpu.VMEM((2, 2, units, rows // 2, LANES), bf16),
                pltpu.VMEM((2, units, rows // 2, LANES), bf16),
                pltpu.VMEM((2, units, rows // 2, LANES), bf16),
                pltpu.VMEM((units, rows, LANES), bf16),
                pltpu.VMEM((fs, units, own, LANES), bf16),
                pltpu.VMEM((rep, units, own, LANES), bf16),
                pltpu.VMEM((rep, 2, 2, 8, LANES), f32),
                pltpu.VMEM((fs, 2, 8, LANES), f32),
                pltpu.VMEM((2, 2, 8, LANES), f32),
                pltpu.VMEM((height // rep, query_cols), f32),
                pltpu.VMEM((height, key_cols), f32),
                dma((2,)),
                dma((2,)),
                dma((fs, 4)),
                dma((fs, 2)),
                dma((fs, 2)),
                dma((2,)),
                dma((fs, 4)),
                dma((fs, 2)),
                dma((1,)),
                dma((fs,)),
                dma((2,)),
                dma((2,)),
                dma((2,)),
                dma((1,)),
                dma((2,)),
                dma((1,)),
                dma((2,)),
                dma((1,)),
                dma((2,)),
                dma((2, fs)),
                dma((fs,)),
                dma((fs, 2)),
                dma((fs,)),
                dma((1,)),
                dma((1,)),
                dma((3,)),
                dma((3,)),
                dma((8,)),
            ],
            compiler_params=pltpu.CompilerParams(
                collective_id=0, has_side_effects=True, vmem_limit_bytes=40 * 1024 * 1024
            ),
        )(
            *(
                pltpu.with_memory_space_constraint(operand, pltpu.HBM)
                for operand in (
                    inputs,
                    cot_query,
                    cot_key,
                    basis_query,
                    basis_key,
                    weight_query,
                    weight_key,
                    moments_query,
                    moments_key,
                )
            )
        )
        return pl.pallas_call(
            write_out,
            out_shape=results,
            in_specs=[vmem] * 8,
            out_specs=(hbm,) * 8,
            scratch_shapes=[dma((8,))],
            compiler_params=pltpu.CompilerParams(vmem_limit_bytes=32 * 1024 * 1024),
        )(*fresh)

    (
        basis_all,
        weight_query_all,
        weight_key_all,
        dir_query,
        dir_key,
        low_query,
        low_key,
        totals,
    ) = pl.pallas_call(
        functools.partial(exchange, fs, rep),
        out_shape=(
            shape((2, height * fs, rank), bf16),
            shape((height * fs, query_cols), bf16),
            shape((height * fs, key_cols), bf16),
            shape((rank, query_cols), bf16),
            shape((rank, key_cols), bf16),
            shape((rows, query_cols), f32),
            shape((rows, key_cols), f32),
            shape((2, 8, LANES), f32),
        ),
        in_specs=[pl.BlockSpec(memory_space=pltpu.HBM)] * 9,
        out_specs=(vmem, hbm, hbm, vmem, vmem, vmem, vmem, vmem),
        scratch_shapes=[
            pltpu.VMEM((tokens, inputs.shape[1]), bf16),
            pltpu.VMEM((tokens, query_cols), bf16),
            pltpu.VMEM((tokens, key_cols), bf16),
            pltpu.VMEM((2, rows, query_cols), f32),
            pltpu.VMEM((2, rows, key_cols), f32),
            pltpu.VMEM((height, query_cols), f32),
            pltpu.VMEM((height, key_cols), f32),
            pltpu.VMEM((height, query_cols), bf16),
            pltpu.VMEM((height, key_cols), bf16),
            pltpu.VMEM((2, rank, tokens), bf16),
            pltpu.VMEM((per * rep, rank, LANES), bf16),
            pltpu.VMEM((rep, per, rank, LANES), bf16),
            pltpu.VMEM((per, rank, LANES), bf16),
            pltpu.VMEM((fs, per, rows, LANES), bf16),
            pltpu.VMEM((per * rep, rows, LANES), bf16),
            pltpu.VMEM((fs, 2, 8, LANES), f32),
            pltpu.VMEM((2, 2, 8, LANES), f32),
            dma((fs,)),
            dma((fs,)),
            dma((fs, rep)),
            dma((fs, rep)),
            dma((2, fs)),
            dma((2, fs)),
            dma((2, fs, rep)),
            dma((2, fs, rep)),
            dma((rep,)),
            dma((rep,)),
            dma((fs,)),
            dma((fs,)),
            dma((rep,)),
            dma((rep,)),
            dma((2, fs)),
            dma((2, fs)),
            dma((2, fs)),
            dma((fs,)),
            dma((fs,)),
            dma((3,)),
            dma((3,)),
            dma((10,)),
        ],
        compiler_params=pltpu.CompilerParams(
            collective_id=0, has_side_effects=True, vmem_limit_bytes=32 * 1024 * 1024
        ),
    )(
        *(
            pltpu.with_memory_space_constraint(operand, pltpu.HBM)
            for operand in (
                inputs,
                cot_query,
                cot_key,
                basis_query,
                basis_key,
                weight_query,
                weight_key,
                moments_query,
                moments_key,
            )
        )
    )

    steps = min(8, height // 16)
    tall, short = height * fs // steps, height // steps

    def fixed(*dims):
        return pl.BlockSpec(dims, lambda i: (0,) * len(dims))

    def banded(*dims):
        return pl.BlockSpec(dims, lambda i: (i, 0))

    owned_specs = tuple(
        banded(short, columns) for columns in (query_cols, key_cols, query_cols, key_cols)
    )
    return pl.pallas_call(
        functools.partial(
            apply, float(rank * query_cols * tp), float(rank * key_cols * tp)
        ),
        grid=(steps,),
        out_shape=results,
        in_specs=[
            fixed(2, 8, LANES),
            fixed(rank, query_cols),
            fixed(rank, key_cols),
            fixed(rows, query_cols),
            fixed(rows, key_cols),
            fixed(2, rows, query_cols),
            fixed(2, rows, key_cols),
            pl.BlockSpec((2, tall, rank), lambda i: (0, i, 0)),
            banded(tall, query_cols),
            banded(tall, key_cols),
            banded(short, rank),
            banded(short, rank),
            banded(short, query_cols),
            banded(short, key_cols),
        ],
        out_specs=owned_specs
        + (
            banded(tall, query_cols),
            banded(tall, key_cols),
            fixed(2, rows, query_cols),
            fixed(2, rows, key_cols),
        ),
        compiler_params=pltpu.CompilerParams(
            dimension_semantics=("arbitrary",), vmem_limit_bytes=32 * 1024 * 1024
        ),
    )(
        totals,
        dir_query,
        dir_key,
        low_query,
        low_key,
        moments_query,
        moments_key,
        basis_all,
        weight_query_all,
        weight_key_all,
        basis_query,
        basis_key,
        weight_query,
        weight_key,
    )


def solution(mesh):
    in_specs = (
        P(("fs", "rep"), None),
        P(("fs", "rep"), "tp"),
        P(("fs", "rep"), "tp"),
        P("fs", None),
        P("fs", None),
        P("fs", "tp"),
        P("fs", "tp"),
        P(None, "fs", "tp"),
        P(None, "fs", "tp"),
    )
    out_specs = (
        P("fs", "tp"),
        P("fs", "tp"),
        P("fs", "tp"),
        P("fs", "tp"),
        P(None, "tp"),
        P(None, "tp"),
        P(None, "fs", "tp"),
        P(None, "fs", "tp"),
    )
    return jax.shard_map(
        on_device, mesh=mesh, in_specs=in_specs, out_specs=out_specs, check_vma=False
    )
```

```python
import functools
import jax
import jax.numpy as jnp
from jax import lax
from jax.experimental import pallas as pl
from jax.experimental.pallas import tpu as pltpu
from jax.sharding import PartitionSpec as P

MESH = pl.DeviceIdType.MESH
LANES = 128


def each(start, stop, body):
    if stop - start <= 4:
        for i in range(start, stop):
            body(i)
    else:
        lax.fori_loop(start, stop, lambda i, carry: (body(i), carry)[1], 0)


def remote(src, dst, send_sem, recv_sem, **device):
    return pltpu.make_async_remote_copy(
        src_ref=src,
        dst_ref=dst,
        send_sem=send_sem,
        recv_sem=recv_sem,
        device_id=device,
        device_id_type=MESH,
    )


def exchange(
    fs,
    rep,
    inputs_far,
    cot_query_far,
    cot_key_far,
    basis_query,
    basis_key,
    full_query,
    full_key,
    moments_query_far,
    moments_key_far,
    basis_all,
    weight_query_all,
    weight_key_all,
    dir_query,
    dir_key,
    low_query,
    low_key,
    totals,
    inputs,
    cot_query,
    cot_key,
    moments_query,
    moments_key,
    loaded_query,
    loaded_key,
    wide_query,
    wide_key,
    factor,
    part_send,
    part_recv,
    slab,
    slab_recv,
    low_all,
    squares,
    pair,
    az_s,
    az_r,
    ap_s,
    ap_r,
    ez_s,
    ez_r,
    ep_s,
    ep_r,
    bp_s,
    bp_r,
    bz_s,
    bz_r,
    lp_s,
    lp_r,
    dr_s,
    dl_s,
    dz_r,
    qz_s,
    qz_r,
    pair_s,
    pair_r,
    local,
):
    f, r, c = lax.axis_index("fs"), lax.axis_index("rep"), lax.axis_index("tp")
    height = basis_query.shape[0]
    part = height // rep
    rank = basis_query.shape[1]
    rows = rank // fs
    tokens = inputs.shape[0]
    per = part_send.shape[0] // rep
    query_units = cot_query.shape[1] // LANES
    units = query_units + cot_key.shape[1] // LANES

    def ahead(i):
        return lax.rem(f + i, fs)

    def behind(i):
        return lax.rem(f + fs - i, fs)

    def beside(j):
        return lax.rem(r + j, rep)

    near = r + 1 - 2 * lax.rem(r, 2)
    far = r + 2 - 4 * (r // 2)
    across = 3 - r
    owners = (r, r, near, far)
    targets = (near, far, far, near)
    senders = (near, far, across, across)

    def span_of(slot, width):
        return (pl.ds(0, width), pl.ds(0, width), pl.ds(0, width // 2), pl.ds(width // 2, width // 2))[slot]

    def piece(source, owner):
        return pl.ds(pl.multiple_of(source * height + owner * part, part), part)

    own_part = pl.ds(pl.multiple_of(r * part, part), part)
    own_block = pl.ds(pl.multiple_of(f * height, height), height)

    def low_rows(source):
        return pl.ds(pl.multiple_of(source * rows, rows), rows)

    loads = [
        pltpu.make_async_copy(source, target, local.at[3 + n])
        for n, (source, target) in enumerate(
            (
                (full_query, loaded_query),
                (full_key, loaded_key),
                (inputs_far, inputs),
                (cot_query_far, cot_query),
                (cot_key_far, cot_key),
                (moments_query_far, moments_query),
                (moments_key_far, moments_key),
            )
        )
    ]
    barrier = pltpu.get_barrier_semaphore()

    def greet_fs(i):
        pl.semaphore_signal(barrier, inc=1, device_id={"fs": ahead(i)}, device_id_type=MESH)

    def greet_rep(j):
        pl.semaphore_signal(barrier, inc=1, device_id={"rep": beside(j)}, device_id_type=MESH)

    each(1, fs, greet_fs)
    each(1, rep, greet_rep)
    pl.semaphore_signal(barrier, inc=1, device_id={"tp": 1 - c}, device_id_type=MESH)
    pl.semaphore_wait(barrier, fs + rep - 1)

    bases = (basis_query, basis_key)
    weights = ((wide_query, weight_query_all), (wide_key, weight_key_all))

    def basis_fs(x, source, target):
        return remote(
            bases[x].at[own_part],
            basis_all.at[c, piece(source, r)],
            az_s.at[target],
            az_r.at[source],
            fs=target,
        )

    for x in range(2):

        @pl.when(c == x)
        def start_basis():
            each(1, fs, lambda i: basis_fs(x, f, ahead(i)).start())
            pltpu.make_async_copy(bases[x], basis_all.at[c, own_block], local.at[0]).start()

    for load in loads:
        load.start()
    own_basis = pltpu.make_async_copy(basis_query, basis_all.at[c, own_block], local.at[0])

    def basis_hop(source, slot, owner):
        block = basis_all.at[c, piece(source, owner), span_of(slot, rank)]
        return remote(
            block, block, ap_s.at[source, slot], ap_r.at[source, slot], rep=targets[slot]
        )

    def weight_fs(x, source, target):
        return remote(
            weights[x][0].at[own_part],
            weights[x][1].at[piece(source, r)],
            ez_s.at[x, target],
            ez_r.at[x, source],
            fs=target,
        )

    def weight_hop(x, source, slot, owner):
        block = weights[x][1].at[piece(source, owner), span_of(slot, weights[x][1].shape[1])]
        return remote(
            block, block, ep_s.at[x, source, slot], ep_r.at[x, source, slot], rep=targets[slot]
        )

    for load in loads[:2]:
        load.wait()
    wide_query[...] = loaded_query[...].astype(jnp.bfloat16)
    wide_key[...] = loaded_key[...].astype(jnp.bfloat16)

    def spread_basis(i):
        source = behind(i)
        basis_fs(0, source, source).wait_recv()
        for slot in (0, 1):
            basis_hop(source, slot, owners[slot]).start()

    each(1, fs, spread_basis)

    own_copies = [
        pltpu.make_async_copy(wide_query, weight_query_all.at[own_block], local.at[1]),
        pltpu.make_async_copy(wide_key, weight_key_all.at[own_block], local.at[2]),
    ]
    for copy in own_copies:
        copy.start()

    def start_weight(i):
        weight_fs(0, f, ahead(i)).start()
        weight_fs(1, f, ahead(i)).start()

    each(1, fs, start_weight)

    def relay_basis(i):
        source = behind(i)
        for slot in (0, 1):
            basis_hop(source, slot, senders[slot]).wait_recv()
            basis_hop(source, slot + 2, owners[slot + 2]).start()

    def all_basis(i):
        for slot in (2, 3):
            basis_hop(behind(i), slot, senders[slot]).wait_recv()

    each(1, fs, relay_basis)
    each(1, fs, all_basis)
    own_basis.wait()
    for load in loads[2:]:
        load.wait()

    for t in range(0, tokens, LANES):
        value = jnp.dot(
            inputs[t : t + LANES, :], basis_all[c], preferred_element_type=jnp.float32
        )
        factor[c, :, t : t + LANES] = value.T.astype(jnp.bfloat16)
    for u in range(units, per * rep):
        part_send[u] = jnp.zeros(part_send.shape[1:], jnp.bfloat16)
    factor_copy = remote(
        factor.at[c], factor.at[c], pair_s.at[0], pair_r.at[0], tp=1 - c
    )
    factor_back = remote(
        factor.at[1 - c], factor.at[1 - c], pair_s.at[0], pair_r.at[0], tp=1 - c
    )
    factor_copy.start()
    swap = remote(basis_all.at[c], basis_all.at[c], pair_s.at[1], pair_r.at[1], tp=1 - c)
    swap_back = remote(
        basis_all.at[1 - c], basis_all.at[1 - c], pair_s.at[1], pair_r.at[1], tp=1 - c
    )
    factor_back.wait_recv()
    swap.start()

    for x, cot in ((0, cot_query), (1, cot_key)):
        columns = cot.shape[1]
        width = 2 * LANES if columns % (2 * LANES) == 0 else LANES
        for n in range(0, columns, width):
            value = jnp.dot(
                factor[x], cot[:, n : n + width], preferred_element_type=jnp.float32
            ).astype(jnp.bfloat16)
            for k in range(0, width, LANES):
                part_send[x * query_units + (n + k) // LANES] = value[:, k : k + LANES]

    def group(owner):
        return pl.ds(owner * per, per)

    def part_rep(source, target):
        return remote(
            part_send.at[group(target)],
            part_recv.at[source],
            bp_s.at[target],
            bp_r.at[source],
            rep=target,
        )

    each(1, rep, lambda j: part_rep(r, beside(j)).start())
    part_recv[r] = part_send[group(r)]
    each(1, rep, lambda j: part_rep(beside(j), beside(j)).wait_recv())
    for p in range(per):
        value = part_recv[0, p].astype(jnp.float32)
        for q in range(1, rep):
            value = value + part_recv[q, p].astype(jnp.float32)
        slab[p] = value.astype(jnp.bfloat16)

    def slab_fs(source, target):
        return remote(
            slab.at[:, low_rows(target)],
            slab_recv.at[source],
            bz_s.at[target],
            bz_r.at[source],
            fs=target,
        )

    each(1, fs, lambda i: slab_fs(f, ahead(i)).start())

    def spread_weight(i):
        source = behind(i)
        for x in range(2):
            weight_fs(x, source, source).wait_recv()
            for slot in (0, 1):
                weight_hop(x, source, slot, owners[slot]).start()

    def relay_weight(i):
        source = behind(i)
        for slot in (0, 1):
            for x in range(2):
                weight_hop(x, source, slot, senders[slot]).wait_recv()
                weight_hop(x, source, slot + 2, owners[slot + 2]).start()

    spread_weight(1)
    slab_recv[f] = slab[:, low_rows(f), :]
    each(1, fs, lambda i: slab_fs(behind(i), behind(i)).wait_recv())
    for p in range(per):
        value = slab_recv[0, p].astype(jnp.float32)
        for q in range(1, fs):
            value = value + slab_recv[q, p].astype(jnp.float32)
        low_all[r * per + p] = value.astype(jnp.bfloat16)

    def low_rep(owner, target):
        block = low_all.at[group(owner)]
        return remote(block, block, lp_s.at[target], lp_r.at[owner], rep=target)

    each(1, rep, lambda j: low_rep(r, beside(j)).start())
    each(1, rep, lambda j: low_rep(beside(j), beside(j)).wait_recv())

    for x, moments, direction, low_out in (
        (0, moments_query, dir_query, low_query),
        (1, moments_key, dir_key, low_key),
    ):
        total = jnp.zeros((8, LANES), jnp.float32)
        for n in range(0, moments.shape[2], LANES):
            span = slice(n, n + LANES)
            low = low_all[x * query_units + n // LANES].astype(jnp.float32)
            low_out[:, span] = low
            first = 0.9 * moments[0, :, span] + 0.1 * low
            second = 0.95 * moments[1, :, span] + 0.05 * low * low
            normed = first / (jnp.sqrt(second) + 1e-08)
            direction[low_rows(f), span] = normed.astype(jnp.bfloat16)
            total = total + jnp.sum((normed * normed).reshape(rows // 8, 8, LANES), axis=0)
        squares[f, x] = total

    directions = (dir_query, dir_key)

    right, left = ahead(1), behind(1)

    def move_right(x, source):
        block = directions[x].at[low_rows(source)]
        return remote(block, block, dr_s.at[x, source], dz_r.at[x, source], fs=right)

    def move_left(x, source):
        block = directions[x].at[low_rows(source)]
        return remote(block, block, dl_s.at[x, source], dz_r.at[x, source], fs=left)

    def squares_fs(source, target):
        block = squares.at[source]
        return remote(block, block, qz_s.at[target], qz_r.at[source], fs=target)

    each(1, fs, lambda i: squares_fs(f, ahead(i)).start())

    @pl.when(f + 1 < fs)
    def start_right():
        for x in range(2):
            move_right(x, f).start()

    @pl.when(f > 0)
    def start_left():
        for x in range(2):
            move_left(x, f).start()

    each(2, fs, spread_weight)

    def relay_direction(k):
        @pl.when(f - k >= 0)
        def from_left():
            for x in range(2):
                move_right(x, f - k).wait_recv()

                @pl.when(f + 1 < fs)
                def onward():
                    move_right(x, f - k).start()

        @pl.when(f + k < fs)
        def from_right():
            for x in range(2):
                move_left(x, f + k).wait_recv()

                @pl.when(f > 0)
                def onward():
                    move_left(x, f + k).start()

    def relay_both(k):
        relay_weight(k)
        relay_direction(k)

    each(1, fs, relay_both)

    each(1, fs, lambda i: squares_fs(behind(i), behind(i)).wait_recv())
    total = squares[0]
    for q in range(1, fs):
        total = total + squares[q]
    pair[c] = total
    total_copy = remote(pair.at[c], pair.at[c], pair_s.at[2], pair_r.at[2], tp=1 - c)
    total_back = remote(pair.at[1 - c], pair.at[1 - c], pair_s.at[2], pair_r.at[2], tp=1 - c)
    total_copy.start()
    total_back.wait_recv()
    totals[...] = pair[0] + pair[1]

    def end_fs(i):
        source, target = behind(i), ahead(i)
        for x in range(2):
            for slot in (2, 3):
                weight_hop(x, source, slot, senders[slot]).wait_recv()
            for slot in range(4):
                weight_hop(x, source, slot, owners[slot]).wait_send()
            weight_fs(x, f, target).wait_send()
        for slot in range(4):
            basis_hop(source, slot, owners[slot]).wait_send()
        basis_fs(0, f, target).wait_send()
        slab_fs(f, target).wait_send()
        squares_fs(f, target).wait_send()

    def end_direction(k):
        @pl.when((f - k >= 0) & (f + 1 < fs))
        def end_right():
            for x in range(2):
                move_right(x, f - k).wait_send()

        @pl.when((f + k < fs) & (f > 0))
        def end_left():
            for x in range(2):
                move_left(x, f + k).wait_send()

    def end_rep(j):
        part_rep(r, beside(j)).wait_send()
        low_rep(r, beside(j)).wait_send()

    each(1, fs, end_fs)
    each(0, fs, end_direction)
    each(1, rep, end_rep)
    swap_back.wait_recv()
    factor_copy.wait_send()
    swap.wait_send()
    total_copy.wait_send()
    for copy in own_copies:
        copy.wait()


def exchange_grid(
    fs,
    rep,
    inputs_far,
    cot_query_far,
    cot_key_far,
    basis_query,
    basis_key,
    full_query,
    full_key,
    moments_query_far,
    moments_key_far,
    step_query,
    step_key,
    new_weight_query,
    new_weight_key,
    copy_query,
    copy_key,
    new_moments_query,
    new_moments_key,
    basis_all,
    weight_query_all,
    weight_key_all,
    dir_query,
    dir_key,
    inputs,
    cot_query,
    cot_key,
    moments_query,
    moments_key,
    loaded_query,
    loaded_key,
    factor,
    part,
    got_first,
    pair_sum,
    got_second,
    slab,
    slab_recv,
    low_all,
    part_squares,
    squares,
    pair,
    late_query,
    late_key,
    line_s,
    key_s,
    basis_line_r,
    query_line_r,
    key_line_r,
    hop_s,
    basis_hop_r,
    query_hop_r,
    basis_end_r,
    query_end_r,
    halve_s,
    first_r,
    second_r,
    slab_s,
    slab_r,
    low_s,
    low_r,
    low_end_r,
    dir_s,
    dir_r,
    dir_hop_s,
    dir_hop_r,
    dir_end_r,
    squares_s,
    squares_r,
    pair_s,
    pair_r,
    local,
):
    f, r, c = lax.axis_index("fs"), lax.axis_index("rep"), lax.axis_index("tp")
    height, rank = basis_query.shape
    quarter = height // rep
    rows = rank // fs
    own = rows // rep
    tokens = inputs.shape[0]
    query_units = cot_query.shape[1] // LANES
    units = query_units + cot_key.shape[1] // LANES
    streams = ((0, units // 2), (units // 2, units // 2))
    f32, bf16 = jnp.float32, jnp.bfloat16

    near = r + 1 - 2 * lax.rem(r, 2)
    far = r + 2 - 4 * (r // 2)
    across = 3 - r

    def when(conds, body):
        if not conds:
            body()
            return
        test = conds[0]
        for cond in conds[1:]:
            test = test & cond
        pl.when(test)(body)

    def send(make, *conds):
        when(conds, lambda: make().start())

    def arrived(block, sem, *conds):
        when(conds, lambda: remote(block, block, sem, sem, tp=1 - c).wait_recv())

    def departed(block, sem, *conds):
        when(conds, lambda: remote(block, block, sem, sem, tp=1 - c).wait_send())

    def sources(d):
        return ((f - d, f >= d), (f + d, f + d < fs))

    def beside(j):
        return lax.rem(r + j, rep)

    def rows_of(start, size):
        return pl.ds(pl.multiple_of(start, size), size)

    chunks = 2
    chunk = quarter // chunks
    fine = basis_line_r.shape[1]

    def piece(source, owner, k, parts=chunks):
        size = quarter // parts
        return rows_of(source * height + owner * quarter + k * size, size)

    mirror = f // (fs // 2)
    place_in_half = f + mirror * (fs - 1 - 2 * f)

    def other(n):
        low_side = n - 1 + (n + fs - 1 - place_in_half) // fs
        return low_side + mirror * (fs - 1 - 2 * low_side)

    own_block = rows_of(f * height, height)

    loads = [
        pltpu.make_async_copy(source, target, local.at[1 + n])
        for n, (source, target) in enumerate(
            (
                (full_query, loaded_query),
                (full_key, loaded_key),
                (inputs_far, inputs),
                (cot_query_far, cot_query),
                (cot_key_far, cot_key),
                (moments_query_far, moments_query),
                (moments_key_far, moments_key),
            )
        )
    ]
    bases = (basis_query, basis_key)
    for x in range(2):

        @pl.when(c == x)
        def load_basis():
            pltpu.make_async_copy(bases[x], basis_all.at[c, own_block], local.at[0]).start()

    for load in loads:
        load.start()
    own_basis = pltpu.make_async_copy(basis_query, basis_all.at[c, own_block], local.at[0])
    ways = ((1, f + 1 < fs), (0, f > 0))
    edge = (f == 0) | (f == fs - 1)
    inner = (f > 0) & (f < fs - 1)
    barrier = pltpu.get_barrier_semaphore()

    def greet(up):
        pl.semaphore_signal(
            barrier, inc=1, device_id={"fs": f + 2 * up - 1}, device_id_type=MESH
        )

    for up, there in ways:
        when((there,), functools.partial(greet, up))
    for mate in (near, far):
        pl.semaphore_signal(barrier, inc=1, device_id={"rep": mate}, device_id_type=MESH)
    pl.semaphore_signal(barrier, inc=1, device_id={"tp": 1 - c}, device_id_type=MESH)
    when((edge,), lambda: pl.semaphore_wait(barrier, 4))
    when((inner,), lambda: pl.semaphore_wait(barrier, 5))

    def basis_z(source, up, k):
        block = basis_all.at[c, piece(source, r, k, fine)]
        return remote(block, block, line_s.at[0], basis_line_r.at[source, k], fs=f + 2 * up - 1)

    def hop_span(slot, width):
        return (pl.ds(0, width), pl.ds(0, width), pl.ds(0, width // 2), pl.ds(width // 2, width // 2))[slot]

    targets = (near, far, far, near)
    sent = (r, r, near, far)

    def basis_hop(k, source, slot):
        block = basis_all.at[c, piece(source, sent[slot], k, fine), hop_span(slot, rank)]
        landed = basis_hop_r.at[source, k] if slot < 2 else basis_end_r.at[0]
        return remote(block, block, hop_s.at[0], landed, rep=targets[slot])

    def weight_hop(k, source, slot):
        width = weight_query_all.shape[1]
        block = weight_query_all.at[piece(source, sent[slot], k), hop_span(slot, width)]
        landed = query_hop_r.at[source, k] if slot < 2 else query_end_r.at[source]
        return remote(block, block, hop_s.at[1], landed, rep=targets[slot])

    def spread(hop, source, *there):
        for slot in (0, 1):
            send(functools.partial(hop, source, slot), *there)

    def relay(hop, both, sem, source, *there):
        arrived(both, sem, *there)
        for slot in (2, 3):
            send(functools.partial(hop, source, slot), *there)

    def relay_basis(k, source, *there):
        both = basis_all.at[c, pl.ds(0, 2 * (quarter // fine))]
        relay(functools.partial(basis_hop, k), both, basis_hop_r.at[source, k], source, *there)

    def relay_weight(k, source):
        both = weight_query_all.at[pl.ds(0, 2 * chunk)]
        relay(functools.partial(weight_hop, k), both, query_hop_r.at[source, k], source)

    def query_z(source, up, k):
        block = weight_query_all.at[piece(source, r, k)]
        return remote(block, block, line_s.at[1], query_line_r.at[source, k], fs=f + 2 * up - 1)

    def key_z(source, up, k):
        size = height // chunks
        block = weight_key_all.at[rows_of(source * height + k * size, size)]
        return remote(block, block, key_s.at[up], key_line_r.at[source, k], fs=f + 2 * up - 1)

    def launch(line, parts=chunks):
        for k in range(parts):
            for up, there in ways:
                send(functools.partial(line, f, up, k), there)

    def onward(line, d, k, *conds):
        for source, there, up, more in (
            (f - d, f >= d, 1, f + 1 < fs),
            (f + d, f + d < fs, 0, f > 0),
        ):
            when((there, *conds), lambda: line(source, up, k).wait_recv())
            if d + 1 < fs:
                send(functools.partial(line, source, up, k), there, more, *conds)

    def onward_all(line, d, parts=chunks):
        for k in range(parts):
            onward(line, d, k)

    own_basis.wait()
    launch(basis_z, fine)
    for load in loads[:2]:
        load.wait()
    weight_query_all[own_block, :] = loaded_query[...].astype(bf16)
    weight_key_all[own_block, :] = loaded_key[...].astype(bf16)

    steps = [(d, k) for d in range(1, fs) for k in range(fine)]
    for n, (d, k) in enumerate(steps):
        onward(basis_z, d, k)
        for source, there in sources(d):
            spread(functools.partial(basis_hop, k), source, there)
        if (d, k) == (max(fs - 2, 1), fine - 1):
            launch(query_z)
        if n >= 6:
            before, j = steps[n - 6]
            for source, there in sources(before):
                relay_basis(j, source, there)
    for d, k in steps[-6:]:
        for source, there in sources(d):
            relay_basis(k, source, there)
    onward_all(query_z, 1)
    launch(key_z)
    spread(functools.partial(weight_hop, 0), other(1))
    spread(functools.partial(weight_hop, 1), other(1), c == 1)
    arrived(basis_all.at[c, pl.ds(0, (fs - 1) * quarter)], basis_end_r.at[0])
    for load in loads[2:]:
        load.wait()

    for t in range(0, tokens, LANES):
        value = jnp.dot(inputs[t : t + LANES, :], basis_all[c], preferred_element_type=f32)
        factor[c, :, t : t + LANES] = value.T.astype(bf16)

    def partner(block, back, n):
        return (
            remote(block, block, pair_s.at[n], pair_r.at[n], tp=1 - c),
            remote(back, back, pair_s.at[n], pair_r.at[n], tp=1 - c),
        )

    factor_copy, factor_back = partner(factor.at[c], factor.at[1 - c], 0)
    swap, swap_back = partner(basis_all.at[c], basis_all.at[1 - c], 1)
    factor_copy.start()
    factor_back.wait_recv()
    swap.start()

    for x, cot in ((0, cot_query), (1, cot_key)):
        columns = cot.shape[1]
        width = 2 * LANES if columns % (2 * LANES) == 0 else LANES
        for n in range(0, columns, width):
            value = jnp.dot(
                factor[x], cot[:, n : n + width], preferred_element_type=f32
            ).astype(bf16)
            for k in range(0, width, LANES):
                for q in range(rep):
                    for s in range(fs):
                        part[x * query_units + (n + k) // LANES, q, s * own : (s + 1) * own] = value[
                            s * rows + q * own : s * rows + (q + 1) * own, k : k + LANES
                        ]

    half = rows // 2
    spans = (slice(0, half), slice(half, rows))
    mates = ((near, far), (far, near))

    def columns_of(g):
        return pl.ds(streams[g][0], streams[g][1])

    def first_hop(h, g, w):
        owner = (across, mates[h][0])[w]
        return remote(
            part.at[columns_of(g), owner, pl.ds(h * half, half)],
            got_first.at[h, w, columns_of(g)],
            halve_s.at[0],
            (first_r, second_r)[w].at[g],
            rep=mates[h][0],
        )

    def second_hop(h, g):
        return remote(
            pair_sum.at[h, columns_of(g)],
            got_second.at[h, columns_of(g)],
            halve_s.at[1],
            second_r.at[g],
            rep=mates[h][1],
        )

    def start_first(g, w):
        for h in range(2):
            first_hop(h, g, w).start()

    def start_second(g):
        arrived(got_first.at[:, 0, columns_of(g)], first_r.at[g])
        for h in range(2):
            for u in range(streams[g][0], sum(streams[g])):
                pair_sum[h, u] = (
                    part[u, mates[h][1], spans[h]].astype(f32) + got_first[h, 0, u].astype(f32)
                ).astype(bf16)
            second_hop(h, g).start()

    def slab_z(g, source, target):
        return remote(
            slab.at[columns_of(g), rows_of(target * own, own)],
            slab_recv.at[source, columns_of(g)],
            slab_s.at[0],
            slab_r.at[g],
            fs=target,
        )

    def end_rep(g):
        arrived(got_first.at[:, :, columns_of(g)], second_r.at[g])
        for h in range(2):
            for u in range(streams[g][0], sum(streams[g])):
                slab[u, spans[h]] = (
                    part[u, r, spans[h]].astype(f32)
                    + got_first[h, 1, u].astype(f32)
                    + got_second[h, u].astype(f32)
                ).astype(bf16)
        for n in range(fs - 1, 0, -1):
            slab_z(g, f, other(n)).start()
        for u in range(streams[g][0], sum(streams[g])):
            slab_recv[f, u] = slab[u, rows_of(f * own, own)]

    start_first(0, 0)
    start_first(0, 1)
    start_first(1, 0)
    start_second(0)
    start_first(1, 1)
    start_second(1)
    spread(functools.partial(weight_hop, 1), other(1), c == 0)
    end_rep(0)
    end_rep(1)
    for k in range(chunks):
        when((edge,), lambda: query_z(other(2), 1, k).wait_recv())
        spread(functools.partial(weight_hop, k), other(2))

    directions, new_moments = (dir_query, dir_key), (new_moments_query, new_moments_key)
    moments = (moments_query, moments_key)

    def place(u):
        x = 0 if u < query_units else 1
        n = (u - x * query_units) * LANES
        return x, slice(n, n + LANES)

    def pieces(g):
        first, last = streams[g][0], sum(streams[g])
        found = []
        if first < query_units:
            found.append((0, first * LANES, (min(last, query_units) - first) * LANES))
        if last > query_units:
            start = max(first, query_units)
            found.append((1, (start - query_units) * LANES, (last - start) * LANES))
        return found

    def dir_rows(source, owner):
        return rows_of(source * rows + owner * own, own)

    def update(g, owner):
        sums = [jnp.zeros((8, LANES), f32), jnp.zeros((8, LANES), f32)]
        mine = rows_of(owner * own, own)
        for u in range(streams[g][0], sum(streams[g])):
            x, span = place(u)
            low = low_all[owner, u].astype(f32)
            first = 0.9 * moments[x][0, mine, span] + 0.1 * low
            second = 0.95 * moments[x][1, mine, span] + 0.05 * low * low
            new_moments[x][0, mine, span] = first
            new_moments[x][1, mine, span] = second
            normed = first / (jnp.sqrt(second) + 1e-08)
            directions[x][dir_rows(f, owner), span] = normed.astype(bf16)
            sums[x] = sums[x] + jnp.sum((normed * normed).reshape(own // 8, 8, LANES), axis=0)
        for x in range(2):
            part_squares[owner, g, x] = sums[x]

    def low_hop(g, slot):
        block = low_all.at[sent[slot], columns_of(g)]
        landed = low_r.at[g] if slot == g else low_end_r.at[0]
        return remote(block, block, low_s.at[0], landed, rep=targets[slot])

    def dir_blocks(g, source, owner):
        return [
            (x, directions[x].at[dir_rows(source, owner), pl.ds(start, size)])
            for x, start, size in pieces(g)
        ]

    def dir_line(g, source, up):
        for x, block in dir_blocks(g, source, r):
            remote(block, block, dir_s.at[x], dir_r.at[g, source], fs=f + 2 * up - 1).start()

    def dir_hop(g, slot, n):
        landed = dir_hop_r.at[n, g] if slot == g else dir_end_r.at[n]
        for x, block in dir_blocks(g, other(n), sent[slot]):
            remote(block, block, dir_hop_s.at[n], landed, rep=targets[slot]).start()

    def end_fs(g):
        arrived(slab_recv.at[pl.ds(0, fs - 1), columns_of(g)], slab_r.at[g])
        for u in range(streams[g][0], sum(streams[g])):
            value = slab_recv[0, u].astype(f32)
            for q in range(1, fs):
                value = value + slab_recv[q, u].astype(f32)
            low_all[r, u] = value.astype(bf16)
        for slot in (0, 1):
            low_hop(g, slot).start()
        update(g, r)
        for up, there in ways:
            when((there,), lambda: dir_line(g, f, up))

    end_fs(0)
    end_fs(1)

    def onward_dir(d):
        for g in range(2):
            for source, there, up, more in (
                (f - d, f >= d, 1, f + 1 < fs),
                (f + d, f + d < fs, 0, f > 0),
            ):
                arrived(low_all.at[r, columns_of(g)], dir_r.at[g, source], there)
                if d + 1 < fs:
                    when((there, more), lambda: dir_line(g, source, up))

    def spread_dir(n, *conds):
        for g in range(2):
            for slot in (0, 1):
                when(conds, lambda: dir_hop(g, slot, n))

    def relay_dir(n):
        for g in range(2):
            arrived(low_all.at[r, columns_of(g)], dir_hop_r.at[n, g])
            dir_hop(g, g + 2, n)

    def finish_dir(n):
        arrived(low_all.at[pl.ds(0, 2)], dir_end_r.at[n])

    for k in range(chunks):
        relay_weight(k, other(1))
    onward_dir(1)
    spread_dir(1)
    spread_dir(2, inner)
    for g in range(2):
        arrived(low_all.at[r, columns_of(g)], low_r.at[g])
        low_hop(g, g + 2).start()
    onward_dir(2)
    spread_dir(2, edge)
    spread_dir(3, inner)
    for k in range(chunks):
        onward(query_z, 2, k, inner)
    relay_dir(1)
    onward_dir(3)
    spread_dir(3, edge)
    arrived(low_all.at[pl.ds(0, 2)], low_end_r.at[0])
    for g in range(2):
        for j in range(1, rep):
            update(g, beside(j))
    for x in range(2):
        total = part_squares[0, 0, x] + part_squares[0, 1, x]
        for q in range(1, rep):
            total = total + (part_squares[q, 0, x] + part_squares[q, 1, x])
        squares[f, x] = total

    mine = squares.at[f]
    for n in range(1, fs):
        remote(mine, mine, squares_s.at[0], squares_r.at[0], fs=other(n)).start()
    onward_all(key_z, 1)
    relay_dir(2)
    relay_dir(3)
    relay_weight(0, other(2))
    for n in range(3, fs):
        for k in range(chunks):
            onward(query_z, n, k)
            spread(functools.partial(weight_hop, k), other(n))
    relay_weight(1, other(2))
    def relay_last(k):
        for n in range(3, fs):
            relay_weight(k, other(n))

    def finish_weight(n):
        arrived(weight_query_all.at[pl.ds(0, quarter)], query_end_r.at[other(n)])

    arrived(squares.at[pl.ds(0, fs - 1)], squares_r.at[0])
    total = squares[0]
    for q in range(1, fs):
        total = total + squares[q]
    pair[c] = total
    total_copy, total_back = partner(pair.at[c], pair.at[1 - c], 2)
    total_copy.start()
    for d in range(1, fs):
        finish_dir(d)
    total_back.wait_recv()
    totals = pair[0] + pair[1]
    onward(key_z, 2, 0)
    weights_all, copies = (weight_query_all, weight_key_all), (copy_query, copy_key)
    scales = [
        lax.rsqrt(jnp.sum(totals[x], keepdims=True) / (pair.shape[0] * rank * copies[x].shape[1]) + 1e-06)
        for x in range(2)
    ]

    def product(x, span, columns):
        return scales[x] * jnp.dot(
            basis_all[x, span], directions[x][:, columns], preferred_element_type=f32
        )

    def column_blocks(x):
        wide = copies[x].shape[1]
        width = 2 * LANES if wide % (2 * LANES) == 0 else LANES
        return [slice(n, n + width) for n in range(0, wide, width)]

    def ahead_rows(x, start, size, held):
        for columns in column_blocks(x):
            held[pl.ds(0, size), columns] = 0.02 * product(x, rows_of(start, size), columns)

    def late_rows(x, start, size, held):
        span = rows_of(start, size)
        weight = weights_all[x][span].astype(f32)
        copies[x][span] = (weight - held[pl.ds(0, size)]).astype(bf16)

    def copy_rows(x, start, size):
        span = rows_of(start, size)
        for columns in column_blocks(x):
            weight = weights_all[x][span, columns].astype(f32)
            copies[x][span, columns] = (weight - 0.02 * product(x, span, columns)).astype(bf16)

    swap_back.wait_recv()
    for x, weight, step_out, new_out in (
        (0, loaded_query, step_query, new_weight_query),
        (1, loaded_key, step_key, new_weight_key),
    ):
        for columns in column_blocks(x):
            step = product(x, own_block, columns)
            step_out[:, columns] = step
            new = weight[:, columns] - 0.02 * step
            new_out[:, columns] = new
            copies[x][own_block, columns] = new.astype(bf16)

    finish_weight(1)
    copy_rows(0, other(1) * height, height)
    relay_last(0)
    onward(key_z, 2, 1)
    for n in (1, 2):
        copy_rows(1, other(n) * height, height)
    relay_last(1)
    for n in range(3, fs):
        for owner in (r, near, far):
            copy_rows(0, other(n) * height + owner * quarter, quarter)
    for n in range(3, fs):
        ahead_rows(0, other(n) * height + across * quarter, quarter, late_query)
        ahead_rows(1, other(n) * height, height, late_key)
    finish_weight(2)
    copy_rows(0, other(2) * height, height)
    for d in range(3, fs):
        onward_all(key_z, d)
    for n in range(3, fs):
        late_rows(1, other(n) * height, height, late_key)
    for n in range(3, fs):
        finish_weight(n)
        late_rows(0, other(n) * height + across * quarter, quarter, late_query)
    hops = (fs - 1) * (rep - 1) * quarter
    for n, block in ((0, basis_all.at[c]), (1, weight_query_all)):
        departed(block.at[pl.ds(0, quarter)], line_s.at[n], edge)
        departed(block.at[pl.ds(0, (fs + 1) * quarter)], line_s.at[n], inner)
        departed(block.at[pl.ds(0, hops)], hop_s.at[n])
    for n in range(fs):
        if n < fs - 1:
            departed(weight_key_all.at[pl.ds(0, (n + 1) * height)], key_s.at[1], f == n)
        if n > 0:
            departed(weight_key_all.at[pl.ds(0, (fs - n) * height)], key_s.at[0], f == n)
    departed(got_first, halve_s.at[0])
    departed(pair_sum, halve_s.at[1])
    departed(slab_recv.at[pl.ds(0, fs - 1)], slab_s.at[0])
    departed(low_all.at[pl.ds(0, rep - 1)], low_s.at[0])
    for x in range(2):
        departed(directions[x].at[pl.ds(0, own)], dir_s.at[x], edge)
        departed(directions[x].at[pl.ds(0, (fs + 1) * own)], dir_s.at[x], inner)
    for n in range(1, fs):
        departed(low_all.at[pl.ds(0, rep - 1)], dir_hop_s.at[n])
    departed(squares.at[pl.ds(0, fs - 1)], squares_s.at[0])
    for copy in (factor_copy, swap, total_copy):
        copy.wait_send()


def write_out(*refs):
    count = len(refs) // 2
    copies, starts = [], []
    for n, (source, target) in enumerate(zip(refs[:count], refs[count : 2 * count])):
        copies.append(pltpu.make_async_copy(source, target, refs[-1].at[n]))
        size = source.shape[0] // 4 if source.ndim == 2 else 1
        for start in range(0, source.shape[0], size):
            span = pl.ds(start, size)
            starts.append(pltpu.make_async_copy(source.at[span], target.at[span], refs[-1].at[n]))
    for copy in starts:
        copy.start()
    for copy in copies:
        copy.wait()


def apply(
    count_query,
    count_key,
    totals,
    dir_query,
    dir_key,
    low_query,
    low_key,
    moments_query,
    moments_key,
    basis_all,
    weight_query_all,
    weight_key_all,
    basis_query,
    basis_key,
    weight_query,
    weight_key,
    step_query,
    step_key,
    new_weight_query,
    new_weight_key,
    copy_query,
    copy_key,
    new_moments_query,
    new_moments_key,
):
    parts = (
        (count_query, dir_query, weight_query_all, basis_query, weight_query),
        (count_key, dir_key, weight_key_all, basis_key, weight_key),
    )
    outs = (
        (step_query, new_weight_query, copy_query),
        (step_key, new_weight_key, copy_key),
    )
    for x in range(2):
        count, direction, weight_all, basis, weight = parts[x]
        step_out, new_weight_out, copy_out = outs[x]
        scale = lax.rsqrt(jnp.sum(totals[x], keepdims=True) / count + 1e-06)
        step = scale * jnp.dot(basis[...], direction[...], preferred_element_type=jnp.float32)
        step_out[...] = step
        new_weight_out[...] = weight[...] - 0.02 * step
        whole = scale * jnp.dot(
            basis_all[x], direction[...], preferred_element_type=jnp.float32
        )
        copy_out[...] = (weight_all[...].astype(jnp.float32) - 0.02 * whole).astype(jnp.bfloat16)

    @pl.when(pl.program_id(0) == 0)
    def moments_once():
        for moments, low_ref, out in (
            (moments_query, low_query, new_moments_query),
            (moments_key, low_key, new_moments_key),
        ):
            low = low_ref[...]
            out[0] = 0.9 * moments[0] + 0.1 * low
            out[1] = 0.95 * moments[1] + 0.05 * low * low


def on_device(
    inputs,
    cot_query,
    cot_key,
    basis_query,
    basis_key,
    weight_query,
    weight_key,
    moments_query,
    moments_key,
):
    fs, rep, tp = lax.axis_size("fs"), lax.axis_size("rep"), lax.axis_size("tp")
    assert tp == 2 and rep == 4
    height, rank = basis_query.shape
    rows = rank // fs
    tokens = inputs.shape[0]
    query_cols, key_cols = cot_query.shape[1], cot_key.shape[1]
    per = -(-((query_cols + key_cols) // LANES) // rep)
    vmem = pl.BlockSpec(memory_space=pltpu.VMEM)
    hbm = pl.BlockSpec(memory_space=pl.ANY)
    bf16, f32 = jnp.bfloat16, jnp.float32
    dma = pltpu.SemaphoreType.DMA
    shape = jax.ShapeDtypeStruct
    owned = tuple(
        shape((height, columns), f32) for columns in (query_cols, key_cols, query_cols, key_cols)
    )
    results = owned + (
        shape((height * fs, query_cols), bf16),
        shape((height * fs, key_cols), bf16),
        shape((2, rows, query_cols), f32),
        shape((2, rows, key_cols), f32),
    )
    own, units = rows // rep, (query_cols + key_cols) // LANES
    if own % 16 == 0 and fs == 4 and units % 2 == 0:
        fresh = pl.pallas_call(
            functools.partial(exchange_grid, fs, rep),
            out_shape=results,
            in_specs=[pl.BlockSpec(memory_space=pltpu.HBM)] * 9,
            out_specs=(vmem,) * 8,
            scratch_shapes=[
                pltpu.VMEM((2, height * fs, rank), bf16),
                pltpu.VMEM((height * fs, query_cols), bf16),
                pltpu.VMEM((height * fs, key_cols), bf16),
                pltpu.VMEM((rank, query_cols), bf16),
                pltpu.VMEM((rank, key_cols), bf16),
                pltpu.VMEM((tokens, inputs.shape[1]), bf16),
                pltpu.VMEM((tokens, query_cols), bf16),
                pltpu.VMEM((tokens, key_cols), bf16),
                pltpu.VMEM((2, rows, query_cols), f32),
                pltpu.VMEM((2, rows, key_cols), f32),
                pltpu.VMEM((height, query_cols), f32),
                pltpu.VMEM((height, key_cols), f32),
                pltpu.VMEM((2, rank, tokens), bf16),
                pltpu.VMEM((units, rep, rows, LANES), bf16),
                pltpu.VMEM((2, 2, units, rows // 2, LANES), bf16),
                pltpu.VMEM((2, units, rows // 2, LANES), bf16),
                pltpu.VMEM((2, units, rows // 2, LANES), bf16),
                pltpu.VMEM((units, rows, LANES), bf16),
                pltpu.VMEM((fs, units, own, LANES), bf16),
                pltpu.VMEM((rep, units, own, LANES), bf16),
                pltpu.VMEM((rep, 2, 2, 8, LANES), f32),
                pltpu.VMEM((fs, 2, 8, LANES), f32),
                pltpu.VMEM((2, 2, 8, LANES), f32),
                pltpu.VMEM((height // rep, query_cols), f32),
                pltpu.VMEM((height, key_cols), f32),
                dma((2,)),
                dma((2,)),
                dma((fs, 4)),
                dma((fs, 2)),
                dma((fs, 2)),
                dma((2,)),
                dma((fs, 4)),
                dma((fs, 2)),
                dma((1,)),
                dma((fs,)),
                dma((2,)),
                dma((2,)),
                dma((2,)),
                dma((1,)),
                dma((2,)),
                dma((1,)),
                dma((2,)),
                dma((1,)),
                dma((2,)),
                dma((2, fs)),
                dma((fs,)),
                dma((fs, 2)),
                dma((fs,)),
                dma((1,)),
                dma((1,)),
                dma((3,)),
                dma((3,)),
                dma((8,)),
            ],
            compiler_params=pltpu.CompilerParams(
                collective_id=0, has_side_effects=True, vmem_limit_bytes=40 * 1024 * 1024
            ),
        )(
            *(
                pltpu.with_memory_space_constraint(operand, pltpu.HBM)
                for operand in (
                    inputs,
                    cot_query,
                    cot_key,
                    basis_query,
                    basis_key,
                    weight_query,
                    weight_key,
                    moments_query,
                    moments_key,
                )
            )
        )
        return pl.pallas_call(
            write_out,
            out_shape=results,
            in_specs=[vmem] * 8,
            out_specs=(hbm,) * 8,
            scratch_shapes=[dma((8,))],
            compiler_params=pltpu.CompilerParams(vmem_limit_bytes=32 * 1024 * 1024),
        )(*fresh)

    (
        basis_all,
        weight_query_all,
        weight_key_all,
        dir_query,
        dir_key,
        low_query,
        low_key,
        totals,
    ) = pl.pallas_call(
        functools.partial(exchange, fs, rep),
        out_shape=(
            shape((2, height * fs, rank), bf16),
            shape((height * fs, query_cols), bf16),
            shape((height * fs, key_cols), bf16),
            shape((rank, query_cols), bf16),
            shape((rank, key_cols), bf16),
            shape((rows, query_cols), f32),
            shape((rows, key_cols), f32),
            shape((2, 8, LANES), f32),
        ),
        in_specs=[pl.BlockSpec(memory_space=pltpu.HBM)] * 9,
        out_specs=(vmem, hbm, hbm, vmem, vmem, vmem, vmem, vmem),
        scratch_shapes=[
            pltpu.VMEM((tokens, inputs.shape[1]), bf16),
            pltpu.VMEM((tokens, query_cols), bf16),
            pltpu.VMEM((tokens, key_cols), bf16),
            pltpu.VMEM((2, rows, query_cols), f32),
            pltpu.VMEM((2, rows, key_cols), f32),
            pltpu.VMEM((height, query_cols), f32),
            pltpu.VMEM((height, key_cols), f32),
            pltpu.VMEM((height, query_cols), bf16),
            pltpu.VMEM((height, key_cols), bf16),
            pltpu.VMEM((2, rank, tokens), bf16),
            pltpu.VMEM((per * rep, rank, LANES), bf16),
            pltpu.VMEM((rep, per, rank, LANES), bf16),
            pltpu.VMEM((per, rank, LANES), bf16),
            pltpu.VMEM((fs, per, rows, LANES), bf16),
            pltpu.VMEM((per * rep, rows, LANES), bf16),
            pltpu.VMEM((fs, 2, 8, LANES), f32),
            pltpu.VMEM((2, 2, 8, LANES), f32),
            dma((fs,)),
            dma((fs,)),
            dma((fs, rep)),
            dma((fs, rep)),
            dma((2, fs)),
            dma((2, fs)),
            dma((2, fs, rep)),
            dma((2, fs, rep)),
            dma((rep,)),
            dma((rep,)),
            dma((fs,)),
            dma((fs,)),
            dma((rep,)),
            dma((rep,)),
            dma((2, fs)),
            dma((2, fs)),
            dma((2, fs)),
            dma((fs,)),
            dma((fs,)),
            dma((3,)),
            dma((3,)),
            dma((10,)),
        ],
        compiler_params=pltpu.CompilerParams(
            collective_id=0, has_side_effects=True, vmem_limit_bytes=32 * 1024 * 1024
        ),
    )(
        *(
            pltpu.with_memory_space_constraint(operand, pltpu.HBM)
            for operand in (
                inputs,
                cot_query,
                cot_key,
                basis_query,
                basis_key,
                weight_query,
                weight_key,
                moments_query,
                moments_key,
            )
        )
    )

    steps = min(8, height // 16)
    tall, short = height * fs // steps, height // steps

    def fixed(*dims):
        return pl.BlockSpec(dims, lambda i: (0,) * len(dims))

    def banded(*dims):
        return pl.BlockSpec(dims, lambda i: (i, 0))

    owned_specs = tuple(
        banded(short, columns) for columns in (query_cols, key_cols, query_cols, key_cols)
    )
    return pl.pallas_call(
        functools.partial(
            apply, float(rank * query_cols * tp), float(rank * key_cols * tp)
        ),
        grid=(steps,),
        out_shape=results,
        in_specs=[
            fixed(2, 8, LANES),
            fixed(rank, query_cols),
            fixed(rank, key_cols),
            fixed(rows, query_cols),
            fixed(rows, key_cols),
            fixed(2, rows, query_cols),
            fixed(2, rows, key_cols),
            pl.BlockSpec((2, tall, rank), lambda i: (0, i, 0)),
            banded(tall, query_cols),
            banded(tall, key_cols),
            banded(short, rank),
            banded(short, rank),
            banded(short, query_cols),
            banded(short, key_cols),
        ],
        out_specs=owned_specs
        + (
            banded(tall, query_cols),
            banded(tall, key_cols),
            fixed(2, rows, query_cols),
            fixed(2, rows, key_cols),
        ),
        compiler_params=pltpu.CompilerParams(
            dimension_semantics=("arbitrary",), vmem_limit_bytes=32 * 1024 * 1024
        ),
    )(
        totals,
        dir_query,
        dir_key,
        low_query,
        low_key,
        moments_query,
        moments_key,
        basis_all,
        weight_query_all,
        weight_key_all,
        basis_query,
        basis_key,
        weight_query,
        weight_key,
    )


def solution(mesh):
    in_specs = (
        P(("fs", "rep"), None),
        P(("fs", "rep"), "tp"),
        P(("fs", "rep"), "tp"),
        P("fs", None),
        P("fs", None),
        P("fs", "tp"),
        P("fs", "tp"),
        P(None, "fs", "tp"),
        P(None, "fs", "tp"),
    )
    out_specs = (
        P("fs", "tp"),
        P("fs", "tp"),
        P("fs", "tp"),
        P("fs", "tp"),
        P(None, "tp"),
        P(None, "tp"),
        P(None, "fs", "tp"),
        P(None, "fs", "tp"),
    )
    return jax.shard_map(
        on_device, mesh=mesh, in_specs=in_specs, out_specs=out_specs, check_vma=False
    )
```

```python
import functools
import jax
import jax.numpy as jnp
from jax import lax
from jax.experimental import pallas as pl
from jax.experimental.pallas import tpu as pltpu
from jax.sharding import PartitionSpec as P

MESH = pl.DeviceIdType.MESH
LANES = 128


def each(start, stop, body):
    if stop - start <= 4:
        for i in range(start, stop):
            body(i)
    else:
        lax.fori_loop(start, stop, lambda i, carry: (body(i), carry)[1], 0)


def remote(src, dst, send_sem, recv_sem, **device):
    return pltpu.make_async_remote_copy(
        src_ref=src,
        dst_ref=dst,
        send_sem=send_sem,
        recv_sem=recv_sem,
        device_id=device,
        device_id_type=MESH,
    )


def exchange(
    fs,
    rep,
    inputs_far,
    cot_query_far,
    cot_key_far,
    basis_query,
    basis_key,
    full_query,
    full_key,
    moments_query_far,
    moments_key_far,
    basis_all,
    weight_query_all,
    weight_key_all,
    dir_query,
    dir_key,
    low_query,
    low_key,
    totals,
    inputs,
    cot_query,
    cot_key,
    moments_query,
    moments_key,
    loaded_query,
    loaded_key,
    wide_query,
    wide_key,
    factor,
    part_send,
    part_recv,
    slab,
    slab_recv,
    low_all,
    squares,
    pair,
    az_s,
    az_r,
    ap_s,
    ap_r,
    ez_s,
    ez_r,
    ep_s,
    ep_r,
    bp_s,
    bp_r,
    bz_s,
    bz_r,
    lp_s,
    lp_r,
    dr_s,
    dl_s,
    dz_r,
    qz_s,
    qz_r,
    pair_s,
    pair_r,
    local,
):
    f, r, c = lax.axis_index("fs"), lax.axis_index("rep"), lax.axis_index("tp")
    height = basis_query.shape[0]
    part = height // rep
    rank = basis_query.shape[1]
    rows = rank // fs
    tokens = inputs.shape[0]
    per = part_send.shape[0] // rep
    query_units = cot_query.shape[1] // LANES
    units = query_units + cot_key.shape[1] // LANES

    def ahead(i):
        return lax.rem(f + i, fs)

    def behind(i):
        return lax.rem(f + fs - i, fs)

    def beside(j):
        return lax.rem(r + j, rep)

    near = r + 1 - 2 * lax.rem(r, 2)
    far = r + 2 - 4 * (r // 2)
    across = 3 - r
    owners = (r, r, near, far)
    targets = (near, far, far, near)
    senders = (near, far, across, across)

    def span_of(slot, width):
        return (pl.ds(0, width), pl.ds(0, width), pl.ds(0, width // 2), pl.ds(width // 2, width // 2))[slot]

    def piece(source, owner):
        return pl.ds(pl.multiple_of(source * height + owner * part, part), part)

    own_part = pl.ds(pl.multiple_of(r * part, part), part)
    own_block = pl.ds(pl.multiple_of(f * height, height), height)

    def low_rows(source):
        return pl.ds(pl.multiple_of(source * rows, rows), rows)

    loads = [
        pltpu.make_async_copy(source, target, local.at[3 + n])
        for n, (source, target) in enumerate(
            (
                (full_query, loaded_query),
                (full_key, loaded_key),
                (inputs_far, inputs),
                (cot_query_far, cot_query),
                (cot_key_far, cot_key),
                (moments_query_far, moments_query),
                (moments_key_far, moments_key),
            )
        )
    ]
    barrier = pltpu.get_barrier_semaphore()

    def greet_fs(i):
        pl.semaphore_signal(barrier, inc=1, device_id={"fs": ahead(i)}, device_id_type=MESH)

    def greet_rep(j):
        pl.semaphore_signal(barrier, inc=1, device_id={"rep": beside(j)}, device_id_type=MESH)

    each(1, fs, greet_fs)
    each(1, rep, greet_rep)
    pl.semaphore_signal(barrier, inc=1, device_id={"tp": 1 - c}, device_id_type=MESH)
    pl.semaphore_wait(barrier, fs + rep - 1)

    bases = (basis_query, basis_key)
    weights = ((wide_query, weight_query_all), (wide_key, weight_key_all))

    def basis_fs(x, source, target):
        return remote(
            bases[x].at[own_part],
            basis_all.at[c, piece(source, r)],
            az_s.at[target],
            az_r.at[source],
            fs=target,
        )

    for x in range(2):

        @pl.when(c == x)
        def start_basis():
            each(1, fs, lambda i: basis_fs(x, f, ahead(i)).start())
            pltpu.make_async_copy(bases[x], basis_all.at[c, own_block], local.at[0]).start()

    for load in loads:
        load.start()
    own_basis = pltpu.make_async_copy(basis_query, basis_all.at[c, own_block], local.at[0])

    def basis_hop(source, slot, owner):
        block = basis_all.at[c, piece(source, owner), span_of(slot, rank)]
        return remote(
            block, block, ap_s.at[source, slot], ap_r.at[source, slot], rep=targets[slot]
        )

    def weight_fs(x, source, target):
        return remote(
            weights[x][0].at[own_part],
            weights[x][1].at[piece(source, r)],
            ez_s.at[x, target],
            ez_r.at[x, source],
            fs=target,
        )

    def weight_hop(x, source, slot, owner):
        block = weights[x][1].at[piece(source, owner), span_of(slot, weights[x][1].shape[1])]
        return remote(
            block, block, ep_s.at[x, source, slot], ep_r.at[x, source, slot], rep=targets[slot]
        )

    for load in loads[:2]:
        load.wait()
    wide_query[...] = loaded_query[...].astype(jnp.bfloat16)
    wide_key[...] = loaded_key[...].astype(jnp.bfloat16)

    def spread_basis(i):
        source = behind(i)
        basis_fs(0, source, source).wait_recv()
        for slot in (0, 1):
            basis_hop(source, slot, owners[slot]).start()

    each(1, fs, spread_basis)

    own_copies = [
        pltpu.make_async_copy(wide_query, weight_query_all.at[own_block], local.at[1]),
        pltpu.make_async_copy(wide_key, weight_key_all.at[own_block], local.at[2]),
    ]
    for copy in own_copies:
        copy.start()

    def start_weight(i):
        weight_fs(0, f, ahead(i)).start()
        weight_fs(1, f, ahead(i)).start()

    each(1, fs, start_weight)

    def relay_basis(i):
        source = behind(i)
        for slot in (0, 1):
            basis_hop(source, slot, senders[slot]).wait_recv()
            basis_hop(source, slot + 2, owners[slot + 2]).start()

    def all_basis(i):
        for slot in (2, 3):
            basis_hop(behind(i), slot, senders[slot]).wait_recv()

    each(1, fs, relay_basis)
    each(1, fs, all_basis)
    own_basis.wait()
    for load in loads[2:]:
        load.wait()

    for t in range(0, tokens, LANES):
        value = jnp.dot(
            inputs[t : t + LANES, :], basis_all[c], preferred_element_type=jnp.float32
        )
        factor[c, :, t : t + LANES] = value.T.astype(jnp.bfloat16)
    for u in range(units, per * rep):
        part_send[u] = jnp.zeros(part_send.shape[1:], jnp.bfloat16)
    factor_copy = remote(
        factor.at[c], factor.at[c], pair_s.at[0], pair_r.at[0], tp=1 - c
    )
    factor_back = remote(
        factor.at[1 - c], factor.at[1 - c], pair_s.at[0], pair_r.at[0], tp=1 - c
    )
    factor_copy.start()
    swap = remote(basis_all.at[c], basis_all.at[c], pair_s.at[1], pair_r.at[1], tp=1 - c)
    swap_back = remote(
        basis_all.at[1 - c], basis_all.at[1 - c], pair_s.at[1], pair_r.at[1], tp=1 - c
    )
    factor_back.wait_recv()
    swap.start()

    for x, cot in ((0, cot_query), (1, cot_key)):
        columns = cot.shape[1]
        width = 2 * LANES if columns % (2 * LANES) == 0 else LANES
        for n in range(0, columns, width):
            value = jnp.dot(
                factor[x], cot[:, n : n + width], preferred_element_type=jnp.float32
            ).astype(jnp.bfloat16)
            for k in range(0, width, LANES):
                part_send[x * query_units + (n + k) // LANES] = value[:, k : k + LANES]

    def group(owner):
        return pl.ds(owner * per, per)

    def part_rep(source, target):
        return remote(
            part_send.at[group(target)],
            part_recv.at[source],
            bp_s.at[target],
            bp_r.at[source],
            rep=target,
        )

    each(1, rep, lambda j: part_rep(r, beside(j)).start())
    part_recv[r] = part_send[group(r)]
    each(1, rep, lambda j: part_rep(beside(j), beside(j)).wait_recv())
    for p in range(per):
        value = part_recv[0, p].astype(jnp.float32)
        for q in range(1, rep):
            value = value + part_recv[q, p].astype(jnp.float32)
        slab[p] = value.astype(jnp.bfloat16)

    def slab_fs(source, target):
        return remote(
            slab.at[:, low_rows(target)],
            slab_recv.at[source],
            bz_s.at[target],
            bz_r.at[source],
            fs=target,
        )

    each(1, fs, lambda i: slab_fs(f, ahead(i)).start())

    def spread_weight(i):
        source = behind(i)
        for x in range(2):
            weight_fs(x, source, source).wait_recv()
            for slot in (0, 1):
                weight_hop(x, source, slot, owners[slot]).start()

    def relay_weight(i):
        source = behind(i)
        for slot in (0, 1):
            for x in range(2):
                weight_hop(x, source, slot, senders[slot]).wait_recv()
                weight_hop(x, source, slot + 2, owners[slot + 2]).start()

    spread_weight(1)
    slab_recv[f] = slab[:, low_rows(f), :]
    each(1, fs, lambda i: slab_fs(behind(i), behind(i)).wait_recv())
    for p in range(per):
        value = slab_recv[0, p].astype(jnp.float32)
        for q in range(1, fs):
            value = value + slab_recv[q, p].astype(jnp.float32)
        low_all[r * per + p] = value.astype(jnp.bfloat16)

    def low_rep(owner, target):
        block = low_all.at[group(owner)]
        return remote(block, block, lp_s.at[target], lp_r.at[owner], rep=target)

    each(1, rep, lambda j: low_rep(r, beside(j)).start())
    each(1, rep, lambda j: low_rep(beside(j), beside(j)).wait_recv())

    for x, moments, direction, low_out in (
        (0, moments_query, dir_query, low_query),
        (1, moments_key, dir_key, low_key),
    ):
        total = jnp.zeros((8, LANES), jnp.float32)
        for n in range(0, moments.shape[2], LANES):
            span = slice(n, n + LANES)
            low = low_all[x * query_units + n // LANES].astype(jnp.float32)
            low_out[:, span] = low
            first = 0.9 * moments[0, :, span] + 0.1 * low
            second = 0.95 * moments[1, :, span] + 0.05 * low * low
            normed = first / (jnp.sqrt(second) + 1e-08)
            direction[low_rows(f), span] = normed.astype(jnp.bfloat16)
            total = total + jnp.sum((normed * normed).reshape(rows // 8, 8, LANES), axis=0)
        squares[f, x] = total

    directions = (dir_query, dir_key)

    right, left = ahead(1), behind(1)

    def move_right(x, source):
        block = directions[x].at[low_rows(source)]
        return remote(block, block, dr_s.at[x, source], dz_r.at[x, source], fs=right)

    def move_left(x, source):
        block = directions[x].at[low_rows(source)]
        return remote(block, block, dl_s.at[x, source], dz_r.at[x, source], fs=left)

    def squares_fs(source, target):
        block = squares.at[source]
        return remote(block, block, qz_s.at[target], qz_r.at[source], fs=target)

    each(1, fs, lambda i: squares_fs(f, ahead(i)).start())

    @pl.when(f + 1 < fs)
    def start_right():
        for x in range(2):
            move_right(x, f).start()

    @pl.when(f > 0)
    def start_left():
        for x in range(2):
            move_left(x, f).start()

    each(2, fs, spread_weight)

    def relay_direction(k):
        @pl.when(f - k >= 0)
        def from_left():
            for x in range(2):
                move_right(x, f - k).wait_recv()

                @pl.when(f + 1 < fs)
                def onward():
                    move_right(x, f - k).start()

        @pl.when(f + k < fs)
        def from_right():
            for x in range(2):
                move_left(x, f + k).wait_recv()

                @pl.when(f > 0)
                def onward():
                    move_left(x, f + k).start()

    def relay_both(k):
        relay_weight(k)
        relay_direction(k)

    each(1, fs, relay_both)

    each(1, fs, lambda i: squares_fs(behind(i), behind(i)).wait_recv())
    total = squares[0]
    for q in range(1, fs):
        total = total + squares[q]
    pair[c] = total
    total_copy = remote(pair.at[c], pair.at[c], pair_s.at[2], pair_r.at[2], tp=1 - c)
    total_back = remote(pair.at[1 - c], pair.at[1 - c], pair_s.at[2], pair_r.at[2], tp=1 - c)
    total_copy.start()
    total_back.wait_recv()
    totals[...] = pair[0] + pair[1]

    def end_fs(i):
        source, target = behind(i), ahead(i)
        for x in range(2):
            for slot in (2, 3):
                weight_hop(x, source, slot, senders[slot]).wait_recv()
            for slot in range(4):
                weight_hop(x, source, slot, owners[slot]).wait_send()
            weight_fs(x, f, target).wait_send()
        for slot in range(4):
            basis_hop(source, slot, owners[slot]).wait_send()
        basis_fs(0, f, target).wait_send()
        slab_fs(f, target).wait_send()
        squares_fs(f, target).wait_send()

    def end_direction(k):
        @pl.when((f - k >= 0) & (f + 1 < fs))
        def end_right():
            for x in range(2):
                move_right(x, f - k).wait_send()

        @pl.when((f + k < fs) & (f > 0))
        def end_left():
            for x in range(2):
                move_left(x, f + k).wait_send()

    def end_rep(j):
        part_rep(r, beside(j)).wait_send()
        low_rep(r, beside(j)).wait_send()

    each(1, fs, end_fs)
    each(0, fs, end_direction)
    each(1, rep, end_rep)
    swap_back.wait_recv()
    factor_copy.wait_send()
    swap.wait_send()
    total_copy.wait_send()
    for copy in own_copies:
        copy.wait()


def exchange_grid(
    fs,
    rep,
    inputs_far,
    cot_query_far,
    cot_key_far,
    basis_query,
    basis_key,
    full_query,
    full_key,
    moments_query_far,
    moments_key_far,
    step_query,
    step_key,
    new_weight_query,
    new_weight_key,
    copy_query,
    copy_key,
    new_moments_query,
    new_moments_key,
    basis_all,
    weight_query_all,
    weight_key_all,
    dir_query,
    dir_key,
    inputs,
    cot_query,
    cot_key,
    moments_query,
    moments_key,
    loaded_query,
    loaded_key,
    factor,
    part,
    got_first,
    pair_sum,
    got_second,
    slab,
    slab_recv,
    low_all,
    part_squares,
    squares,
    pair,
    late_query,
    late_key,
    line_s,
    key_s,
    basis_line_r,
    query_line_r,
    key_line_r,
    hop_s,
    basis_hop_r,
    query_hop_r,
    basis_end_r,
    query_end_r,
    halve_s,
    first_r,
    second_r,
    slab_s,
    slab_r,
    low_s,
    low_r,
    low_end_r,
    dir_s,
    dir_r,
    dir_hop_s,
    dir_hop_r,
    dir_end_r,
    squares_s,
    squares_r,
    pair_s,
    pair_r,
    local,
):
    f, r, c = lax.axis_index("fs"), lax.axis_index("rep"), lax.axis_index("tp")
    height, rank = basis_query.shape
    quarter = height // rep
    rows = rank // fs
    own = rows // rep
    tokens = inputs.shape[0]
    query_units = cot_query.shape[1] // LANES
    units = query_units + cot_key.shape[1] // LANES
    streams = ((0, units // 2), (units // 2, units // 2))
    f32, bf16 = jnp.float32, jnp.bfloat16

    near = r + 1 - 2 * lax.rem(r, 2)
    far = r + 2 - 4 * (r // 2)
    across = 3 - r

    def when(conds, body):
        if not conds:
            body()
            return
        test = conds[0]
        for cond in conds[1:]:
            test = test & cond
        pl.when(test)(body)

    def send(make, *conds):
        when(conds, lambda: make().start())

    def arrived(block, sem, *conds):
        when(conds, lambda: remote(block, block, sem, sem, tp=1 - c).wait_recv())

    def departed(block, sem, *conds):
        when(conds, lambda: remote(block, block, sem, sem, tp=1 - c).wait_send())

    def sources(d):
        return ((f - d, f >= d), (f + d, f + d < fs))

    def beside(j):
        return lax.rem(r + j, rep)

    def rows_of(start, size):
        return pl.ds(pl.multiple_of(start, size), size)

    chunks = 2
    chunk = quarter // chunks
    fine = basis_line_r.shape[1]

    def piece(source, owner, k, parts=chunks):
        size = quarter // parts
        return rows_of(source * height + owner * quarter + k * size, size)

    mirror = f // (fs // 2)
    place_in_half = f + mirror * (fs - 1 - 2 * f)

    def other(n):
        low_side = n - 1 + (n + fs - 1 - place_in_half) // fs
        return low_side + mirror * (fs - 1 - 2 * low_side)

    own_block = rows_of(f * height, height)

    loads = [
        pltpu.make_async_copy(source, target, local.at[1 + n])
        for n, (source, target) in enumerate(
            (
                (full_query, loaded_query),
                (full_key, loaded_key),
                (inputs_far, inputs),
                (cot_query_far, cot_query),
                (cot_key_far, cot_key),
                (moments_query_far, moments_query),
                (moments_key_far, moments_key),
            )
        )
    ]
    bases = (basis_query, basis_key)
    for x in range(2):

        @pl.when(c == x)
        def load_basis():
            pltpu.make_async_copy(bases[x], basis_all.at[c, own_block], local.at[0]).start()

    for load in loads:
        load.start()
    own_basis = pltpu.make_async_copy(basis_query, basis_all.at[c, own_block], local.at[0])
    ways = ((1, f + 1 < fs), (0, f > 0))
    edge = (f == 0) | (f == fs - 1)
    inner = (f > 0) & (f < fs - 1)
    barrier = pltpu.get_barrier_semaphore()

    def greet(up):
        pl.semaphore_signal(
            barrier, inc=1, device_id={"fs": f + 2 * up - 1}, device_id_type=MESH
        )

    for up, there in ways:
        when((there,), functools.partial(greet, up))
    for mate in (near, far):
        pl.semaphore_signal(barrier, inc=1, device_id={"rep": mate}, device_id_type=MESH)
    pl.semaphore_signal(barrier, inc=1, device_id={"tp": 1 - c}, device_id_type=MESH)
    when((edge,), lambda: pl.semaphore_wait(barrier, 4))
    when((inner,), lambda: pl.semaphore_wait(barrier, 5))

    def basis_z(source, up, k):
        block = basis_all.at[c, piece(source, r, k, fine)]
        return remote(block, block, line_s.at[0], basis_line_r.at[source, k], fs=f + 2 * up - 1)

    def hop_span(slot, width):
        return (pl.ds(0, width), pl.ds(0, width), pl.ds(0, width // 2), pl.ds(width // 2, width // 2))[slot]

    targets = (near, far, far, near)
    sent = (r, r, near, far)

    def basis_hop(k, source, slot):
        block = basis_all.at[c, piece(source, sent[slot], k, fine), hop_span(slot, rank)]
        landed = basis_hop_r.at[source, k] if slot < 2 else basis_end_r.at[0]
        return remote(block, block, hop_s.at[0], landed, rep=targets[slot])

    def weight_hop(k, source, slot):
        width = weight_query_all.shape[1]
        block = weight_query_all.at[piece(source, sent[slot], k), hop_span(slot, width)]
        landed = query_hop_r.at[source, k] if slot < 2 else query_end_r.at[source]
        return remote(block, block, hop_s.at[1], landed, rep=targets[slot])

    def spread(hop, source, *there):
        for slot in (0, 1):
            send(functools.partial(hop, source, slot), *there)

    def relay(hop, both, sem, source, *there):
        arrived(both, sem, *there)
        for slot in (2, 3):
            send(functools.partial(hop, source, slot), *there)

    def relay_basis(k, source, *there):
        both = basis_all.at[c, pl.ds(0, 2 * (quarter // fine))]
        relay(functools.partial(basis_hop, k), both, basis_hop_r.at[source, k], source, *there)

    def relay_weight(k, source):
        both = weight_query_all.at[pl.ds(0, 2 * chunk)]
        relay(functools.partial(weight_hop, k), both, query_hop_r.at[source, k], source)

    def query_z(source, up, k):
        block = weight_query_all.at[piece(source, r, k)]
        return remote(block, block, line_s.at[1], query_line_r.at[source, k], fs=f + 2 * up - 1)

    def key_z(source, up, k):
        size = height // chunks
        block = weight_key_all.at[rows_of(source * height + k * size, size)]
        return remote(block, block, key_s.at[up], key_line_r.at[source, k], fs=f + 2 * up - 1)

    def launch(line, parts=chunks):
        for k in range(parts):
            for up, there in ways:
                send(functools.partial(line, f, up, k), there)

    def onward(line, d, k, *conds):
        for source, there, up, more in (
            (f - d, f >= d, 1, f + 1 < fs),
            (f + d, f + d < fs, 0, f > 0),
        ):
            when((there, *conds), lambda: line(source, up, k).wait_recv())
            if d + 1 < fs:
                send(functools.partial(line, source, up, k), there, more, *conds)

    def onward_all(line, d, parts=chunks):
        for k in range(parts):
            onward(line, d, k)

    own_basis.wait()
    launch(basis_z, fine)
    for load in loads[:2]:
        load.wait()
    weight_query_all[own_block, :] = loaded_query[...].astype(bf16)
    weight_key_all[own_block, :] = loaded_key[...].astype(bf16)

    steps = [(d, k) for d in range(1, fs) for k in range(fine)]
    for n, (d, k) in enumerate(steps):
        onward(basis_z, d, k)
        for source, there in sources(d):
            spread(functools.partial(basis_hop, k), source, there)
        if (d, k) == (max(fs - 2, 1), fine - 1):
            launch(query_z)
        if n >= 6:
            before, j = steps[n - 6]
            for source, there in sources(before):
                relay_basis(j, source, there)
    for d, k in steps[-6:]:
        for source, there in sources(d):
            relay_basis(k, source, there)
    onward_all(query_z, 1)
    launch(key_z)
    spread(functools.partial(weight_hop, 0), other(1))
    spread(functools.partial(weight_hop, 1), other(1), c == 1)
    arrived(basis_all.at[c, pl.ds(0, (fs - 1) * quarter)], basis_end_r.at[0])
    for load in loads[2:]:
        load.wait()

    for t in range(0, tokens, LANES):
        value = jnp.dot(inputs[t : t + LANES, :], basis_all[c], preferred_element_type=f32)
        factor[c, :, t : t + LANES] = value.T.astype(bf16)

    def partner(block, back, n):
        return (
            remote(block, block, pair_s.at[n], pair_r.at[n], tp=1 - c),
            remote(back, back, pair_s.at[n], pair_r.at[n], tp=1 - c),
        )

    factor_copy, factor_back = partner(factor.at[c], factor.at[1 - c], 0)
    swap, swap_back = partner(basis_all.at[c], basis_all.at[1 - c], 1)
    factor_copy.start()
    factor_back.wait_recv()
    swap.start()

    for x, cot in ((0, cot_query), (1, cot_key)):
        columns = cot.shape[1]
        width = 2 * LANES if columns % (2 * LANES) == 0 else LANES
        for n in range(0, columns, width):
            value = jnp.dot(
                factor[x], cot[:, n : n + width], preferred_element_type=f32
            ).astype(bf16)
            for k in range(0, width, LANES):
                for q in range(rep):
                    for s in range(fs):
                        part[x * query_units + (n + k) // LANES, q, s * own : (s + 1) * own] = value[
                            s * rows + q * own : s * rows + (q + 1) * own, k : k + LANES
                        ]

    half = rows // 2
    spans = (slice(0, half), slice(half, rows))
    mates = ((near, far), (far, near))

    def columns_of(g):
        return pl.ds(streams[g][0], streams[g][1])

    def first_hop(h, g, w):
        owner = (across, mates[h][0])[w]
        return remote(
            part.at[columns_of(g), owner, pl.ds(h * half, half)],
            got_first.at[h, w, columns_of(g)],
            halve_s.at[0],
            (first_r, second_r)[w].at[g],
            rep=mates[h][0],
        )

    def second_hop(h, g):
        return remote(
            pair_sum.at[h, columns_of(g)],
            got_second.at[h, columns_of(g)],
            halve_s.at[1],
            second_r.at[g],
            rep=mates[h][1],
        )

    def start_first(g, w):
        for h in range(2):
            first_hop(h, g, w).start()

    def start_second(g):
        arrived(got_first.at[:, 0, columns_of(g)], first_r.at[g])
        for h in range(2):
            for u in range(streams[g][0], sum(streams[g])):
                pair_sum[h, u] = (
                    part[u, mates[h][1], spans[h]].astype(f32) + got_first[h, 0, u].astype(f32)
                ).astype(bf16)
            second_hop(h, g).start()

    def slab_z(g, source, target):
        return remote(
            slab.at[columns_of(g), rows_of(target * own, own)],
            slab_recv.at[source, columns_of(g)],
            slab_s.at[0],
            slab_r.at[g],
            fs=target,
        )

    def end_rep(g):
        arrived(got_first.at[:, :, columns_of(g)], second_r.at[g])
        for h in range(2):
            for u in range(streams[g][0], sum(streams[g])):
                slab[u, spans[h]] = (
                    part[u, r, spans[h]].astype(f32)
                    + got_first[h, 1, u].astype(f32)
                    + got_second[h, u].astype(f32)
                ).astype(bf16)
        for n in range(fs - 1, 0, -1):
            slab_z(g, f, other(n)).start()
        for u in range(streams[g][0], sum(streams[g])):
            slab_recv[f, u] = slab[u, rows_of(f * own, own)]

    start_first(0, 0)
    start_first(0, 1)
    start_first(1, 0)
    start_second(0)
    start_first(1, 1)
    start_second(1)
    spread(functools.partial(weight_hop, 1), other(1), c == 0)
    end_rep(0)
    end_rep(1)
    for k in range(chunks):
        when((edge,), lambda: query_z(other(2), 1, k).wait_recv())
        spread(functools.partial(weight_hop, k), other(2))

    directions, new_moments = (dir_query, dir_key), (new_moments_query, new_moments_key)
    moments = (moments_query, moments_key)

    def place(u):
        x = 0 if u < query_units else 1
        n = (u - x * query_units) * LANES
        return x, slice(n, n + LANES)

    def pieces(g):
        first, last = streams[g][0], sum(streams[g])
        found = []
        if first < query_units:
            found.append((0, first * LANES, (min(last, query_units) - first) * LANES))
        if last > query_units:
            start = max(first, query_units)
            found.append((1, (start - query_units) * LANES, (last - start) * LANES))
        return found

    def dir_rows(source, owner):
        return rows_of(source * rows + owner * own, own)

    def update(g, owner):
        sums = [jnp.zeros((8, LANES), f32), jnp.zeros((8, LANES), f32)]
        mine = rows_of(owner * own, own)
        for u in range(streams[g][0], sum(streams[g])):
            x, span = place(u)
            low = low_all[owner, u].astype(f32)
            first = 0.9 * moments[x][0, mine, span] + 0.1 * low
            second = 0.95 * moments[x][1, mine, span] + 0.05 * low * low
            new_moments[x][0, mine, span] = first
            new_moments[x][1, mine, span] = second
            normed = first / (jnp.sqrt(second) + 1e-08)
            directions[x][dir_rows(f, owner), span] = normed.astype(bf16)
            sums[x] = sums[x] + jnp.sum((normed * normed).reshape(own // 8, 8, LANES), axis=0)
        for x in range(2):
            part_squares[owner, g, x] = sums[x]

    def low_hop(g, slot):
        block = low_all.at[sent[slot], columns_of(g)]
        landed = low_r.at[g] if slot == g else low_end_r.at[0]
        return remote(block, block, low_s.at[0], landed, rep=targets[slot])

    def dir_blocks(g, source, owner):
        return [
            (x, directions[x].at[dir_rows(source, owner), pl.ds(start, size)])
            for x, start, size in pieces(g)
        ]

    def dir_line(g, source, up):
        for x, block in dir_blocks(g, source, r):
            remote(block, block, dir_s.at[x], dir_r.at[g, source], fs=f + 2 * up - 1).start()

    def dir_hop(g, slot, n):
        landed = dir_hop_r.at[n - 1, g] if slot == g else dir_end_r.at[0]
        for x, block in dir_blocks(g, other(n), sent[slot]):
            remote(block, block, dir_hop_s.at[0], landed, rep=targets[slot]).start()

    def end_fs(g):
        arrived(slab_recv.at[pl.ds(0, fs - 1), columns_of(g)], slab_r.at[g])
        for u in range(streams[g][0], sum(streams[g])):
            value = slab_recv[0, u].astype(f32)
            for q in range(1, fs):
                value = value + slab_recv[q, u].astype(f32)
            low_all[r, u] = value.astype(bf16)
        for slot in (0, 1):
            low_hop(g, slot).start()
        update(g, r)
        for up, there in ways:
            when((there,), lambda: dir_line(g, f, up))

    end_fs(0)
    end_fs(1)

    def onward_dir(d):
        for g in range(2):
            for source, there, up, more in (
                (f - d, f >= d, 1, f + 1 < fs),
                (f + d, f + d < fs, 0, f > 0),
            ):
                arrived(low_all.at[r, columns_of(g)], dir_r.at[g, source], there)
                if d + 1 < fs:
                    when((there, more), lambda: dir_line(g, source, up))

    def spread_dir(n, *conds):
        for g in range(2):
            for slot in (0, 1):
                when(conds, lambda: dir_hop(g, slot, n))

    def relay_dir(n):
        for g in range(2):
            arrived(low_all.at[r, columns_of(g)], dir_hop_r.at[n - 1, g])
            dir_hop(g, g + 2, n)

    for k in range(chunks):
        relay_weight(k, other(1))
    onward_dir(1)
    spread_dir(1)
    spread_dir(2, inner)
    for g in range(2):
        arrived(low_all.at[r, columns_of(g)], low_r.at[g])
        low_hop(g, g + 2).start()
    onward_dir(2)
    spread_dir(2, edge)
    spread_dir(3, inner)
    for k in range(chunks):
        onward(query_z, 2, k, inner)
    relay_dir(1)
    onward_dir(3)
    spread_dir(3, edge)
    arrived(low_all.at[pl.ds(0, 2)], low_end_r.at[0])
    for g in range(2):
        for j in range(1, rep):
            update(g, beside(j))
    for x in range(2):
        total = part_squares[0, 0, x] + part_squares[0, 1, x]
        for q in range(1, rep):
            total = total + (part_squares[q, 0, x] + part_squares[q, 1, x])
        squares[f, x] = total

    mine = squares.at[f]
    for n in range(1, fs):
        remote(mine, mine, squares_s.at[0], squares_r.at[0], fs=other(n)).start()
    onward_all(key_z, 1)
    relay_dir(2)
    relay_dir(3)
    relay_weight(0, other(2))
    for n in range(3, fs):
        for k in range(chunks):
            onward(query_z, n, k)
            spread(functools.partial(weight_hop, k), other(n))
    relay_weight(1, other(2))
    def relay_last(k):
        for n in range(3, fs):
            relay_weight(k, other(n))

    def finish_weight(n):
        arrived(weight_query_all.at[pl.ds(0, quarter)], query_end_r.at[other(n)])

    arrived(squares.at[pl.ds(0, fs - 1)], squares_r.at[0])
    total = squares[0]
    for q in range(1, fs):
        total = total + squares[q]
    pair[c] = total
    total_copy, total_back = partner(pair.at[c], pair.at[1 - c], 2)
    total_copy.start()
    arrived(part.at[:, pl.ds(0, fs - 1), pl.ds(0, 2 * own)], dir_end_r.at[0])
    total_back.wait_recv()
    totals = pair[0] + pair[1]
    onward(key_z, 2, 0)
    weights_all, copies = (weight_query_all, weight_key_all), (copy_query, copy_key)
    scales = [
        lax.rsqrt(jnp.sum(totals[x], keepdims=True) / (pair.shape[0] * rank * copies[x].shape[1]) + 1e-06)
        for x in range(2)
    ]

    def product(x, span, columns):
        return scales[x] * jnp.dot(
            basis_all[x, span], directions[x][:, columns], preferred_element_type=f32
        )

    def column_blocks(x):
        wide = copies[x].shape[1]
        width = 2 * LANES if wide % (2 * LANES) == 0 else LANES
        return [slice(n, n + width) for n in range(0, wide, width)]

    def ahead_rows(x, start, size, held):
        for columns in column_blocks(x):
            held[pl.ds(0, size), columns] = 0.02 * product(x, rows_of(start, size), columns)

    def late_rows(x, start, size, held):
        span = rows_of(start, size)
        weight = weights_all[x][span].astype(f32)
        copies[x][span] = (weight - held[pl.ds(0, size)]).astype(bf16)

    def copy_rows(x, start, size):
        span = rows_of(start, size)
        for columns in column_blocks(x):
            weight = weights_all[x][span, columns].astype(f32)
            copies[x][span, columns] = (weight - 0.02 * product(x, span, columns)).astype(bf16)

    swap_back.wait_recv()
    for x, weight, step_out, new_out in (
        (0, loaded_query, step_query, new_weight_query),
        (1, loaded_key, step_key, new_weight_key),
    ):
        for columns in column_blocks(x):
            step = product(x, own_block, columns)
            step_out[:, columns] = step
            new = weight[:, columns] - 0.02 * step
            new_out[:, columns] = new
            copies[x][own_block, columns] = new.astype(bf16)

    finish_weight(1)
    copy_rows(0, other(1) * height, height)
    relay_last(0)
    onward(key_z, 2, 1)
    for n in (1, 2):
        copy_rows(1, other(n) * height, height)
    relay_last(1)
    for n in range(3, fs):
        for owner in (r, near, far):
            copy_rows(0, other(n) * height + owner * quarter, quarter)
    for n in range(3, fs):
        ahead_rows(0, other(n) * height + across * quarter, quarter, late_query)
        ahead_rows(1, other(n) * height, height, late_key)
    finish_weight(2)
    copy_rows(0, other(2) * height, height)
    for d in range(3, fs):
        onward_all(key_z, d)
    for n in range(3, fs):
        late_rows(1, other(n) * height, height, late_key)
    for n in range(3, fs):
        finish_weight(n)
        late_rows(0, other(n) * height + across * quarter, quarter, late_query)
    hops = (fs - 1) * (rep - 1) * quarter
    for n, block in ((0, basis_all.at[c]), (1, weight_query_all)):
        departed(block.at[pl.ds(0, quarter)], line_s.at[n], edge)
        departed(block.at[pl.ds(0, (fs + 1) * quarter)], line_s.at[n], inner)
        departed(block.at[pl.ds(0, hops)], hop_s.at[n])
    for n in range(fs):
        if n < fs - 1:
            departed(weight_key_all.at[pl.ds(0, (n + 1) * height)], key_s.at[1], f == n)
        if n > 0:
            departed(weight_key_all.at[pl.ds(0, (fs - n) * height)], key_s.at[0], f == n)
    departed(got_first, halve_s.at[0])
    departed(pair_sum, halve_s.at[1])
    departed(slab_recv.at[pl.ds(0, fs - 1)], slab_s.at[0])
    departed(low_all.at[pl.ds(0, rep - 1)], low_s.at[0])
    for x in range(2):
        departed(directions[x].at[pl.ds(0, own)], dir_s.at[x], edge)
        departed(directions[x].at[pl.ds(0, (fs + 1) * own)], dir_s.at[x], inner)
    departed(part.at[:, pl.ds(0, fs - 1), pl.ds(0, (rep - 1) * own)], dir_hop_s.at[0])
    departed(squares.at[pl.ds(0, fs - 1)], squares_s.at[0])
    for copy in (factor_copy, swap, total_copy):
        copy.wait_send()


def write_out(*refs):
    count = len(refs) // 2
    copies, starts = [], []
    for n, (source, target) in enumerate(zip(refs[:count], refs[count : 2 * count])):
        copies.append(pltpu.make_async_copy(source, target, refs[-1].at[n]))
        size = source.shape[0] // 4 if source.ndim == 2 else 1
        for start in range(0, source.shape[0], size):
            span = pl.ds(start, size)
            starts.append(pltpu.make_async_copy(source.at[span], target.at[span], refs[-1].at[n]))
    for copy in starts:
        copy.start()
    for copy in copies:
        copy.wait()


def apply(
    count_query,
    count_key,
    totals,
    dir_query,
    dir_key,
    low_query,
    low_key,
    moments_query,
    moments_key,
    basis_all,
    weight_query_all,
    weight_key_all,
    basis_query,
    basis_key,
    weight_query,
    weight_key,
    step_query,
    step_key,
    new_weight_query,
    new_weight_key,
    copy_query,
    copy_key,
    new_moments_query,
    new_moments_key,
):
    parts = (
        (count_query, dir_query, weight_query_all, basis_query, weight_query),
        (count_key, dir_key, weight_key_all, basis_key, weight_key),
    )
    outs = (
        (step_query, new_weight_query, copy_query),
        (step_key, new_weight_key, copy_key),
    )
    for x in range(2):
        count, direction, weight_all, basis, weight = parts[x]
        step_out, new_weight_out, copy_out = outs[x]
        scale = lax.rsqrt(jnp.sum(totals[x], keepdims=True) / count + 1e-06)
        step = scale * jnp.dot(basis[...], direction[...], preferred_element_type=jnp.float32)
        step_out[...] = step
        new_weight_out[...] = weight[...] - 0.02 * step
        whole = scale * jnp.dot(
            basis_all[x], direction[...], preferred_element_type=jnp.float32
        )
        copy_out[...] = (weight_all[...].astype(jnp.float32) - 0.02 * whole).astype(jnp.bfloat16)

    @pl.when(pl.program_id(0) == 0)
    def moments_once():
        for moments, low_ref, out in (
            (moments_query, low_query, new_moments_query),
            (moments_key, low_key, new_moments_key),
        ):
            low = low_ref[...]
            out[0] = 0.9 * moments[0] + 0.1 * low
            out[1] = 0.95 * moments[1] + 0.05 * low * low


def on_device(
    inputs,
    cot_query,
    cot_key,
    basis_query,
    basis_key,
    weight_query,
    weight_key,
    moments_query,
    moments_key,
):
    fs, rep, tp = lax.axis_size("fs"), lax.axis_size("rep"), lax.axis_size("tp")
    assert tp == 2 and rep == 4
    height, rank = basis_query.shape
    rows = rank // fs
    tokens = inputs.shape[0]
    query_cols, key_cols = cot_query.shape[1], cot_key.shape[1]
    per = -(-((query_cols + key_cols) // LANES) // rep)
    vmem = pl.BlockSpec(memory_space=pltpu.VMEM)
    hbm = pl.BlockSpec(memory_space=pl.ANY)
    bf16, f32 = jnp.bfloat16, jnp.float32
    dma = pltpu.SemaphoreType.DMA
    shape = jax.ShapeDtypeStruct
    owned = tuple(
        shape((height, columns), f32) for columns in (query_cols, key_cols, query_cols, key_cols)
    )
    results = owned + (
        shape((height * fs, query_cols), bf16),
        shape((height * fs, key_cols), bf16),
        shape((2, rows, query_cols), f32),
        shape((2, rows, key_cols), f32),
    )
    own, units = rows // rep, (query_cols + key_cols) // LANES
    if own % 16 == 0 and fs == 4 and units % 2 == 0:
        fresh = pl.pallas_call(
            functools.partial(exchange_grid, fs, rep),
            out_shape=results,
            in_specs=[pl.BlockSpec(memory_space=pltpu.HBM)] * 9,
            out_specs=(vmem,) * 8,
            scratch_shapes=[
                pltpu.VMEM((2, height * fs, rank), bf16),
                pltpu.VMEM((height * fs, query_cols), bf16),
                pltpu.VMEM((height * fs, key_cols), bf16),
                pltpu.VMEM((rank, query_cols), bf16),
                pltpu.VMEM((rank, key_cols), bf16),
                pltpu.VMEM((tokens, inputs.shape[1]), bf16),
                pltpu.VMEM((tokens, query_cols), bf16),
                pltpu.VMEM((tokens, key_cols), bf16),
                pltpu.VMEM((2, rows, query_cols), f32),
                pltpu.VMEM((2, rows, key_cols), f32),
                pltpu.VMEM((height, query_cols), f32),
                pltpu.VMEM((height, key_cols), f32),
                pltpu.VMEM((2, rank, tokens), bf16),
                pltpu.VMEM((units, rep, rows, LANES), bf16),
                pltpu.VMEM((2, 2, units, rows // 2, LANES), bf16),
                pltpu.VMEM((2, units, rows // 2, LANES), bf16),
                pltpu.VMEM((2, units, rows // 2, LANES), bf16),
                pltpu.VMEM((units, rows, LANES), bf16),
                pltpu.VMEM((fs, units, own, LANES), bf16),
                pltpu.VMEM((rep, units, own, LANES), bf16),
                pltpu.VMEM((rep, 2, 2, 8, LANES), f32),
                pltpu.VMEM((fs, 2, 8, LANES), f32),
                pltpu.VMEM((2, 2, 8, LANES), f32),
                pltpu.VMEM((height // rep, query_cols), f32),
                pltpu.VMEM((height, key_cols), f32),
                dma((2,)),
                dma((2,)),
                dma((fs, 4)),
                dma((fs, 2)),
                dma((fs, 2)),
                dma((2,)),
                dma((fs, 4)),
                dma((fs, 2)),
                dma((1,)),
                dma((fs,)),
                dma((2,)),
                dma((2,)),
                dma((2,)),
                dma((1,)),
                dma((2,)),
                dma((1,)),
                dma((2,)),
                dma((1,)),
                dma((2,)),
                dma((2, fs)),
                dma((1,)),
                dma((fs - 1, 2)),
                dma((1,)),
                dma((1,)),
                dma((1,)),
                dma((3,)),
                dma((3,)),
                dma((8,)),
            ],
            compiler_params=pltpu.CompilerParams(
                collective_id=0, has_side_effects=True, vmem_limit_bytes=40 * 1024 * 1024
            ),
        )(
            *(
                pltpu.with_memory_space_constraint(operand, pltpu.HBM)
                for operand in (
                    inputs,
                    cot_query,
                    cot_key,
                    basis_query,
                    basis_key,
                    weight_query,
                    weight_key,
                    moments_query,
                    moments_key,
                )
            )
        )
        return pl.pallas_call(
            write_out,
            out_shape=results,
            in_specs=[vmem] * 8,
            out_specs=(hbm,) * 8,
            scratch_shapes=[dma((8,))],
            compiler_params=pltpu.CompilerParams(vmem_limit_bytes=32 * 1024 * 1024),
        )(*fresh)

    (
        basis_all,
        weight_query_all,
        weight_key_all,
        dir_query,
        dir_key,
        low_query,
        low_key,
        totals,
    ) = pl.pallas_call(
        functools.partial(exchange, fs, rep),
        out_shape=(
            shape((2, height * fs, rank), bf16),
            shape((height * fs, query_cols), bf16),
            shape((height * fs, key_cols), bf16),
            shape((rank, query_cols), bf16),
            shape((rank, key_cols), bf16),
            shape((rows, query_cols), f32),
            shape((rows, key_cols), f32),
            shape((2, 8, LANES), f32),
        ),
        in_specs=[pl.BlockSpec(memory_space=pltpu.HBM)] * 9,
        out_specs=(vmem, hbm, hbm, vmem, vmem, vmem, vmem, vmem),
        scratch_shapes=[
            pltpu.VMEM((tokens, inputs.shape[1]), bf16),
            pltpu.VMEM((tokens, query_cols), bf16),
            pltpu.VMEM((tokens, key_cols), bf16),
            pltpu.VMEM((2, rows, query_cols), f32),
            pltpu.VMEM((2, rows, key_cols), f32),
            pltpu.VMEM((height, query_cols), f32),
            pltpu.VMEM((height, key_cols), f32),
            pltpu.VMEM((height, query_cols), bf16),
            pltpu.VMEM((height, key_cols), bf16),
            pltpu.VMEM((2, rank, tokens), bf16),
            pltpu.VMEM((per * rep, rank, LANES), bf16),
            pltpu.VMEM((rep, per, rank, LANES), bf16),
            pltpu.VMEM((per, rank, LANES), bf16),
            pltpu.VMEM((fs, per, rows, LANES), bf16),
            pltpu.VMEM((per * rep, rows, LANES), bf16),
            pltpu.VMEM((fs, 2, 8, LANES), f32),
            pltpu.VMEM((2, 2, 8, LANES), f32),
            dma((fs,)),
            dma((fs,)),
            dma((fs, rep)),
            dma((fs, rep)),
            dma((2, fs)),
            dma((2, fs)),
            dma((2, fs, rep)),
            dma((2, fs, rep)),
            dma((rep,)),
            dma((rep,)),
            dma((fs,)),
            dma((fs,)),
            dma((rep,)),
            dma((rep,)),
            dma((2, fs)),
            dma((2, fs)),
            dma((2, fs)),
            dma((fs,)),
            dma((fs,)),
            dma((3,)),
            dma((3,)),
            dma((10,)),
        ],
        compiler_params=pltpu.CompilerParams(
            collective_id=0, has_side_effects=True, vmem_limit_bytes=32 * 1024 * 1024
        ),
    )(
        *(
            pltpu.with_memory_space_constraint(operand, pltpu.HBM)
            for operand in (
                inputs,
                cot_query,
                cot_key,
                basis_query,
                basis_key,
                weight_query,
                weight_key,
                moments_query,
                moments_key,
            )
        )
    )

    steps = min(8, height // 16)
    tall, short = height * fs // steps, height // steps

    def fixed(*dims):
        return pl.BlockSpec(dims, lambda i: (0,) * len(dims))

    def banded(*dims):
        return pl.BlockSpec(dims, lambda i: (i, 0))

    owned_specs = tuple(
        banded(short, columns) for columns in (query_cols, key_cols, query_cols, key_cols)
    )
    return pl.pallas_call(
        functools.partial(
            apply, float(rank * query_cols * tp), float(rank * key_cols * tp)
        ),
        grid=(steps,),
        out_shape=results,
        in_specs=[
            fixed(2, 8, LANES),
            fixed(rank, query_cols),
            fixed(rank, key_cols),
            fixed(rows, query_cols),
            fixed(rows, key_cols),
            fixed(2, rows, query_cols),
            fixed(2, rows, key_cols),
            pl.BlockSpec((2, tall, rank), lambda i: (0, i, 0)),
            banded(tall, query_cols),
            banded(tall, key_cols),
            banded(short, rank),
            banded(short, rank),
            banded(short, query_cols),
            banded(short, key_cols),
        ],
        out_specs=owned_specs
        + (
            banded(tall, query_cols),
            banded(tall, key_cols),
            fixed(2, rows, query_cols),
            fixed(2, rows, key_cols),
        ),
        compiler_params=pltpu.CompilerParams(
            dimension_semantics=("arbitrary",), vmem_limit_bytes=32 * 1024 * 1024
        ),
    )(
        totals,
        dir_query,
        dir_key,
        low_query,
        low_key,
        moments_query,
        moments_key,
        basis_all,
        weight_query_all,
        weight_key_all,
        basis_query,
        basis_key,
        weight_query,
        weight_key,
    )


def solution(mesh):
    in_specs = (
        P(("fs", "rep"), None),
        P(("fs", "rep"), "tp"),
        P(("fs", "rep"), "tp"),
        P("fs", None),
        P("fs", None),
        P("fs", "tp"),
        P("fs", "tp"),
        P(None, "fs", "tp"),
        P(None, "fs", "tp"),
    )
    out_specs = (
        P("fs", "tp"),
        P("fs", "tp"),
        P("fs", "tp"),
        P("fs", "tp"),
        P(None, "tp"),
        P(None, "tp"),
        P(None, "fs", "tp"),
        P(None, "fs", "tp"),
    )
    return jax.shard_map(
        on_device, mesh=mesh, in_specs=in_specs, out_specs=out_specs, check_vma=False
    )
```
